32 devices in a mesh: fs: 8 (over z, y), tp: 4 (over x, core).
Axes of the slice: x: 2, y: 2, z: 4, core: 2. Of those that a mesh axis runs over, the one named last changes fastest.
Arguments:
- inputs: bfloat16 [4096, 2048], P(('fs', 'tp')), may hold values from -6 to 6
- w_gate: float32 [2048, 5632], P('fs', 'tp'), may hold values from -0.125 to 0.125
- w_value: float32 [2048, 5632], P('fs', 'tp'), may hold values from -0.125 to 0.125
- gate_scale: float32 [5632], P('tp'), may hold values from 0.5 to 2
- value_scale: float32 [5632], P('tp'), may hold values from 0.5 to 2
- conv_gate: float32 [3, 5632], P(None, 'tp'), may hold values from -3.5 to 3.5
- conv_value: float32 [3, 5632], P(None, 'tp'), may hold values from -3.5 to 3.5
- gate_pre: bfloat16 [4096, 5632], P('fs', 'tp'), may hold values from -6 to 6
- value_pre: bfloat16 [4096, 5632], P('fs', 'tp'), may hold values from -6 to 6
- grad_out: bfloat16 [4096, 5632], P('fs', 'tp'), may hold values from -6 to 6
Outputs:
- grad_inputs: bfloat16 [4096, 2048], P(('fs', 'tp'))
- grad_w_gate: float32 [2048, 5632], P('fs', 'tp')
- grad_w_value: float32 [2048, 5632], P('fs', 'tp')
- grad_gate_scale: float32 [5632], P('tp')
- grad_value_scale: float32 [5632], P('tp')
- grad_conv_gate: float32 [3, 5632], P(None, 'tp')
- grad_conv_value: float32 [3, 5632], P(None, 'tp')
The draws below stay inside these ranges and needn't reach their ends.
All inputs are finite; a program needn't handle non-finite values.
Results may differ from the reference program's by a relative error of at most 0.015.
Values may be sent and summed in bfloat16 or wider, within the bound.
A program may use at most 128 MiB of HBM per device.

```python
import math
import jax
import jax.numpy as jnp

D = 2048
FF = 5632
KW = 3
SEQ = 512
TOKENS = 4096
N_FS = 8
N_TP = 4


def strengthened(result, rng, source, target, parts, factor):
    def block_of(position):
        return (jnp.arange(result.shape[position]) // (result.shape[position] // parts)).reshape((-1,) + (1,) * (result.ndim - 1 - position))

    one_side = jax.random.permutation(rng, parts)[block_of(target)]
    second = (block_of(target) + parts // 2) % parts
    return jnp.where((block_of(source) == one_side) | (block_of(source) == second), factor * result, result)


def levels(key, dims, split, least, largest):
    factor_of = 1.0
    for dim, shards_of in split:
        draws = jax.random.uniform(jax.random.fold_in(jax.random.fold_in(key, 6), dim), (shards_of,), jnp.float32, least / len(split), largest / len(split))
        factor_of = factor_of * jnp.repeat(jnp.exp(draws), dims[dim] // shards_of).reshape((-1,) + (1,) * (len(dims) - 1 - dim))
    return factor_of


def bell_draw(rng, dims, scale, most, shards=(), held_as=jnp.bfloat16):
    result = jax.random.normal(rng, dims, jnp.float32) * scale
    if len(shards) > 0:
        result = levels(rng, dims, shards, -0.22, 0.18) * result
    return jnp.clip(result, min=-most, max=most).astype(held_as)


def gaussian_with(stream_key, extent, spread, reach, shards, heavy, dtype=jnp.bfloat16):
    array = spread * jax.random.normal(stream_key, extent, jnp.float32)
    if shards:
        array = array * levels(stream_key, extent, shards, -0.22, 0.18)
    return jnp.clip(strengthened(array, jax.random.fold_in(stream_key, 3), *heavy), -reach, reach).astype(dtype)


def setup_inputs(seed: int = 0) -> dict:
    key_of = jax.random.split(jax.random.key(seed), 11)
    inputs = gaussian_with(key_of[0], (TOKENS, D), 1.0, 6.0, ((0, 32),), (0, 1, 32, 2.75))
    w_gate = bell_draw(key_of[1], (D, FF), D ** -0.5, 0.125, ((0, 8), (1, 4)), jnp.float32)
    w_value = bell_draw(key_of[2], (D, FF), D ** -0.5, 0.125, ((0, 8), (1, 4)), jnp.float32)
    gate_scale = jnp.clip(jnp.exp(math.log(2.0) - 1.3862944 * jax.random.uniform(key_of[3], (FF,), jnp.float32) ** levels(key_of[3], (FF,), ((0, 4),), -0.2, 0.2)), 0.5, 2.0)
    value_scale = jnp.clip(jnp.exp(math.log(2.0) - 1.3862944 * jax.random.uniform(key_of[4], (FF,), jnp.float32) ** levels(key_of[4], (FF,), ((0, 4),), -0.2, 0.2)), 0.5, 2.0)
    conv_gate = bell_draw(key_of[5], (KW, FF), KW ** -0.5, 3.5, ((1, 4),), jnp.float32)
    conv_value = bell_draw(key_of[6], (KW, FF), KW ** -0.5, 3.5, ((1, 4),), jnp.float32)
    gate_pre = bell_draw(key_of[7], (TOKENS, FF), 1.0, 6.0, ((0, 8), (1, 4)))
    value_pre = bell_draw(key_of[8], (TOKENS, FF), 1.0, 6.0, ((0, 8), (1, 4)))
    grad_out = gaussian_with(key_of[9], (TOKENS, FF), 1.0, 6.0, ((0, 8), (1, 4)), (0, 1, 8, 2.0))
    return {"inputs": inputs, "w_gate": w_gate, "w_value": w_value, "gate_scale": gate_scale, "value_scale": value_scale, "conv_gate": conv_gate, "conv_value": conv_value, "gate_pre": gate_pre, "value_pre": value_pre, "grad_out": grad_out}


def shift_down(field, steps):
    return jnp.pad(field, ((0, 0), (steps, 0), (0, 0)))[:, :field.shape[1]]


def shift_up(field, steps):
    return jnp.pad(field, ((0, 0), (0, steps), (0, 0)))[:, steps:]


def reference(inputs, w_gate, w_value, gate_scale, value_scale, conv_gate, conv_value, gate_pre, value_pre, grad_out):
    gate_raw = gate_pre.astype(jnp.float32).reshape(N_FS, SEQ, FF)
    value_raw = value_pre.astype(jnp.float32).reshape(N_FS, SEQ, FF)
    gate_lin = gate_raw * gate_scale
    value_lin = value_raw * value_scale
    gate_conv = conv_gate[2] * gate_lin + conv_gate[1] * shift_down(gate_lin, 1) + conv_gate[0] * shift_down(gate_lin, 2)
    value_conv = conv_value[2] * value_lin + conv_value[1] * shift_down(value_lin, 1) + conv_value[0] * shift_down(value_lin, 2)
    sig = jax.nn.sigmoid(gate_conv)
    upstream = grad_out.astype(jnp.float32).reshape(N_FS, SEQ, FF)
    d_gate_conv = upstream * value_conv * sig * (1.0 + gate_conv * (1.0 - sig))
    d_value_conv = upstream * gate_conv * sig
    grad_conv_gate = jnp.stack([jnp.sum(d_gate_conv * shift_down(gate_lin, 2), axis=(0, 1)),
                                jnp.sum(d_gate_conv * shift_down(gate_lin, 1), axis=(0, 1)),
                                jnp.sum(d_gate_conv * gate_lin, axis=(0, 1))])
    grad_conv_value = jnp.stack([jnp.sum(d_value_conv * shift_down(value_lin, 2), axis=(0, 1)),
                                 jnp.sum(d_value_conv * shift_down(value_lin, 1), axis=(0, 1)),
                                 jnp.sum(d_value_conv * value_lin, axis=(0, 1))])
    d_gate_lin = conv_gate[2] * d_gate_conv + conv_gate[1] * shift_up(d_gate_conv, 1) + conv_gate[0] * shift_up(d_gate_conv, 2)
    d_value_lin = conv_value[2] * d_value_conv + conv_value[1] * shift_up(d_value_conv, 1) + conv_value[0] * shift_up(d_value_conv, 2)
    grad_gate_scale = jnp.sum(d_gate_lin * gate_raw, axis=(0, 1))
    grad_value_scale = jnp.sum(d_value_lin * value_raw, axis=(0, 1))
    d_gate_lin = d_gate_lin.reshape(TOKENS, FF)
    d_value_lin = d_value_lin.reshape(TOKENS, FF)
    gate_cot = d_gate_lin.astype(jnp.bfloat16)
    value_cot = d_value_lin.astype(jnp.bfloat16)
    gate_back = (d_gate_lin * gate_scale).astype(jnp.bfloat16)
    value_back = (d_value_lin * value_scale).astype(jnp.bfloat16)
    grad_w_gate = jnp.dot(inputs.T, gate_cot, preferred_element_type=jnp.float32) * gate_scale
    grad_w_value = jnp.dot(inputs.T, value_cot, preferred_element_type=jnp.float32) * value_scale
    gate_half = w_gate.astype(jnp.bfloat16)
    value_half = w_value.astype(jnp.bfloat16)
    width = FF // N_TP
    total = jnp.zeros((TOKENS, D), jnp.float32)
    for block in range(N_TP):
        lo = block * width
        part = jnp.dot(gate_back[:, lo:lo + width], gate_half[:, lo:lo + width].T, preferred_element_type=jnp.float32)
        part = part + jnp.dot(value_back[:, lo:lo + width], value_half[:, lo:lo + width].T, preferred_element_type=jnp.float32)
        total = total + part.astype(jnp.bfloat16).astype(jnp.float32)
    grad_inputs = total.astype(jnp.bfloat16)
    return (grad_inputs, grad_w_gate, grad_w_value, grad_gate_scale, grad_value_scale, grad_conv_gate, grad_conv_value)
```

```python
import functools

import jax
import jax.numpy as jnp
from jax import lax
from jax.experimental import pallas as pl
from jax.experimental.pallas import tpu as pltpu
from jax.sharding import PartitionSpec as P


BF = jnp.bfloat16
F32 = jnp.float32


LANES = 128


def elementwise(gs_ref, vs_ref, cg_ref, cv_ref, g_ref, v_ref, up_ref, gc_ref, vc_ref, s_ref):
    tokens = g_ref.shape[0]
    row = lax.broadcasted_iota(jnp.int32, g_ref.shape, 0)

    def down(x, k):
        return jnp.where(row >= k, pltpu.roll(x, k, 0), 0.0)

    def up(x, k):
        return jnp.where(row < tokens - k, pltpu.roll(x, tokens - k, 0), 0.0)

    def shifted(ref):
        x = ref[...].astype(F32)
        return down(x, 2), down(x, 1), x

    def conv(taps, xs):
        return taps[0:1] * xs[0] + taps[1:2] * xs[1] + taps[2:3] * xs[2]

    def back(taps, d):
        return (taps[2:3] * d + taps[1:2] * up(d, 1) + taps[0:1] * up(d, 2)).astype(BF)

    gs, vs = shifted(g_ref), shifted(v_ref)
    g = conv(cg_ref[...] * gs_ref[...], gs)
    v = conv(cv_ref[...] * vs_ref[...], vs)
    sig = 1.0 / (1.0 + jnp.exp(-g))
    base = up_ref[...].astype(F32) * sig
    d_gate = base * v * (1.0 + g * (1.0 - sig))
    d_value = base * g
    for j in range(3):
        s_ref[j : j + 1] = jnp.sum(d_gate * gs[j], axis=0, keepdims=True)
        s_ref[3 + j : 4 + j] = jnp.sum(d_value * vs[j], axis=0, keepdims=True)
    s_ref[6:8] = jnp.zeros((2, g_ref.shape[1]), F32)
    gc_ref[...] = back(cg_ref[...], d_gate)
    vc_ref[...] = back(cv_ref[...], d_value)


def cotangents(gs, vs, cg, cv, g, v, up):
    tokens, columns = g.shape
    big = pl.BlockSpec((tokens, LANES), lambda i: (0, i))

    def small(n):
        return pl.BlockSpec((n, LANES), lambda i: (0, i))

    return pl.pallas_call(
        elementwise,
        grid=(pl.cdiv(columns, LANES),),
        in_specs=[small(1), small(1), small(3), small(3), big, big, big],
        out_specs=[big, big, small(8)],
        out_shape=[jax.ShapeDtypeStruct(g.shape, BF)] * 2
        + [jax.ShapeDtypeStruct((8, columns), F32)],
        compiler_params=pltpu.CompilerParams(vmem_limit_bytes=24 * 2**20),
        cost_estimate=pl.CostEstimate(
            flops=g.size * 400, bytes_accessed=g.size * 10, transcendentals=g.size
        ),
    )(gs[None], vs[None], cg, cv, g, v, up)


def rescale(gs_ref, vs_ref, g_ref, v_ref, out_ref):
    out_ref[0] = (g_ref[...] * gs_ref[...]).astype(BF)
    out_ref[1] = (v_ref[...] * vs_ref[...]).astype(BF)


def scaled_weights(gs, vs, g, v):
    own, columns = g.shape
    parts = 4
    block = pl.BlockSpec((own // parts, columns), lambda i: (i, 0))
    scale = pl.BlockSpec((1, columns), lambda i: (0, 0))
    return pl.pallas_call(
        rescale,
        grid=(parts,),
        in_specs=[scale, scale, block, block],
        out_specs=pl.BlockSpec((2, own // parts, columns), lambda i: (0, i, 0)),
        out_shape=jax.ShapeDtypeStruct((2, own, columns), BF),
        compiler_params=pltpu.CompilerParams(vmem_limit_bytes=24 * 2**20),
        cost_estimate=pl.CostEstimate(
            flops=g.size * 100, bytes_accessed=g.size * 12, transcendentals=0
        ),
    )(gs[None], vs[None], g, v)


def tdot(a, b):
    return lax.dot_general(a, b, (((0,), (0,)), ((), ())), preferred_element_type=F32)


def ndot(a, b):
    return lax.dot_general(a, b, (((1,), (1,)), ((), ())), preferred_element_type=F32)


def make(n_fs, n_tp):
    links = n_fs // 2

    def on_device(
        inputs,
        w_gate,
        w_value,
        gate_scale,
        value_scale,
        conv_gate,
        conv_value,
        gate_pre,
        value_pre,
        grad_out,
    ):
        fs = lax.axis_index("fs")
        tp = lax.axis_index("tp")
        c, y = fs // 2, fs % 2
        rows, depth = inputs.shape
        own = w_gate.shape[0]
        half = depth // 2
        tokens, columns = gate_pre.shape

        def swap(x, axis, bit, n):
            return lax.ppermute(x, axis, [(i, i ^ bit) for i in range(n)])

        def chain(x, right, senders):
            step = 1 if right else -1
            pairs = [(2 * s + j, 2 * (s + step) + j) for s in senders for j in (0, 1)]
            return lax.ppermute(x, "fs", pairs)

        stacked = scaled_weights(gate_scale, value_scale, w_gate, w_value)
        rights, lefts = [], []
        r = l = stacked
        for s in range(links - 1):
            r = chain(r, True, range(s, links - 1))
            l = chain(l, False, range(1, links - s))
            rights.append(r)
            lefts.append(l)

        by_half = inputs.reshape(rows, links, 2, own)
        mine = lax.dynamic_index_in_dim(by_half, y, 2, keepdims=False)
        other = lax.dynamic_index_in_dim(by_half, 1 - y, 2, keepdims=False)
        mine, other = mine.reshape(rows, half), other.reshape(rows, half)
        other = swap(other, "fs", 1, n_fs)
        x = jnp.stack([mine, other])[:, None]
        bit = n_tp // 2
        while bit:
            got = swap(x, "tp", bit, n_tp)
            high = (tp // bit) % 2 == 1
            x = jnp.where(high, jnp.stack([got, x], 2), jnp.stack([x, got], 2))
            x = x.reshape(2, -1, rows, half)
            bit //= 2
        x = x.reshape(2, tokens, half)

        gate_cot, value_cot, sums = cotangents(
            gate_scale, value_scale, conv_gate, conv_value, gate_pre, value_pre, grad_out
        )
        bit = n_fs // 2
        while bit:
            sums = sums + swap(sums, "fs", bit, n_fs)
            bit //= 2

        gate_theirs = swap(gate_cot, "fs", 1, n_fs)
        value_theirs = swap(value_cot, "fs", 1, n_fs)
        pair = [(gate_cot, gate_theirs), (value_cot, value_theirs)]

        def at(blocks, i):
            return lax.dynamic_index_in_dim(
                blocks, jnp.clip(i, 0, links - 1), 0, keepdims=False
            )

        def collect(parts):
            r = l = None
            for t in range(links - 1):
                send_r = at(parts, links - 1 - t + c)
                send_l = at(parts, c - (links - 1 - t) + 0)
                if t:
                    send_r = (send_r.astype(F32) + r.astype(F32)).astype(BF)
                    send_l = (send_l.astype(F32) + l.astype(F32)).astype(BF)
                r = chain(send_r, True, range(0, t + 1))
                l = chain(send_l, False, range(links - 1 - t, links))
            total = at(parts, c).astype(F32)
            if r is not None:
                total = total + r.astype(F32) + l.astype(F32)
            return total

        grads = []
        for (cot, theirs), scale in zip(pair, (gate_scale, value_scale)):
            first = tdot(x[0], cot)
            parts = (first + tdot(x[1], theirs)).astype(BF)
            blocks = parts.reshape(links, own, columns)
            grads.append(collect(blocks) * scale)

        blocks = [stacked]
        for s in range(links - 1):
            blocks.append(jnp.where(c > s, rights[s], lefts[links - 2 - s]))
        columns_of = []
        for block in blocks:
            columns_of.append(
                [
                    (ndot(g, block[0]) + ndot(v, block[1])).astype(BF)
                    for g, v in zip(pair[0], pair[1])
                ]
            )
        part = jnp.stack([jnp.concatenate(t, 1) for t in zip(*columns_of)])
        part = part.reshape(2, n_tp, rows, half)
        bit = 1
        while bit < n_tp:
            split = part.reshape(2, -1, 2, rows, half)
            which = (tp // bit) % 2
            keep = lax.dynamic_index_in_dim(split, which, 2, keepdims=False)
            send = lax.dynamic_index_in_dim(split, 1 - which, 2, keepdims=False)
            got = swap(send, "tp", bit, n_tp)
            part = (keep.astype(F32) + got.astype(F32)).astype(BF)
            bit *= 2
        mine = part.reshape(2, rows, half)[0]
        other = swap(part.reshape(2, rows, half)[1], "fs", 1, n_fs)
        both = jnp.where(
            y == 0, jnp.stack([mine, other], 1), jnp.stack([other, mine], 1)
        ).reshape(rows, 2, links, own)
        order = (c - jnp.arange(links)) % links
        grad_inputs = jnp.take(both, order, axis=2).transpose(0, 2, 1, 3)
        return (
            grad_inputs.reshape(rows, depth),
            grads[0],
            grads[1],
            jnp.sum(conv_gate * sums[0:3], axis=0),
            jnp.sum(conv_value * sums[3:6], axis=0),
            sums[0:3] * gate_scale,
            sums[3:6] * value_scale,
        )

    return on_device


MESH = pl.DeviceIdType.MESH
SKEW = 2


def segments(links, pieces):
    table = []
    for pos in range(links - 1):
        reach = links - 1 - pos
        rows, count, last = [], 0, None
        for tick in range(pieces + SKEW * (reach - 1)):
            live = [k for k in range(reach) if 0 <= tick - SKEW * k < pieces]
            key = (live[0], len(live)) if live else None
            if key and key != last:
                rows.append((count, tick, live[0], len(live)))
            last = key
            count += len(live)
        table.append(rows)
    return table


def fused(dims, *refs):
    n_fs, n_tp = dims
    (
        inp, wg, wv, gs, vs, cg, cv, gp, vp, up,
        gi, gwg, gwv, ggs, gvs, gcg, gcv,
        wraw, pre, wbuf, cot, part, rs0, rs1, xin, xs, xb, xt,
        acc, dxb, dx1, ds1, dx2, ds2, dx3, stage, fin, sown, spair, sfrom, sgot, sput,
        load_sem, ag_sem, rs_sem, z_sem, y_sem, ysend_sem, xsend_sem, xrecv_sem,
        dsend_sem, drecv_sem, ssend_sem, srecv_sem, out_sem,
    ) = refs
    rs = (rs0, rs1)
    links = n_fs // 2
    pieces = cot.shape[0]
    own = wg.shape[0]
    rows, _ = inp.shape
    tokens = gp.shape[0]
    slots = links * pieces

    fs = lax.axis_index("fs")
    tp = lax.axis_index("tp")
    c, y = lax.div(fs, 2), lax.rem(fs, 2)
    xx, core = lax.div(tp, 2), lax.rem(tp, 2)
    y_dev = (fs + 1 - 2 * y, tp)
    x_dev = (fs, tp + 2 - 4 * xx)
    core_dev = (fs, tp + 1 - 2 * core)
    x_tp = tp + 2 - 4 * xx
    position = (c, links - 1 - c)
    follower = ((fs + 2, tp), (fs - 2, tp))

    def real(way, index):
        return index if way == 0 else links - 1 - index

    def remote(src, dst, send, recv, device):
        return pltpu.make_async_remote_copy(
            src_ref=src, dst_ref=dst, send_sem=send, recv_sem=recv,
            device_id=device, device_id_type=MESH,
        )

    def lanes(j):
        return pl.ds(pl.multiple_of(j * LANES, LANES), LANES)

    loads = [
        pltpu.make_async_copy(wg, wraw.at[0], load_sem.at[0]),
        pltpu.make_async_copy(wv, wraw.at[1], load_sem.at[1]),
        pltpu.make_async_copy(inp, xin, load_sem.at[2]),
        pltpu.make_async_copy(gp, pre.at[0], load_sem.at[3]),
        pltpu.make_async_copy(vp, pre.at[1], load_sem.at[4]),
        pltpu.make_async_copy(up, pre.at[2], load_sem.at[5]),
    ]
    for copy in loads:
        copy.start()

    barrier = pltpu.get_barrier_semaphore()
    for device in (y_dev, x_dev, core_dev):
        pl.semaphore_signal(barrier, inc=1, device_id=device, device_id_type=MESH)
    for way in (0, 1):
        @pl.when(position[way] < links - 1)
        def _():
            pl.semaphore_signal(barrier, inc=1, device_id=follower[way], device_id_type=MESH)
    inner = jnp.where((c > 0) & (c < links - 1), 5, 4)
    pl.semaphore_wait(barrier, inner)

    def ag_copy(way, o, j):
        return remote(
            wbuf.at[o, j], wbuf.at[o, j], z_sem.at[way], ag_sem.at[way, o, j], follower[way]
        )

    def rs_copy(way, src, t, j):
        return remote(
            src.at[t, j], rs[way].at[t, j], z_sem.at[way], rs_sem.at[way, t, j], follower[way]
        )

    def y_copy(j):
        return remote(
            cot.at[j, pl.ds(0, tokens)], cot.at[j, pl.ds(tokens, tokens)],
            ysend_sem.at[0], y_sem.at[j], y_dev,
        )

    loads[0].wait()
    loads[1].wait()

    def weights(j, _):
        at = lanes(j)
        wbuf[c, j, :, 0:LANES] = (wraw[0, :, at] * gs[:, at]).astype(BF)
        wbuf[c, j, :, LANES : 2 * LANES] = (wraw[1, :, at] * vs[:, at]).astype(BF)
        for way in (0, 1):
            @pl.when(position[way] < links - 1)
            def _():
                ag_copy(way, c, j).start()
        return 0

    lax.fori_loop(0, pieces, weights, 0)

    loads[2].wait()
    for o in range(links):
        for h in (0, 1):
            block = xin[:, (2 * o + h) * own : (2 * o + h + 1) * own]

            @pl.when(y == h)
            def _():
                xb[0, tp, :, o * own : (o + 1) * own] = block

            @pl.when(y != h)
            def _():
                xs[:, o * own : (o + 1) * own] = block

    xy = remote(xs, xb.at[1, tp], xsend_sem.at[0], xrecv_sem.at[0], y_dev)
    xy.start()
    xx0 = remote(xb.at[0, tp], xb.at[0, tp], xsend_sem.at[1], xrecv_sem.at[1], x_dev)
    xx0.start()
    xc0 = remote(xb.at[0, tp], xb.at[0, tp], xsend_sem.at[2], xrecv_sem.at[2], core_dev)
    xc0.start()

    for k in (3, 4, 5):
        loads[k].wait()

    row = lax.broadcasted_iota(jnp.int32, (tokens, LANES), 0)

    def down(a, k):
        return jnp.where(row >= k, pltpu.roll(a, k, 0), 0.0)

    def upward(a, k):
        return jnp.where(row < tokens - k, pltpu.roll(a, tokens - k, 0), 0.0)

    def elements(j, _):
        at = lanes(j)

        def shifted(i):
            a = pre[i, :, at].astype(F32)
            return down(a, 2), down(a, 1), a

        def conv(taps, a):
            return taps[0:1] * a[0] + taps[1:2] * a[1] + taps[2:3] * a[2]

        def back(taps, d):
            return (taps[2:3] * d + taps[1:2] * upward(d, 1) + taps[0:1] * upward(d, 2)).astype(BF)

        tg, tv = cg[:, at], cv[:, at]
        ga, va = shifted(0), shifted(1)
        g = conv(tg * gs[:, at], ga)
        v = conv(tv * vs[:, at], va)
        sig = 1.0 / (1.0 + jnp.exp(-g))
        base = pre[2, :, at].astype(F32) * sig
        d_gate = base * v * (1.0 + g * (1.0 - sig))
        d_value = base * g
        cot[j, 0:tokens, 0:LANES] = back(tg, d_gate)
        cot[j, 0:tokens, LANES : 2 * LANES] = back(tv, d_value)
        y_copy(j).start()
        for k in range(3):
            sown[k : k + 1, at] = jnp.sum(d_gate * ga[k], axis=0, keepdims=True)
            sown[3 + k : 4 + k, at] = jnp.sum(d_value * va[k], axis=0, keepdims=True)
        sown[6:8, at] = jnp.zeros((2, LANES), F32)
        return 0

    lax.fori_loop(0, pieces, elements, 0)

    sy = remote(sown, sfrom, ssend_sem.at[2], srecv_sem.at[2], y_dev)
    sy.start()

    xy.wait_recv()
    xx1 = remote(xb.at[1, tp], xb.at[1, tp], xsend_sem.at[3], xrecv_sem.at[3], x_dev)
    xx1.start()
    xc1 = remote(xb.at[1, tp], xb.at[1, tp], xsend_sem.at[4], xrecv_sem.at[4], core_dev)
    xc1.start()
    xx0.wait_recv()
    xc2 = remote(xb.at[0, x_tp], xb.at[0, x_tp], xsend_sem.at[5], xrecv_sem.at[5], core_dev)
    xc2.start()
    xx1.wait_recv()
    xc3 = remote(xb.at[1, x_tp], xb.at[1, x_tp], xsend_sem.at[6], xrecv_sem.at[6], core_dev)
    xc3.start()
    for copy in (xc0, xc1, xc2, xc3):
        copy.wait_recv()
    for q in (0, 1):
        for i in range(n_tp):
            for o in range(links):
                at = (q * n_tp + i) * rows
                xt[o, :, at : at + rows] = xb[q, i, :, o * own : (o + 1) * own].T

    def wait_y(j):
        y_copy(j).wait_recv()

    def partial(j):
        def one(o, _):
            part[o, j] = jnp.dot(xt[o], cot[j], preferred_element_type=F32).astype(BF)
            return 0

        lax.fori_loop(0, links, one, 0)

    table = segments(links, pieces)

    def decode(p, n):
        m = n - pieces * (p + 1)
        k, j = jnp.int32(0), jnp.int32(0)
        for first, tick, low, count in table[p]:
            q = lax.div(m - first, count)
            kk = low + (m - first) - q * count
            here = m >= first
            k = jnp.where(here, kk, k)
            j = jnp.where(here, tick + q - SKEW * kk, j)
        return k, j

    def relay(way, n):
        pos = position[way]

        @pl.when((pos < links - 1) & (n < pieces * (pos + 1)))
        def _():
            q = lax.div(n, pieces)
            j = n - q * pieces
            copy = ag_copy(way, real(way, pos - q), j)
            copy.wait_recv()
            copy.start()

        @pl.when((pos < links - 1) & (n >= pieces * (pos + 1)) & (n < slots))
        def _():
            k, j = decode(0, n)
            for p in range(1, links - 1):
                kp, jp = decode(p, n)
                k, j = jnp.where(pos == p, kp, k), jnp.where(pos == p, jp, j)
            t = real(way, links - 1 - k)

            @pl.when(pos == 0)
            def _():
                rs_copy(way, part, t, j).start()

            @pl.when(pos > 0)
            def _():
                rs_copy(way, part, t, j).wait_recv()
                rs[way][t, j] = (rs[way][t, j].astype(F32) + part[t, j].astype(F32)).astype(BF)
                rs_copy(way, rs[way], t, j).start()

    start = (5 * pieces) // 2

    def sum_copy(way):
        return remote(
            sput.at[way], sgot.at[way], ssend_sem.at[way], srecv_sem.at[way], follower[way]
        )

    def sums_step(way, n):
        pos = position[way]

        @pl.when((n == start + 1 + 2 * pos) & (pos < links - 1))
        def _():
            @pl.when(pos == 0)
            def _():
                sput[way] = spair[...]

            @pl.when(pos > 0)
            def _():
                sum_copy(way).wait_recv()
                sput[way] = spair[...] + sgot[way]

            sum_copy(way).start()

    dx_at = [start + 2 * p for p in range(links - 1)] + [(links - 1) * pieces + 3]
    order = [sorted(range(links), key=lambda o, a=a: (abs(o - a), o)) for a in range(links)]

    def block_at(n, shift):
        p_is = [n == at + shift for at in dx_at]
        o = jnp.int32(0)
        for a in range(links):
            for p in range(links):
                o = jnp.where(p_is[p] & (c == a), order[a][p], o)
        hit = p_is[0]
        for one in p_is[1:]:
            hit = hit | one
        return hit, o

    def core_copy(o):
        return remote(
            dxb.at[o, 1 - core], dx1.at[o], dsend_sem.at[0, o], drecv_sem.at[0, o], core_dev
        )

    def across_copy(o):
        return remote(
            ds1.at[o, 1 - xx], dx2.at[o], dsend_sem.at[1, o], drecv_sem.at[1, o], x_dev
        )

    def home_copy(o):
        return remote(
            ds2.at[o, 1], dx3.at[o], dsend_sem.at[2, o], drecv_sem.at[2, o], y_dev
        )

    first_late = len([n for n in range(slots) if pieces <= n <= start and _is_lead(table, pieces, n)])

    def dx_steps(n):
        hit, o = block_at(n, 0)

        @pl.when(hit)
        def _():
            for way in (0, 1):
                @pl.when((position[way] == links - 1) & (o != c))
                def _():
                    def one(j, _):
                        ag_copy(way, o, j).wait_recv()
                        return 0

                    lax.fori_loop(0, pieces, one, 0)

            acc[...] = ndot(cot[0], wbuf[o, 0])

            def one(j, _):
                acc[...] += ndot(cot[j], wbuf[o, j])
                return 0

            lax.fori_loop(1, pieces, one, 0)
            for q in (0, 1):
                for i in range(n_tp):
                    at = (q * n_tp + i) * rows
                    dxb[o, i % 2, i // 2, q] = acc[at : at + rows].astype(BF)
            core_copy(o).start()

        hit1, o1 = block_at(n, 1)

        @pl.when(hit1)
        def _():
            core_copy(o1).wait_recv()
            ds1[o1] = (dxb[o1, core].astype(F32) + dx1[o1].astype(F32)).astype(BF)
            across_copy(o1).start()

        hit2, o2 = block_at(n, 3)

        @pl.when(hit2)
        def _():
            across_copy(o2).wait_recv()
            ds2[o2] = (ds1[o2, xx].astype(F32) + dx2[o2].astype(F32)).astype(BF)
            home_copy(o2).start()

    def out_copy(j, k):
        dst = gwg if k == 0 else gwv
        return pltpu.make_async_copy(stage.at[j, k], dst.at[:, lanes(j)], out_sem.at[j, k])

    def final(j):
        fin[...] = part[c, j].astype(F32)
        for way in (0, 1):
            @pl.when(position[way] > 0)
            def _():
                rs_copy(way, part, c, j).wait_recv()
                fin[...] += rs[way][c, j].astype(F32)
        at = lanes(j)
        stage[j, 0] = fin[:, 0:LANES] * gs[:, at]
        stage[j, 1] = fin[:, LANES : 2 * LANES] * vs[:, at]
        for k in (0, 1):
            out_copy(j, k).start()

    wait_y(0)
    partial(0)
    last = (links - 1) * pieces + 3

    def slot(n, _):
        for way in (0, 1):
            relay(way, n)
            sums_step(way, n)

        @pl.when(n == start)
        def _():
            for late in range(first_late, pieces):
                wait_y(late)
            sy.wait_recv()
            spair[...] = sown[...] + sfrom[...]

        k, j = decode(0, n + 1)

        @pl.when((k == 0) & (n + 1 < slots))
        def _():
            @pl.when(n < start)
            def _():
                wait_y(j)

            partial(j)

        dx_steps(n)

        @pl.when(n >= last)
        def _():
            final(n - last)

        return 0

    lax.fori_loop(pieces, last + pieces, slot, 0)

    for o in range(links):
        home_copy(o).wait_recv()
        for h in (0, 1):
            at = (2 * o + h) * own

            @pl.when(y == h)
            def _():
                gi[:, at : at + own] = ds2[o, 0]

            @pl.when(y != h)
            def _():
                gi[:, at : at + own] = dx3[o]

    for way in (0, 1):
        @pl.when(position[way] == links - 1)
        def _():
            sum_copy(way).wait_recv()

        @pl.when(position[way] > 0)
        def _():
            spair[...] += sgot[way]

    total = spair[...]
    ggs[...] = jnp.sum(cg[...] * total[0:3], axis=0, keepdims=True)
    gvs[...] = jnp.sum(cv[...] * total[3:6], axis=0, keepdims=True)
    gcg[...] = total[0:3] * gs[...]
    gcv[...] = total[3:6] * vs[...]

    for j in range(pieces):
        for k in (0, 1):
            out_copy(j, k).wait()
    for copy in (xy, xx0, xc0, xx1, xc1, xc2, xc3, sy):
        copy.wait_send()
    for o in range(links):
        core_copy(o).wait_send()
        across_copy(o).wait_send()
        home_copy(o).wait_send()
    for way in (0, 1):
        @pl.when(position[way] < links - 1)
        def _():
            sum_copy(way).wait_send()
            remote(wbuf, wbuf, z_sem.at[way], ag_sem.at[way, 0, 0], follower[way]).wait_send()
    mine = cot.at[:, pl.ds(0, tokens)]
    remote(mine, mine, ysend_sem.at[0], y_sem.at[0], y_dev).wait_send()


def _is_lead(table, pieces, n):
    m = n - pieces
    k = None
    for first, tick, low, count in table[0]:
        if m >= first:
            k = low + (m - first) % count
    return k == 0


def whole_kernel(n_fs, n_tp):
    links = n_fs // 2

    def on_device(inputs, w_gate, w_value, gate_scale, value_scale, conv_gate, conv_value,
                  gate_pre, value_pre, grad_out):
        rows, depth = inputs.shape
        own, columns = w_gate.shape
        tokens = gate_pre.shape[0]
        half = depth // 2
        pieces = columns // LANES
        anywhere = pl.BlockSpec(memory_space=pl.ANY)
        vmem = pl.BlockSpec(memory_space=pltpu.VMEM)
        dma, vm = pltpu.SemaphoreType.DMA, pltpu.VMEM
        wide = 2 * LANES
        outs = pl.pallas_call(
            functools.partial(fused, (n_fs, n_tp)),
            in_specs=[anywhere] * 3 + [vmem] * 4 + [anywhere] * 3,
            out_specs=[vmem] + [anywhere] * 2 + [vmem] * 4,
            out_shape=[
                jax.ShapeDtypeStruct((rows, depth), BF),
                jax.ShapeDtypeStruct((own, columns), F32),
                jax.ShapeDtypeStruct((own, columns), F32),
                jax.ShapeDtypeStruct((1, columns), F32),
                jax.ShapeDtypeStruct((1, columns), F32),
                jax.ShapeDtypeStruct((3, columns), F32),
                jax.ShapeDtypeStruct((3, columns), F32),
            ],
            scratch_shapes=[
                vm((2, own, columns), F32),
                vm((3, tokens, columns), BF),
                vm((links, pieces, own, wide), BF),
                vm((pieces, 2 * tokens, wide), BF),
                vm((links, pieces, own, wide), BF),
                vm((links, pieces, own, wide), BF),
                vm((links, pieces, own, wide), BF),
                vm((rows, depth), BF),
                vm((rows, half), BF),
                vm((2, n_tp, rows, half), BF),
                vm((links, own, 2 * tokens), BF),
                vm((2 * tokens, own), F32),
                vm((links, 2, 2, 2, rows, own), BF),
                vm((links, 2, 2, rows, own), BF),
                vm((links, 2, 2, rows, own), BF),
                vm((links, 2, rows, own), BF),
                vm((links, 2, rows, own), BF),
                vm((links, rows, own), BF),
                vm((pieces, 2, own, LANES), F32),
                vm((own, wide), F32),
                vm((8, columns), F32),
                vm((8, columns), F32),
                vm((8, columns), F32),
                vm((2, 8, columns), F32),
                vm((2, 8, columns), F32),
                dma((6,)),
                dma((2, links, pieces)),
                dma((2, links, pieces)),
                dma((2,)),
                dma((pieces,)),
                dma((1,)),
                dma((7,)),
                dma((7,)),
                dma((3, links)),
                dma((3, links)),
                dma((3,)),
                dma((3,)),
                dma((pieces, 2)),
            ],
            compiler_params=pltpu.CompilerParams(
                collective_id=0, has_side_effects=True, vmem_limit_bytes=60 * 2**20
            ),
        )(
            inputs, w_gate, w_value, gate_scale[None], value_scale[None], conv_gate, conv_value,
            gate_pre, value_pre, grad_out,
        )
        gi, gwg, gwv, ggs, gvs, gcg, gcv = outs
        return gi, gwg, gwv, ggs[0], gvs[0], gcg, gcv

    return on_device


def solution(mesh):
    placed = (
        P(("fs", "tp"), None),
        P("fs", "tp"),
        P("fs", "tp"),
        P("tp"),
        P("tp"),
        P(None, "tp"),
        P(None, "tp"),
        P("fs", "tp"),
        P("fs", "tp"),
        P("fs", "tp"),
    )
    body = make(mesh.shape["fs"], mesh.shape["tp"])

    given = (
        P(("fs", "tp"), None),
        P("fs", "tp"),
        P("fs", "tp"),
        P("tp"),
        P("tp"),
        P(None, "tp"),
        P(None, "tp"),
    )

    def spread(one):
        return jax.shard_map(one, mesh=mesh, in_specs=placed, out_specs=given, check_vma=False)

    step = spread(body)
    general = step
    n_fs, n_tp = mesh.shape["fs"], mesh.shape["tp"]
    fast = spread(whole_kernel(n_fs, n_tp))

    def pick(*args):
        columns = args[1].shape[1] // n_tp
        if n_tp == 4 and 2 < n_fs // 2 <= 4 and columns % LANES == 0:
            return fast(*args)
        return general(*args)

    return pick
```

```python
import functools

import jax
import jax.numpy as jnp
from jax import lax
from jax.experimental import pallas as pl
from jax.experimental.pallas import tpu as pltpu
from jax.sharding import PartitionSpec as P


BF = jnp.bfloat16
F32 = jnp.float32


LANES = 128


def elementwise(gs_ref, vs_ref, cg_ref, cv_ref, g_ref, v_ref, up_ref, gc_ref, vc_ref, s_ref):
    tokens = g_ref.shape[0]
    row = lax.broadcasted_iota(jnp.int32, g_ref.shape, 0)

    def down(x, k):
        return jnp.where(row >= k, pltpu.roll(x, k, 0), 0.0)

    def up(x, k):
        return jnp.where(row < tokens - k, pltpu.roll(x, tokens - k, 0), 0.0)

    def shifted(ref):
        x = ref[...].astype(F32)
        return down(x, 2), down(x, 1), x

    def conv(taps, xs):
        return taps[0:1] * xs[0] + taps[1:2] * xs[1] + taps[2:3] * xs[2]

    def back(taps, d):
        return (taps[2:3] * d + taps[1:2] * up(d, 1) + taps[0:1] * up(d, 2)).astype(BF)

    gs, vs = shifted(g_ref), shifted(v_ref)
    g = conv(cg_ref[...] * gs_ref[...], gs)
    v = conv(cv_ref[...] * vs_ref[...], vs)
    sig = 1.0 / (1.0 + jnp.exp(-g))
    base = up_ref[...].astype(F32) * sig
    d_gate = base * v * (1.0 + g * (1.0 - sig))
    d_value = base * g
    for j in range(3):
        s_ref[j : j + 1] = jnp.sum(d_gate * gs[j], axis=0, keepdims=True)
        s_ref[3 + j : 4 + j] = jnp.sum(d_value * vs[j], axis=0, keepdims=True)
    s_ref[6:8] = jnp.zeros((2, g_ref.shape[1]), F32)
    gc_ref[...] = back(cg_ref[...], d_gate)
    vc_ref[...] = back(cv_ref[...], d_value)


def cotangents(gs, vs, cg, cv, g, v, up):
    tokens, columns = g.shape
    big = pl.BlockSpec((tokens, LANES), lambda i: (0, i))

    def small(n):
        return pl.BlockSpec((n, LANES), lambda i: (0, i))

    return pl.pallas_call(
        elementwise,
        grid=(pl.cdiv(columns, LANES),),
        in_specs=[small(1), small(1), small(3), small(3), big, big, big],
        out_specs=[big, big, small(8)],
        out_shape=[jax.ShapeDtypeStruct(g.shape, BF)] * 2
        + [jax.ShapeDtypeStruct((8, columns), F32)],
        compiler_params=pltpu.CompilerParams(vmem_limit_bytes=24 * 2**20),
        cost_estimate=pl.CostEstimate(
            flops=g.size * 400, bytes_accessed=g.size * 10, transcendentals=g.size
        ),
    )(gs[None], vs[None], cg, cv, g, v, up)


def rescale(gs_ref, vs_ref, g_ref, v_ref, out_ref):
    out_ref[0] = (g_ref[...] * gs_ref[...]).astype(BF)
    out_ref[1] = (v_ref[...] * vs_ref[...]).astype(BF)


def scaled_weights(gs, vs, g, v):
    own, columns = g.shape
    parts = 4
    block = pl.BlockSpec((own // parts, columns), lambda i: (i, 0))
    scale = pl.BlockSpec((1, columns), lambda i: (0, 0))
    return pl.pallas_call(
        rescale,
        grid=(parts,),
        in_specs=[scale, scale, block, block],
        out_specs=pl.BlockSpec((2, own // parts, columns), lambda i: (0, i, 0)),
        out_shape=jax.ShapeDtypeStruct((2, own, columns), BF),
        compiler_params=pltpu.CompilerParams(vmem_limit_bytes=24 * 2**20),
        cost_estimate=pl.CostEstimate(
            flops=g.size * 100, bytes_accessed=g.size * 12, transcendentals=0
        ),
    )(gs[None], vs[None], g, v)


def tdot(a, b):
    return lax.dot_general(a, b, (((0,), (0,)), ((), ())), preferred_element_type=F32)


def ndot(a, b):
    return lax.dot_general(a, b, (((1,), (1,)), ((), ())), preferred_element_type=F32)


def make(n_fs, n_tp):
    links = n_fs // 2

    def on_device(
        inputs,
        w_gate,
        w_value,
        gate_scale,
        value_scale,
        conv_gate,
        conv_value,
        gate_pre,
        value_pre,
        grad_out,
    ):
        fs = lax.axis_index("fs")
        tp = lax.axis_index("tp")
        c, y = fs // 2, fs % 2
        rows, depth = inputs.shape
        own = w_gate.shape[0]
        half = depth // 2
        tokens, columns = gate_pre.shape

        def swap(x, axis, bit, n):
            return lax.ppermute(x, axis, [(i, i ^ bit) for i in range(n)])

        def chain(x, right, senders):
            step = 1 if right else -1
            pairs = [(2 * s + j, 2 * (s + step) + j) for s in senders for j in (0, 1)]
            return lax.ppermute(x, "fs", pairs)

        stacked = scaled_weights(gate_scale, value_scale, w_gate, w_value)
        rights, lefts = [], []
        r = l = stacked
        for s in range(links - 1):
            r = chain(r, True, range(s, links - 1))
            l = chain(l, False, range(1, links - s))
            rights.append(r)
            lefts.append(l)

        by_half = inputs.reshape(rows, links, 2, own)
        mine = lax.dynamic_index_in_dim(by_half, y, 2, keepdims=False)
        other = lax.dynamic_index_in_dim(by_half, 1 - y, 2, keepdims=False)
        mine, other = mine.reshape(rows, half), other.reshape(rows, half)
        other = swap(other, "fs", 1, n_fs)
        x = jnp.stack([mine, other])[:, None]
        bit = n_tp // 2
        while bit:
            got = swap(x, "tp", bit, n_tp)
            high = (tp // bit) % 2 == 1
            x = jnp.where(high, jnp.stack([got, x], 2), jnp.stack([x, got], 2))
            x = x.reshape(2, -1, rows, half)
            bit //= 2
        x = x.reshape(2, tokens, half)

        gate_cot, value_cot, sums = cotangents(
            gate_scale, value_scale, conv_gate, conv_value, gate_pre, value_pre, grad_out
        )
        bit = n_fs // 2
        while bit:
            sums = sums + swap(sums, "fs", bit, n_fs)
            bit //= 2

        gate_theirs = swap(gate_cot, "fs", 1, n_fs)
        value_theirs = swap(value_cot, "fs", 1, n_fs)
        pair = [(gate_cot, gate_theirs), (value_cot, value_theirs)]

        def at(blocks, i):
            return lax.dynamic_index_in_dim(
                blocks, jnp.clip(i, 0, links - 1), 0, keepdims=False
            )

        def collect(parts):
            r = l = None
            for t in range(links - 1):
                send_r = at(parts, links - 1 - t + c)
                send_l = at(parts, c - (links - 1 - t) + 0)
                if t:
                    send_r = (send_r.astype(F32) + r.astype(F32)).astype(BF)
                    send_l = (send_l.astype(F32) + l.astype(F32)).astype(BF)
                r = chain(send_r, True, range(0, t + 1))
                l = chain(send_l, False, range(links - 1 - t, links))
            total = at(parts, c).astype(F32)
            if r is not None:
                total = total + r.astype(F32) + l.astype(F32)
            return total

        grads = []
        for (cot, theirs), scale in zip(pair, (gate_scale, value_scale)):
            first = tdot(x[0], cot)
            parts = (first + tdot(x[1], theirs)).astype(BF)
            blocks = parts.reshape(links, own, columns)
            grads.append(collect(blocks) * scale)

        blocks = [stacked]
        for s in range(links - 1):
            blocks.append(jnp.where(c > s, rights[s], lefts[links - 2 - s]))
        columns_of = []
        for block in blocks:
            columns_of.append(
                [
                    (ndot(g, block[0]) + ndot(v, block[1])).astype(BF)
                    for g, v in zip(pair[0], pair[1])
                ]
            )
        part = jnp.stack([jnp.concatenate(t, 1) for t in zip(*columns_of)])
        part = part.reshape(2, n_tp, rows, half)
        bit = 1
        while bit < n_tp:
            split = part.reshape(2, -1, 2, rows, half)
            which = (tp // bit) % 2
            keep = lax.dynamic_index_in_dim(split, which, 2, keepdims=False)
            send = lax.dynamic_index_in_dim(split, 1 - which, 2, keepdims=False)
            got = swap(send, "tp", bit, n_tp)
            part = (keep.astype(F32) + got.astype(F32)).astype(BF)
            bit *= 2
        mine = part.reshape(2, rows, half)[0]
        other = swap(part.reshape(2, rows, half)[1], "fs", 1, n_fs)
        both = jnp.where(
            y == 0, jnp.stack([mine, other], 1), jnp.stack([other, mine], 1)
        ).reshape(rows, 2, links, own)
        order = (c - jnp.arange(links)) % links
        grad_inputs = jnp.take(both, order, axis=2).transpose(0, 2, 1, 3)
        return (
            grad_inputs.reshape(rows, depth),
            grads[0],
            grads[1],
            jnp.sum(conv_gate * sums[0:3], axis=0),
            jnp.sum(conv_value * sums[3:6], axis=0),
            sums[0:3] * gate_scale,
            sums[3:6] * value_scale,
        )

    return on_device


MESH = pl.DeviceIdType.MESH
SKEW = 2


def segments(links, pieces):
    table = []
    for pos in range(links - 1):
        reach = links - 1 - pos
        rows, count, last = [], 0, None
        for tick in range(pieces + SKEW * (reach - 1)):
            live = [k for k in range(reach) if 0 <= tick - SKEW * k < pieces]
            key = (live[0], len(live)) if live else None
            if key and key != last:
                rows.append((count, tick, live[0], len(live)))
            last = key
            count += len(live)
        table.append(rows)
    return table


def fused(dims, *refs):
    n_fs, n_tp = dims
    (
        inp, wg, wv, gs_in, vs_in, cg_in, cv_in, gp, vp, up,
        gi, gw, small,
        wraw, pre, wbuf, cot, part, rs0, rs1, xin, xs, xb, xt,
        acc, dxb, dx1, ds1, dx2, ds2, dx3, gs1, vs1, gs, vs, cg, cv, fin, sown, spair, sfrom, sgot, sput,
        load_sem, hop_sem, z_sem, y_sem, ysend_sem, xsend_sem, xrecv_sem,
        dsend_sem, drecv_sem, ssend_sem, srecv_sem,
    ) = refs
    rs = (rs0, rs1)
    links = n_fs // 2
    pieces = cot.shape[0]
    own = wg.shape[0]
    rows, _ = inp.shape
    tokens = gp.shape[0]
    slots = links * pieces

    fs = lax.axis_index("fs")
    tp = lax.axis_index("tp")
    c, y = lax.div(fs, 2), lax.rem(fs, 2)
    xx, core = lax.div(tp, 2), lax.rem(tp, 2)
    y_dev = (fs + 1 - 2 * y, tp)
    x_dev = (fs, tp + 2 - 4 * xx)
    core_dev = (fs, tp + 1 - 2 * core)
    x_tp = tp + 2 - 4 * xx
    position = (c, links - 1 - c)
    follower = ((fs + 2, tp), (fs - 2, tp))

    def real(way, index):
        return index if way == 0 else links - 1 - index

    def remote(src, dst, send, recv, device):
        return pltpu.make_async_remote_copy(
            src_ref=src, dst_ref=dst, send_sem=send, recv_sem=recv,
            device_id=device, device_id_type=MESH,
        )

    def lanes(j):
        return pl.ds(pl.multiple_of(j * LANES, LANES), LANES)

    def load(src, dst, k):
        copy = pltpu.make_async_copy(src, dst, load_sem.at[k])
        copy.start()
        return copy

    def loaded(ref, k):
        pltpu.make_async_copy(ref, ref, load_sem.at[k]).wait()

    head, rest = pl.ds(0, LANES), pl.ds(LANES, (pieces - 1) * LANES)
    scales = [load(gs_in, gs1, 4), load(vs_in, vs1, 5)]
    for at, k in ((head, 0), (rest, 1)):
        for i, w in enumerate((wg, wv)):
            load(w.at[:, at], wraw.at[i, :, at], k)
    load(inp, xin, 2)
    for i, a in enumerate((gp, vp, up)):
        load(a, pre.at[i], 3)
    taps = [load(cg_in, cg, 6), load(cv_in, cv, 7)]

    barrier = pltpu.get_barrier_semaphore()
    for device in (y_dev, x_dev, core_dev):
        pl.semaphore_signal(barrier, inc=1, device_id=device, device_id_type=MESH)
    for way in (0, 1):
        @pl.when(position[way] < links - 1)
        def _():
            pl.semaphore_signal(barrier, inc=1, device_id=follower[way], device_id_type=MESH)
    inner = jnp.where((c > 0) & (c < links - 1), 5, 4)
    pl.semaphore_wait(barrier, inner)

    def ag_copy(way, o, j):
        return remote(
            wbuf.at[o, j], wbuf.at[o, j], z_sem.at[way], hop_sem.at[way, o, j], follower[way]
        )

    def rs_copy(way, src, t, j):
        return remote(
            src.at[t, j], rs[way].at[t, j], z_sem.at[way], hop_sem.at[way, t, j], follower[way]
        )

    def y_copy(j):
        return remote(
            cot.at[j, pl.ds(0, tokens)], cot.at[j, pl.ds(tokens, tokens)],
            ysend_sem.at[0], y_sem.at[j], y_dev,
        )

    for copy in scales:
        copy.wait()
    gs[...] = gs1[...].reshape(gs.shape)
    vs[...] = vs1[...].reshape(vs.shape)
    loaded(wraw.at[:, :, head], 0)

    def weights(j, _):
        at = lanes(j)
        wbuf[c, j, :, 0:LANES] = (wraw[0, :, at] * gs[:, at]).astype(BF)
        wbuf[c, j, :, LANES : 2 * LANES] = (wraw[1, :, at] * vs[:, at]).astype(BF)
        for way in (0, 1):
            @pl.when(position[way] < links - 1)
            def _():
                ag_copy(way, c, j).start()
        return 0

    weights(0, 0)
    loaded(wraw.at[:, :, rest], 1)
    lax.fori_loop(1, pieces, weights, 0)

    loaded(xin, 2)
    for o in range(links):
        for h in (0, 1):
            block = xin[:, (2 * o + h) * own : (2 * o + h + 1) * own]

            @pl.when(y == h)
            def _():
                xb[tp, :, o * own : (o + 1) * own] = block

            @pl.when(y != h)
            def _():
                xs[:, o * own : (o + 1) * own] = block

    xy = remote(xs, xb.at[n_tp + tp], xsend_sem.at[0], xrecv_sem.at[0], y_dev)
    xy.start()
    xx0 = remote(xb.at[tp], xb.at[tp], xsend_sem.at[0], xrecv_sem.at[1], x_dev)
    xx0.start()
    xc0 = remote(xb.at[tp], xb.at[tp], xsend_sem.at[0], xrecv_sem.at[2], core_dev)
    xc0.start()

    loaded(pre, 3)
    for copy in taps:
        copy.wait()

    row = lax.broadcasted_iota(jnp.int32, (tokens, LANES), 0)

    def down(a, k):
        return jnp.where(row >= k, pltpu.roll(a, k, 0), 0.0)

    def upward(a, k):
        return jnp.where(row < tokens - k, pltpu.roll(a, tokens - k, 0), 0.0)

    def elements(j, _):
        at = lanes(j)

        def shifted(i):
            a = pre[i, :, at].astype(F32)
            return down(a, 2), down(a, 1), a

        def conv(taps, a):
            return taps[0:1] * a[0] + taps[1:2] * a[1] + taps[2:3] * a[2]

        def back(taps, d):
            return (taps[2:3] * d + taps[1:2] * upward(d, 1) + taps[0:1] * upward(d, 2)).astype(BF)

        tg, tv = cg[:, at], cv[:, at]
        ga, va = shifted(0), shifted(1)
        g = conv(tg * gs[:, at], ga)
        v = conv(tv * vs[:, at], va)
        sig = 1.0 / (1.0 + jnp.exp(-g))
        base = pre[2, :, at].astype(F32) * sig
        d_gate = base * v * (1.0 + g * (1.0 - sig))
        d_value = base * g
        cot[j, 0:tokens, 0:LANES] = back(tg, d_gate)
        cot[j, 0:tokens, LANES : 2 * LANES] = back(tv, d_value)
        y_copy(j).start()
        for k in range(3):
            sown[k : k + 1, at] = jnp.sum(d_gate * ga[k], axis=0, keepdims=True)
            sown[3 + k : 4 + k, at] = jnp.sum(d_value * va[k], axis=0, keepdims=True)
        sown[6:8, at] = jnp.zeros((2, LANES), F32)
        return 0

    lax.fori_loop(0, pieces, elements, 0)

    sy = remote(sown, sfrom, ssend_sem.at[2], srecv_sem.at[2], y_dev)
    sy.start()

    xy.wait_recv()
    xx1 = remote(xb.at[n_tp + tp], xb.at[n_tp + tp], xsend_sem.at[0], xrecv_sem.at[3], x_dev)
    xx1.start()
    xc1 = remote(xb.at[n_tp + tp], xb.at[n_tp + tp], xsend_sem.at[0], xrecv_sem.at[4], core_dev)
    xc1.start()
    xx0.wait_recv()
    xc2 = remote(xb.at[x_tp], xb.at[x_tp], xsend_sem.at[0], xrecv_sem.at[5], core_dev)
    xc2.start()
    xx1.wait_recv()
    xc3 = remote(xb.at[n_tp + x_tp], xb.at[n_tp + x_tp], xsend_sem.at[0], xrecv_sem.at[6], core_dev)
    xc3.start()
    for copy in (xc0, xc1, xc2, xc3):
        copy.wait_recv()
    for q in (0, 1):
        for i in range(n_tp):
            for o in range(links):
                at = (q * n_tp + i) * rows
                xt[o, :, at : at + rows] = xb[q * n_tp + i, :, o * own : (o + 1) * own].T

    def wait_y(j):
        y_copy(j).wait_recv()

    def partial(j):
        def one(o, _):
            part[o, j] = jnp.dot(xt[o], cot[j], preferred_element_type=F32).astype(BF)
            return 0

        lax.fori_loop(0, links, one, 0)

    table = segments(links, pieces)

    def decode(p, n):
        m = n - pieces * (p + 1)
        k, j = jnp.int32(0), jnp.int32(0)
        for first, tick, low, count in table[p]:
            q = lax.div(m - first, count)
            kk = low + (m - first) - q * count
            here = m >= first
            k = jnp.where(here, kk, k)
            j = jnp.where(here, tick + q - SKEW * kk, j)
        return k, j

    def relay(way, n):
        pos = position[way]

        @pl.when((pos < links - 1) & (n < pieces * (pos + 1)))
        def _():
            q = lax.div(n, pieces)
            j = n - q * pieces
            copy = ag_copy(way, real(way, pos - q), j)
            copy.wait_recv()
            copy.start()

        @pl.when((pos < links - 1) & (n >= pieces * (pos + 1)) & (n < slots))
        def _():
            k, j = decode(0, n)
            for p in range(1, links - 1):
                kp, jp = decode(p, n)
                k, j = jnp.where(pos == p, kp, k), jnp.where(pos == p, jp, j)
            t = real(way, links - 1 - k)

            @pl.when(pos == 0)
            def _():
                rs_copy(way, part, t, j).start()

            @pl.when(pos > 0)
            def _():
                rs_copy(way, part, t, j).wait_recv()
                rs[way][t, j] = (rs[way][t, j].astype(F32) + part[t, j].astype(F32)).astype(BF)
                rs_copy(way, rs[way], t, j).start()

    start = (5 * pieces) // 2

    def sum_copy(way):
        return remote(
            sput.at[way], sgot.at[way], ssend_sem.at[way], srecv_sem.at[way], follower[way]
        )

    def sums_step(way, n):
        pos = position[way]

        @pl.when((n == start + 1 + 2 * pos) & (pos < links - 1))
        def _():
            @pl.when(pos == 0)
            def _():
                sput[way] = spair[...]

            @pl.when(pos > 0)
            def _():
                sum_copy(way).wait_recv()
                sput[way] = spair[...] + sgot[way]

            sum_copy(way).start()

    dx_at = [start + 2 * p for p in range(links - 1)] + [(links - 1) * pieces + 3]
    order = [sorted(range(links), key=lambda o, a=a: (abs(o - a), o)) for a in range(links)]

    def block_at(n, shift):
        p_is = [n == at + shift for at in dx_at]
        o = jnp.int32(0)
        for a in range(links):
            for p in range(links):
                o = jnp.where(p_is[p] & (c == a), order[a][p], o)
        hit = p_is[0]
        for one in p_is[1:]:
            hit = hit | one
        return hit, o

    def core_copy(o):
        return remote(
            dxb.at[o, 1 - core], dx1.at[o], dsend_sem.at[0], drecv_sem.at[0, o], core_dev
        )

    def across_copy(o):
        return remote(
            ds1.at[o, 1 - xx], dx2.at[o], dsend_sem.at[1], drecv_sem.at[1, o], x_dev
        )

    def home_copy(o):
        return remote(
            ds2.at[o, 1], dx3.at[o], dsend_sem.at[2], drecv_sem.at[2, o], y_dev
        )

    first_late = len([n for n in range(slots) if pieces <= n <= start and _is_lead(table, pieces, n)])

    def dx_steps(n):
        hit, o = block_at(n, 0)

        @pl.when(hit)
        def _():
            for way in (0, 1):
                @pl.when((position[way] == links - 1) & (o != c))
                def _():
                    def one(j, _):
                        ag_copy(way, o, j).wait_recv()
                        return 0

                    lax.fori_loop(0, pieces, one, 0)

            acc[...] = ndot(cot[0], wbuf[o, 0])

            def one(j, _):
                acc[...] += ndot(cot[j], wbuf[o, j])
                return 0

            lax.fori_loop(1, pieces, one, 0)
            for q in (0, 1):
                for i in range(n_tp):
                    at = (q * n_tp + i) * rows
                    dxb[o, i % 2, i // 2, q] = acc[at : at + rows].astype(BF)
            core_copy(o).start()

        hit1, o1 = block_at(n, 1)

        @pl.when(hit1)
        def _():
            core_copy(o1).wait_recv()
            ds1[o1] = (dxb[o1, core].astype(F32) + dx1[o1].astype(F32)).astype(BF)
            across_copy(o1).start()

        hit2, o2 = block_at(n, 3)

        @pl.when(hit2)
        def _():
            across_copy(o2).wait_recv()
            ds2[o2] = (ds1[o2, xx].astype(F32) + dx2[o2].astype(F32)).astype(BF)
            home_copy(o2).start()

    def final(j):
        fin[...] = part[c, j].astype(F32)
        for way in (0, 1):
            @pl.when(position[way] > 0)
            def _():
                rs_copy(way, part, c, j).wait_recv()
                fin[...] += rs[way][c, j].astype(F32)
        at = lanes(j)
        gw[0, :, at] = fin[:, 0:LANES] * gs[:, at]
        gw[1, :, at] = fin[:, LANES : 2 * LANES] * vs[:, at]

    def results():
        for o in range(links):
            home_copy(o).wait_recv()
            for h in (0, 1):
                at = (2 * o + h) * own

                @pl.when(y == h)
                def _():
                    gi[:, at : at + own] = ds2[o, 0]

                @pl.when(y != h)
                def _():
                    gi[:, at : at + own] = dx3[o]

        for way in (0, 1):
            @pl.when(position[way] == links - 1)
            def _():
                sum_copy(way).wait_recv()

            @pl.when(position[way] > 0)
            def _():
                spair[...] += sgot[way]

        total = spair[...]
        small[0:3] = total[0:3] * gs[...]
        small[3:6] = total[3:6] * vs[...]
        small[6:7] = jnp.sum(cg[...] * total[0:3], axis=0, keepdims=True)
        small[7:8] = jnp.sum(cv[...] * total[3:6], axis=0, keepdims=True)

    wait_y(0)
    partial(0)
    last = (links - 1) * pieces + 3

    def slot(n, _):
        for way in (0, 1):
            relay(way, n)
            sums_step(way, n)

        @pl.when(n == start)
        def _():
            for late in range(first_late, pieces):
                wait_y(late)
            sy.wait_recv()
            spair[...] = sown[...] + sfrom[...]

        k, j = decode(0, n + 1)

        @pl.when((k == 0) & (n + 1 < slots))
        def _():
            @pl.when(n < start)
            def _():
                wait_y(j)

            partial(j)

        dx_steps(n)

        @pl.when(n >= last)
        def _():
            final(n - last)

        @pl.when(n == last + pieces - 3)
        def _():
            results()

        return 0

    lax.fori_loop(pieces, last + pieces, slot, 0)

    seven = xb.at[pl.ds(0, 7)]
    remote(seven, seven, xsend_sem.at[0], xrecv_sem.at[0], x_dev).wait_send()
    sy.wait_send()
    for ref, k in ((dx1, 0), (ds1.at[:, 0], 1), (dx3, 2)):
        remote(ref, ref, dsend_sem.at[k], drecv_sem.at[k, 0], y_dev).wait_send()
    for way in (0, 1):
        @pl.when(position[way] < links - 1)
        def _():
            sum_copy(way).wait_send()
            remote(wbuf, wbuf, z_sem.at[way], hop_sem.at[way, 0, 0], follower[way]).wait_send()
    mine = cot.at[:, pl.ds(0, tokens)]
    remote(mine, mine, ysend_sem.at[0], y_sem.at[0], y_dev).wait_send()


def _is_lead(table, pieces, n):
    m = n - pieces
    k = None
    for first, tick, low, count in table[0]:
        if m >= first:
            k = low + (m - first) % count
    return k == 0


def deliver(gi_in, gw_in, small, *refs):
    gi, gwg, gwv, ggs, gvs, gcg, gcv, sg, sv, tg, tv, sem = refs
    copies = [
        pltpu.make_async_copy(gw_in.at[0], gwg, sem.at[0]),
        pltpu.make_async_copy(gw_in.at[1], gwv, sem.at[1]),
        pltpu.make_async_copy(gi_in, gi, sem.at[2]),
    ]
    for copy in copies:
        copy.start()
    tg[...] = small[0:3]
    tv[...] = small[3:6]
    sg[...] = small[6:7].reshape(sg.shape)
    sv[...] = small[7:8].reshape(sv.shape)
    for k, (src, dst) in enumerate(((tg, gcg), (tv, gcv), (sg, ggs), (sv, gvs))):
        copies.append(pltpu.make_async_copy(src, dst, sem.at[3 + k]))
        copies[-1].start()
    for copy in copies:
        copy.wait()


def whole_kernel(n_fs, n_tp):
    links = n_fs // 2

    def on_device(inputs, w_gate, w_value, gate_scale, value_scale, conv_gate, conv_value,
                  gate_pre, value_pre, grad_out):
        rows, depth = inputs.shape
        own, columns = w_gate.shape
        tokens = gate_pre.shape[0]
        half = depth // 2
        pieces = columns // LANES
        anywhere = pl.BlockSpec(memory_space=pl.ANY)
        vmem = pl.BlockSpec(memory_space=pltpu.VMEM)
        dma, vm = pltpu.SemaphoreType.DMA, pltpu.VMEM
        wide = 2 * LANES
        outs = pl.pallas_call(
            functools.partial(fused, (n_fs, n_tp)),
            in_specs=[anywhere] * 10,
            out_specs=[vmem] * 3,
            out_shape=[
                vm((rows, depth), BF),
                vm((2, own, columns), F32),
                vm((8, columns), F32),
            ],
            scratch_shapes=[
                vm((2, own, columns), F32),
                vm((3, tokens, columns), BF),
                vm((links, pieces, own, wide), BF),
                vm((pieces, 2 * tokens, wide), BF),
                vm((links, pieces, own, wide), BF),
                vm((links, pieces, own, wide), BF),
                vm((links, pieces, own, wide), BF),
                vm((rows, depth), BF),
                vm((rows, half), BF),
                vm((2 * n_tp, rows, half), BF),
                vm((links, own, 2 * tokens), BF),
                vm((2 * tokens, own), F32),
                vm((links, 2, 2, 2, rows, own), BF),
                vm((links, 2, 2, rows, own), BF),
                vm((links, 2, 2, rows, own), BF),
                vm((links, 2, rows, own), BF),
                vm((links, 2, rows, own), BF),
                vm((links, rows, own), BF),
                vm((columns,), F32),
                vm((columns,), F32),
                vm((1, columns), F32),
                vm((1, columns), F32),
                vm((3, columns), F32),
                vm((3, columns), F32),
                vm((own, wide), F32),
                vm((8, columns), F32),
                vm((8, columns), F32),
                vm((8, columns), F32),
                vm((2, 8, columns), F32),
                vm((2, 8, columns), F32),
                dma((8,)),
                dma((2, links, pieces)),
                dma((2,)),
                dma((pieces,)),
                dma((1,)),
                dma((1,)),
                dma((7,)),
                dma((3,)),
                dma((3, links)),
                dma((3,)),
                dma((3,)),
            ],
            compiler_params=pltpu.CompilerParams(
                collective_id=0, has_side_effects=True, vmem_limit_bytes=52 * 2**20
            ),
        )(
            inputs, w_gate, w_value, gate_scale, value_scale, conv_gate, conv_value,
            gate_pre, value_pre, grad_out,
        )
        return pl.pallas_call(
            deliver,
            in_specs=[vmem] * 3,
            out_specs=[anywhere] * 7,
            out_shape=[
                jax.ShapeDtypeStruct((rows, depth), BF),
                jax.ShapeDtypeStruct((own, columns), F32),
                jax.ShapeDtypeStruct((own, columns), F32),
                jax.ShapeDtypeStruct((columns,), F32),
                jax.ShapeDtypeStruct((columns,), F32),
                jax.ShapeDtypeStruct((3, columns), F32),
                jax.ShapeDtypeStruct((3, columns), F32),
            ],
            scratch_shapes=[
                vm((columns,), F32),
                vm((columns,), F32),
                vm((3, columns), F32),
                vm((3, columns), F32),
                dma((7,)),
            ],
            compiler_params=pltpu.CompilerParams(vmem_limit_bytes=2 * 2**20),
        )(*outs)

    return on_device


def solution(mesh):
    placed = (
        P(("fs", "tp"), None),
        P("fs", "tp"),
        P("fs", "tp"),
        P("tp"),
        P("tp"),
        P(None, "tp"),
        P(None, "tp"),
        P("fs", "tp"),
        P("fs", "tp"),
        P("fs", "tp"),
    )
    body = make(mesh.shape["fs"], mesh.shape["tp"])

    given = (
        P(("fs", "tp"), None),
        P("fs", "tp"),
        P("fs", "tp"),
        P("tp"),
        P("tp"),
        P(None, "tp"),
        P(None, "tp"),
    )

    def spread(one):
        return jax.shard_map(one, mesh=mesh, in_specs=placed, out_specs=given, check_vma=False)

    step = spread(body)
    general = step
    n_fs, n_tp = mesh.shape["fs"], mesh.shape["tp"]
    fast = spread(whole_kernel(n_fs, n_tp))

    def pick(*args):
        columns = args[1].shape[1] // n_tp
        if n_tp == 4 and 2 < n_fs // 2 <= 4 and columns % LANES == 0:
            return fast(*args)
        return general(*args)

    return pick
```

```python
import functools

import jax
import jax.numpy as jnp
from jax import lax
from jax.experimental import pallas as pl
from jax.experimental.pallas import tpu as pltpu
from jax.sharding import PartitionSpec as P


BF = jnp.bfloat16
F32 = jnp.float32


LANES = 128


def elementwise(gs_ref, vs_ref, cg_ref, cv_ref, g_ref, v_ref, up_ref, gc_ref, vc_ref, s_ref):
    tokens = g_ref.shape[0]
    row = lax.broadcasted_iota(jnp.int32, g_ref.shape, 0)

    def down(x, k):
        return jnp.where(row >= k, pltpu.roll(x, k, 0), 0.0)

    def up(x, k):
        return jnp.where(row < tokens - k, pltpu.roll(x, tokens - k, 0), 0.0)

    def shifted(ref):
        x = ref[...].astype(F32)
        return down(x, 2), down(x, 1), x

    def conv(taps, xs):
        return taps[0:1] * xs[0] + taps[1:2] * xs[1] + taps[2:3] * xs[2]

    def back(taps, d):
        return (taps[2:3] * d + taps[1:2] * up(d, 1) + taps[0:1] * up(d, 2)).astype(BF)

    gs, vs = shifted(g_ref), shifted(v_ref)
    g = conv(cg_ref[...] * gs_ref[...], gs)
    v = conv(cv_ref[...] * vs_ref[...], vs)
    sig = 1.0 / (1.0 + jnp.exp(-g))
    base = up_ref[...].astype(F32) * sig
    d_gate = base * v * (1.0 + g * (1.0 - sig))
    d_value = base * g
    for j in range(3):
        s_ref[j : j + 1] = jnp.sum(d_gate * gs[j], axis=0, keepdims=True)
        s_ref[3 + j : 4 + j] = jnp.sum(d_value * vs[j], axis=0, keepdims=True)
    s_ref[6:8] = jnp.zeros((2, g_ref.shape[1]), F32)
    gc_ref[...] = back(cg_ref[...], d_gate)
    vc_ref[...] = back(cv_ref[...], d_value)


def cotangents(gs, vs, cg, cv, g, v, up):
    tokens, columns = g.shape
    big = pl.BlockSpec((tokens, LANES), lambda i: (0, i))

    def small(n):
        return pl.BlockSpec((n, LANES), lambda i: (0, i))

    return pl.pallas_call(
        elementwise,
        grid=(pl.cdiv(columns, LANES),),
        in_specs=[small(1), small(1), small(3), small(3), big, big, big],
        out_specs=[big, big, small(8)],
        out_shape=[jax.ShapeDtypeStruct(g.shape, BF)] * 2
        + [jax.ShapeDtypeStruct((8, columns), F32)],
        compiler_params=pltpu.CompilerParams(vmem_limit_bytes=24 * 2**20),
        cost_estimate=pl.CostEstimate(
            flops=g.size * 400, bytes_accessed=g.size * 10, transcendentals=g.size
        ),
    )(gs[None], vs[None], cg, cv, g, v, up)


def rescale(gs_ref, vs_ref, g_ref, v_ref, out_ref):
    out_ref[0] = (g_ref[...] * gs_ref[...]).astype(BF)
    out_ref[1] = (v_ref[...] * vs_ref[...]).astype(BF)


def scaled_weights(gs, vs, g, v):
    own, columns = g.shape
    parts = 4
    block = pl.BlockSpec((own // parts, columns), lambda i: (i, 0))
    scale = pl.BlockSpec((1, columns), lambda i: (0, 0))
    return pl.pallas_call(
        rescale,
        grid=(parts,),
        in_specs=[scale, scale, block, block],
        out_specs=pl.BlockSpec((2, own // parts, columns), lambda i: (0, i, 0)),
        out_shape=jax.ShapeDtypeStruct((2, own, columns), BF),
        compiler_params=pltpu.CompilerParams(vmem_limit_bytes=24 * 2**20),
        cost_estimate=pl.CostEstimate(
            flops=g.size * 100, bytes_accessed=g.size * 12, transcendentals=0
        ),
    )(gs[None], vs[None], g, v)


def tdot(a, b):
    return lax.dot_general(a, b, (((0,), (0,)), ((), ())), preferred_element_type=F32)


def ndot(a, b):
    return lax.dot_general(a, b, (((1,), (1,)), ((), ())), preferred_element_type=F32)


def make(n_fs, n_tp):
    links = n_fs // 2

    def on_device(
        inputs,
        w_gate,
        w_value,
        gate_scale,
        value_scale,
        conv_gate,
        conv_value,
        gate_pre,
        value_pre,
        grad_out,
    ):
        fs = lax.axis_index("fs")
        tp = lax.axis_index("tp")
        c, y = fs // 2, fs % 2
        rows, depth = inputs.shape
        own = w_gate.shape[0]
        half = depth // 2
        tokens, columns = gate_pre.shape

        def swap(x, axis, bit, n):
            return lax.ppermute(x, axis, [(i, i ^ bit) for i in range(n)])

        def chain(x, right, senders):
            step = 1 if right else -1
            pairs = [(2 * s + j, 2 * (s + step) + j) for s in senders for j in (0, 1)]
            return lax.ppermute(x, "fs", pairs)

        stacked = scaled_weights(gate_scale, value_scale, w_gate, w_value)
        rights, lefts = [], []
        r = l = stacked
        for s in range(links - 1):
            r = chain(r, True, range(s, links - 1))
            l = chain(l, False, range(1, links - s))
            rights.append(r)
            lefts.append(l)

        by_half = inputs.reshape(rows, links, 2, own)
        mine = lax.dynamic_index_in_dim(by_half, y, 2, keepdims=False)
        other = lax.dynamic_index_in_dim(by_half, 1 - y, 2, keepdims=False)
        mine, other = mine.reshape(rows, half), other.reshape(rows, half)
        other = swap(other, "fs", 1, n_fs)
        x = jnp.stack([mine, other])[:, None]
        bit = n_tp // 2
        while bit:
            got = swap(x, "tp", bit, n_tp)
            high = (tp // bit) % 2 == 1
            x = jnp.where(high, jnp.stack([got, x], 2), jnp.stack([x, got], 2))
            x = x.reshape(2, -1, rows, half)
            bit //= 2
        x = x.reshape(2, tokens, half)

        gate_cot, value_cot, sums = cotangents(
            gate_scale, value_scale, conv_gate, conv_value, gate_pre, value_pre, grad_out
        )
        bit = n_fs // 2
        while bit:
            sums = sums + swap(sums, "fs", bit, n_fs)
            bit //= 2

        gate_theirs = swap(gate_cot, "fs", 1, n_fs)
        value_theirs = swap(value_cot, "fs", 1, n_fs)
        pair = [(gate_cot, gate_theirs), (value_cot, value_theirs)]

        def at(blocks, i):
            return lax.dynamic_index_in_dim(
                blocks, jnp.clip(i, 0, links - 1), 0, keepdims=False
            )

        def collect(parts):
            r = l = None
            for t in range(links - 1):
                send_r = at(parts, links - 1 - t + c)
                send_l = at(parts, c - (links - 1 - t) + 0)
                if t:
                    send_r = (send_r.astype(F32) + r.astype(F32)).astype(BF)
                    send_l = (send_l.astype(F32) + l.astype(F32)).astype(BF)
                r = chain(send_r, True, range(0, t + 1))
                l = chain(send_l, False, range(links - 1 - t, links))
            total = at(parts, c).astype(F32)
            if r is not None:
                total = total + r.astype(F32) + l.astype(F32)
            return total

        grads = []
        for (cot, theirs), scale in zip(pair, (gate_scale, value_scale)):
            first = tdot(x[0], cot)
            parts = (first + tdot(x[1], theirs)).astype(BF)
            blocks = parts.reshape(links, own, columns)
            grads.append(collect(blocks) * scale)

        blocks = [stacked]
        for s in range(links - 1):
            blocks.append(jnp.where(c > s, rights[s], lefts[links - 2 - s]))
        columns_of = []
        for block in blocks:
            columns_of.append(
                [
                    (ndot(g, block[0]) + ndot(v, block[1])).astype(BF)
                    for g, v in zip(pair[0], pair[1])
                ]
            )
        part = jnp.stack([jnp.concatenate(t, 1) for t in zip(*columns_of)])
        part = part.reshape(2, n_tp, rows, half)
        bit = 1
        while bit < n_tp:
            split = part.reshape(2, -1, 2, rows, half)
            which = (tp // bit) % 2
            keep = lax.dynamic_index_in_dim(split, which, 2, keepdims=False)
            send = lax.dynamic_index_in_dim(split, 1 - which, 2, keepdims=False)
            got = swap(send, "tp", bit, n_tp)
            part = (keep.astype(F32) + got.astype(F32)).astype(BF)
            bit *= 2
        mine = part.reshape(2, rows, half)[0]
        other = swap(part.reshape(2, rows, half)[1], "fs", 1, n_fs)
        both = jnp.where(
            y == 0, jnp.stack([mine, other], 1), jnp.stack([other, mine], 1)
        ).reshape(rows, 2, links, own)
        order = (c - jnp.arange(links)) % links
        grad_inputs = jnp.take(both, order, axis=2).transpose(0, 2, 1, 3)
        return (
            grad_inputs.reshape(rows, depth),
            grads[0],
            grads[1],
            jnp.sum(conv_gate * sums[0:3], axis=0),
            jnp.sum(conv_value * sums[3:6], axis=0),
            sums[0:3] * gate_scale,
            sums[3:6] * value_scale,
        )

    return on_device


MESH = pl.DeviceIdType.MESH
SKEW = 2


def segments(links, pieces):
    table = []
    for pos in range(links - 1):
        reach = links - 1 - pos
        rows, count, last = [], 0, None
        for tick in range(pieces + SKEW * (reach - 1)):
            live = [k for k in range(reach) if 0 <= tick - SKEW * k < pieces]
            key = (live[0], len(live)) if live else None
            if key and key != last:
                rows.append((count, tick, live[0], len(live)))
            last = key
            count += len(live)
        table.append(rows)
    return table


def fused(dims, *refs):
    n_fs, n_tp = dims
    (
        inp, wg, wv, gs_in, vs_in, cg_in, cv_in, gp, vp, up,
        gi, gw, small,
        wraw, pre, wbuf, cot, part, rs0, rs1, xin, xs, xb, xt,
        acc, dxb, dx1, ds1, dx2, ds2, dx3, gs1, vs1, gs, vs, cg, cv, fin, sown, spair, sfrom, sgot, sput,
        load_sem, hop_sem, z_sem, y_sem, ysend_sem, xsend_sem, xrecv_sem,
        dsend_sem, drecv_sem, ssend_sem, srecv_sem,
    ) = refs
    rs = (rs0, rs1)
    links = n_fs // 2
    pieces = cot.shape[0]
    own = wg.shape[0]
    rows, _ = inp.shape
    tokens = gp.shape[0]
    slots = links * pieces

    fs = lax.axis_index("fs")
    tp = lax.axis_index("tp")
    c, y = lax.div(fs, 2), lax.rem(fs, 2)
    xx, core = lax.div(tp, 2), lax.rem(tp, 2)
    y_dev = (fs + 1 - 2 * y, tp)
    x_dev = (fs, tp + 2 - 4 * xx)
    core_dev = (fs, tp + 1 - 2 * core)
    x_tp = tp + 2 - 4 * xx
    position = (c, links - 1 - c)
    follower = ((fs + 2, tp), (fs - 2, tp))

    def real(way, index):
        return index if way == 0 else links - 1 - index

    def remote(src, dst, send, recv, device):
        return pltpu.make_async_remote_copy(
            src_ref=src, dst_ref=dst, send_sem=send, recv_sem=recv,
            device_id=device, device_id_type=MESH,
        )

    def lanes(j):
        return pl.ds(pl.multiple_of(j * LANES, LANES), LANES)

    def load(src, dst, k):
        copy = pltpu.make_async_copy(src, dst, load_sem.at[k])
        copy.start()
        return copy

    def loaded(ref, k):
        pltpu.make_async_copy(ref, ref, load_sem.at[k]).wait()

    head, rest = pl.ds(0, LANES), pl.ds(LANES, (pieces - 1) * LANES)
    scales = [load(gs_in, gs1, 4), load(vs_in, vs1, 5)]
    for at, k in ((head, 0), (rest, 1)):
        for i, w in enumerate((wg, wv)):
            load(w.at[:, at], wraw.at[i, :, at], k)
    load(inp, xin, 2)
    for i, a in enumerate((gp, vp, up)):
        load(a, pre.at[i], 3)
    taps = [load(cg_in, cg, 6), load(cv_in, cv, 7)]

    barrier = pltpu.get_barrier_semaphore()
    for device in (y_dev, x_dev, core_dev):
        pl.semaphore_signal(barrier, inc=1, device_id=device, device_id_type=MESH)
    for way in (0, 1):
        @pl.when(position[way] < links - 1)
        def _():
            pl.semaphore_signal(barrier, inc=1, device_id=follower[way], device_id_type=MESH)
    inner = jnp.where((c > 0) & (c < links - 1), 5, 4)
    pl.semaphore_wait(barrier, inner)

    def ag_copy(way, o, j):
        return remote(
            wbuf.at[o, j], wbuf.at[o, j], z_sem.at[way], hop_sem.at[way, o, lax.div(j, 2)], follower[way]
        )

    def rs_copy(way, src, t, j):
        return remote(
            src.at[t, j], rs[way].at[t, j], z_sem.at[way], hop_sem.at[way, t, lax.div(j, 2)], follower[way]
        )

    def arrived(way, ref, i, j):
        even = lax.rem(j, 2) == 0

        def take(n):
            both = ref.at[i, pl.ds(j, n)]
            sem = hop_sem.at[way, i, lax.div(j, 2)]
            remote(both, both, z_sem.at[way], sem, follower[way]).wait_recv()

        @pl.when(even & (j + 1 < pieces))
        def _():
            take(2)

        if pieces % 2:
            @pl.when(j == pieces - 1)
            def _():
                take(1)

    def y_copy(j):
        return remote(
            cot.at[j, pl.ds(0, tokens)], cot.at[j, pl.ds(tokens, tokens)],
            ysend_sem.at[0], y_sem.at[j], y_dev,
        )

    for copy in scales:
        copy.wait()
    gs[...] = gs1[...].reshape(gs.shape)
    vs[...] = vs1[...].reshape(vs.shape)
    loaded(wraw.at[:, :, head], 0)

    def weights(j, _):
        at = lanes(j)
        wbuf[c, j, :, 0:LANES] = (wraw[0, :, at] * gs[:, at]).astype(BF)
        wbuf[c, j, :, LANES : 2 * LANES] = (wraw[1, :, at] * vs[:, at]).astype(BF)
        for way in (0, 1):
            @pl.when(position[way] < links - 1)
            def _():
                ag_copy(way, c, j).start()
        return 0

    weights(0, 0)
    loaded(wraw.at[:, :, rest], 1)
    lax.fori_loop(1, pieces, weights, 0)

    loaded(xin, 2)
    for o in range(links):
        for h in (0, 1):
            block = xin[:, (2 * o + h) * own : (2 * o + h + 1) * own]

            @pl.when(y == h)
            def _():
                xb[tp, :, o * own : (o + 1) * own] = block

            @pl.when(y != h)
            def _():
                xs[:, o * own : (o + 1) * own] = block

    xy = remote(xs, xb.at[n_tp + tp], xsend_sem.at[0], xrecv_sem.at[0], y_dev)
    xy.start()
    xx0 = remote(xb.at[tp], xb.at[tp], xsend_sem.at[0], xrecv_sem.at[1], x_dev)
    xx0.start()
    xc0 = remote(xb.at[tp], xb.at[tp], xsend_sem.at[0], xrecv_sem.at[2], core_dev)
    xc0.start()

    loaded(pre, 3)
    for copy in taps:
        copy.wait()

    row = lax.broadcasted_iota(jnp.int32, (tokens, LANES), 0)

    def down(a, k):
        return jnp.where(row >= k, pltpu.roll(a, k, 0), 0.0)

    def upward(a, k):
        return jnp.where(row < tokens - k, pltpu.roll(a, tokens - k, 0), 0.0)

    def elements(j, _):
        at = lanes(j)

        def shifted(i):
            a = pre[i, :, at].astype(F32)
            return down(a, 2), down(a, 1), a

        def conv(taps, a):
            return taps[0:1] * a[0] + taps[1:2] * a[1] + taps[2:3] * a[2]

        def back(taps, d):
            return (taps[2:3] * d + taps[1:2] * upward(d, 1) + taps[0:1] * upward(d, 2)).astype(BF)

        tg, tv = cg[:, at], cv[:, at]
        ga, va = shifted(0), shifted(1)
        g = conv(tg * gs[:, at], ga)
        v = conv(tv * vs[:, at], va)
        sig = 1.0 / (1.0 + jnp.exp(-g))
        base = pre[2, :, at].astype(F32) * sig
        d_gate = base * v * (1.0 + g * (1.0 - sig))
        d_value = base * g
        cot[j, 0:tokens, 0:LANES] = back(tg, d_gate)
        cot[j, 0:tokens, LANES : 2 * LANES] = back(tv, d_value)
        y_copy(j).start()
        for k in range(3):
            sown[k : k + 1, at] = jnp.sum(d_gate * ga[k], axis=0, keepdims=True)
            sown[3 + k : 4 + k, at] = jnp.sum(d_value * va[k], axis=0, keepdims=True)
        sown[6:8, at] = jnp.zeros((2, LANES), F32)
        return 0

    lax.fori_loop(0, pieces, elements, 0)

    xy.wait_recv()
    xx1 = remote(xb.at[n_tp + tp], xb.at[n_tp + tp], xsend_sem.at[0], xrecv_sem.at[3], x_dev)
    xx1.start()
    xc1 = remote(xb.at[n_tp + tp], xb.at[n_tp + tp], xsend_sem.at[0], xrecv_sem.at[4], core_dev)
    xc1.start()
    xx0.wait_recv()
    xc2 = remote(xb.at[x_tp], xb.at[x_tp], xsend_sem.at[0], xrecv_sem.at[5], core_dev)
    xc2.start()
    xx1.wait_recv()
    xc3 = remote(xb.at[n_tp + x_tp], xb.at[n_tp + x_tp], xsend_sem.at[0], xrecv_sem.at[6], core_dev)
    xc3.start()
    for copy in (xc0, xc1, xc2, xc3):
        copy.wait_recv()
    for q in (0, 1):
        for i in range(n_tp):
            for o in range(links):
                at = (q * n_tp + i) * rows
                xt[o, :, at : at + rows] = xb[q * n_tp + i, :, o * own : (o + 1) * own].T

    def wait_y(j):
        y_copy(j).wait_recv()

    def partial(j):
        def one(o, _):
            part[o, j] = jnp.dot(xt[o], cot[j], preferred_element_type=F32).astype(BF)
            return 0

        lax.fori_loop(0, links, one, 0)

    table = segments(links, pieces)

    def decode(p, n):
        m = n - pieces * (p + 1)
        k, j = jnp.int32(0), jnp.int32(0)
        for first, tick, low, count in table[p]:
            q = lax.div(m - first, count)
            kk = low + (m - first) - q * count
            here = m >= first
            k = jnp.where(here, kk, k)
            j = jnp.where(here, tick + q - SKEW * kk, j)
        return k, j

    def relay(way, n):
        pos = position[way]

        @pl.when((pos < links - 1) & (n < pieces * (pos + 1)))
        def _():
            q = lax.div(n, pieces)
            j = n - q * pieces
            o = real(way, pos - q)
            arrived(way, wbuf, o, j)
            ag_copy(way, o, j).start()

        @pl.when((pos < links - 1) & (n >= pieces * (pos + 1)) & (n < slots))
        def _():
            k, j = decode(0, n)
            for p in range(1, links - 1):
                kp, jp = decode(p, n)
                k, j = jnp.where(pos == p, kp, k), jnp.where(pos == p, jp, j)
            t = real(way, links - 1 - k)

            @pl.when(pos == 0)
            def _():
                rs_copy(way, part, t, j).start()

            @pl.when(pos > 0)
            def _():
                arrived(way, rs[way], t, j)
                rs[way][t, j] = (rs[way][t, j].astype(F32) + part[t, j].astype(F32)).astype(BF)
                rs_copy(way, rs[way], t, j).start()

    start = (8 * pieces) // 3

    def sum_copy(way):
        return remote(
            sput.at[way], sgot.at[way], ssend_sem.at[way], srecv_sem.at[way], follower[way]
        )

    sy = remote(spair, sfrom, ssend_sem.at[2], srecv_sem.at[2], y_dev)

    def sums_step(way, n):
        pos = position[way]

        @pl.when(n == pieces + (pieces - 1) * pos)
        def _():
            @pl.when(pos == 0)
            def _():
                sput[way] = sown[...]

            @pl.when(pos > 0)
            def _():
                sum_copy(way).wait_recv()
                sput[way] = sown[...] + sgot[way]

            @pl.when(pos < links - 1)
            def _():
                sum_copy(way).start()

    def sums_pair():
        spair[...] = sput[0] + sput[1] - sown[...]
        sy.start()

    dx_at = [start + 2 * p for p in range(links - 1)] + [(links - 1) * pieces + 3]
    order = [sorted(range(links), key=lambda o, a=a: (abs(o - a), o)) for a in range(links)]

    def block_at(n, shift):
        p_is = [n == at + shift for at in dx_at]
        o = jnp.int32(0)
        for a in range(links):
            for p in range(links):
                o = jnp.where(p_is[p] & (c == a), order[a][p], o)
        hit = p_is[0]
        for one in p_is[1:]:
            hit = hit | one
        return hit, o

    def core_copy(o):
        return remote(
            dxb.at[o, 1 - core], dx1.at[o], dsend_sem.at[0], drecv_sem.at[0, o], core_dev
        )

    def across_copy(o):
        return remote(
            ds1.at[o, 1 - xx], dx2.at[o], dsend_sem.at[1], drecv_sem.at[1, o], x_dev
        )

    def home_copy(o):
        return remote(
            ds2.at[o, 1], dx3.at[o], dsend_sem.at[2], drecv_sem.at[2, o], y_dev
        )

    first_late = len([n for n in range(slots) if pieces <= n <= start and _is_lead(table, pieces, n)])

    def dx_steps(n):
        hit, o = block_at(n, 0)

        @pl.when(hit)
        def _():
            for way in (0, 1):
                @pl.when((position[way] == links - 1) & (o != c))
                def _():
                    def one(j, _):
                        arrived(way, wbuf, o, j)
                        return 0

                    lax.fori_loop(0, pieces, one, 0)

            group = next(k for k in (5, 4, 3, 2, 1) if (pieces - 1) % k == 0)

            def one(i, _):
                new = acc[...]
                for j in range(group):
                    at = 1 + group * i + j
                    new = new + ndot(cot[at], wbuf[o, at])
                acc[...] = new
                return 0

            acc[...] = ndot(cot[0], wbuf[o, 0])
            lax.fori_loop(0, (pieces - 1) // group, one, 0)
            for q in (0, 1):
                for i in range(n_tp):
                    at = (q * n_tp + i) * rows
                    dxb[o, i % 2, i // 2, q] = acc[at : at + rows].astype(BF)
            core_copy(o).start()

        hit1, o1 = block_at(n, 1)

        @pl.when(hit1)
        def _():
            core_copy(o1).wait_recv()
            ds1[o1] = (dxb[o1, core].astype(F32) + dx1[o1].astype(F32)).astype(BF)
            across_copy(o1).start()

        hit2, o2 = block_at(n, 3)

        @pl.when(hit2)
        def _():
            across_copy(o2).wait_recv()
            ds2[o2] = (ds1[o2, xx].astype(F32) + dx2[o2].astype(F32)).astype(BF)
            home_copy(o2).start()

    def final(j):
        fin[...] = part[c, j].astype(F32)
        for way in (0, 1):
            @pl.when(position[way] > 0)
            def _():
                arrived(way, rs[way], c, j)
                fin[...] += rs[way][c, j].astype(F32)
        at = lanes(j)
        gw[0, :, at] = fin[:, 0:LANES] * gs[:, at]
        gw[1, :, at] = fin[:, LANES : 2 * LANES] * vs[:, at]

    def results():
        for o in range(links):
            home_copy(o).wait_recv()
            for h in (0, 1):
                at = (2 * o + h) * own

                @pl.when(y == h)
                def _():
                    gi[:, at : at + own] = ds2[o, 0]

                @pl.when(y != h)
                def _():
                    gi[:, at : at + own] = dx3[o]

        sy.wait_recv()
        total = spair[...] + sfrom[...]
        small[0:3] = total[0:3] * gs[...]
        small[3:6] = total[3:6] * vs[...]
        small[6:7] = jnp.sum(cg[...] * total[0:3], axis=0, keepdims=True)
        small[7:8] = jnp.sum(cv[...] * total[3:6], axis=0, keepdims=True)

    wait_y(0)
    partial(0)
    last = (links - 1) * pieces + 3

    def slot(n, _):
        for way in (0, 1):
            relay(way, n)
            sums_step(way, n)

        @pl.when(n == start)
        def _():
            for late in range(first_late, pieces):
                wait_y(late)

        k, j = decode(0, n + 1)

        @pl.when((k == 0) & (n + 1 < slots))
        def _():
            @pl.when(n < start)
            def _():
                wait_y(j)

            partial(j)

        dx_steps(n)

        @pl.when(n == pieces + (pieces - 1) * (links - 1))
        def _():
            sums_pair()

        @pl.when(n >= last)
        def _():
            final(n - last)

        @pl.when(n == last + pieces - 3)
        def _():
            results()

        return 0

    lax.fori_loop(pieces, last + pieces, slot, 0)

    seven = xb.at[pl.ds(0, 7)]
    remote(seven, seven, xsend_sem.at[0], xrecv_sem.at[0], x_dev).wait_send()
    sy.wait_send()
    for ref, k in ((dx1, 0), (ds1.at[:, 0], 1), (dx3, 2)):
        remote(ref, ref, dsend_sem.at[k], drecv_sem.at[k, 0], y_dev).wait_send()
    for way in (0, 1):
        @pl.when(position[way] < links - 1)
        def _():
            sum_copy(way).wait_send()
            remote(wbuf, wbuf, z_sem.at[way], hop_sem.at[way, 0, 0], follower[way]).wait_send()
    mine = cot.at[:, pl.ds(0, tokens)]
    remote(mine, mine, ysend_sem.at[0], y_sem.at[0], y_dev).wait_send()


def _is_lead(table, pieces, n):
    m = n - pieces
    k = None
    for first, tick, low, count in table[0]:
        if m >= first:
            k = low + (m - first) % count
    return k == 0


def deliver(gi_in, gw_in, small, *refs):
    gi, gwg, gwv, ggs, gvs, gcg, gcv, sg, sv, tg, tv, sem = refs
    copies = []

    def send(src, dst):
        copies.append(pltpu.make_async_copy(src, dst, sem.at[len(copies)]))
        copies[-1].start()

    part = gwg.shape[0] // 4
    for i in range(4):
        at = pl.ds(i * part, part)
        send(gw_in.at[0, at], gwg.at[at])
        send(gw_in.at[1, at], gwv.at[at])
    send(gi_in, gi)
    tg[...] = small[0:3]
    tv[...] = small[3:6]
    sg[...] = small[6:7].reshape(sg.shape)
    sv[...] = small[7:8].reshape(sv.shape)
    for src, dst in ((tg, gcg), (tv, gcv), (sg, ggs), (sv, gvs)):
        send(src, dst)
    for copy in copies:
        copy.wait()


def whole_kernel(n_fs, n_tp):
    links = n_fs // 2

    def on_device(inputs, w_gate, w_value, gate_scale, value_scale, conv_gate, conv_value,
                  gate_pre, value_pre, grad_out):
        rows, depth = inputs.shape
        own, columns = w_gate.shape
        tokens = gate_pre.shape[0]
        half = depth // 2
        pieces = columns // LANES
        anywhere = pl.BlockSpec(memory_space=pl.ANY)
        vmem = pl.BlockSpec(memory_space=pltpu.VMEM)
        dma, vm = pltpu.SemaphoreType.DMA, pltpu.VMEM
        wide = 2 * LANES
        outs = pl.pallas_call(
            functools.partial(fused, (n_fs, n_tp)),
            in_specs=[anywhere] * 10,
            out_specs=[vmem] * 3,
            out_shape=[
                vm((rows, depth), BF),
                vm((2, own, columns), F32),
                vm((8, columns), F32),
            ],
            scratch_shapes=[
                vm((2, own, columns), F32),
                vm((3, tokens, columns), BF),
                vm((links, pieces, own, wide), BF),
                vm((pieces, 2 * tokens, wide), BF),
                vm((links, pieces, own, wide), BF),
                vm((links, pieces, own, wide), BF),
                vm((links, pieces, own, wide), BF),
                vm((rows, depth), BF),
                vm((rows, half), BF),
                vm((2 * n_tp, rows, half), BF),
                vm((links, own, 2 * tokens), BF),
                vm((2 * tokens, own), F32),
                vm((links, 2, 2, 2, rows, own), BF),
                vm((links, 2, 2, rows, own), BF),
                vm((links, 2, 2, rows, own), BF),
                vm((links, 2, rows, own), BF),
                vm((links, 2, rows, own), BF),
                vm((links, rows, own), BF),
                vm((columns,), F32),
                vm((columns,), F32),
                vm((1, columns), F32),
                vm((1, columns), F32),
                vm((3, columns), F32),
                vm((3, columns), F32),
                vm((own, wide), F32),
                vm((8, columns), F32),
                vm((8, columns), F32),
                vm((8, columns), F32),
                vm((2, 8, columns), F32),
                vm((2, 8, columns), F32),
                dma((8,)),
                dma((2, links, (pieces + 1) // 2)),
                dma((2,)),
                dma((pieces,)),
                dma((1,)),
                dma((1,)),
                dma((7,)),
                dma((3,)),
                dma((3, links)),
                dma((3,)),
                dma((3,)),
            ],
            compiler_params=pltpu.CompilerParams(
                collective_id=0, has_side_effects=True, vmem_limit_bytes=52 * 2**20
            ),
        )(
            inputs, w_gate, w_value, gate_scale, value_scale, conv_gate, conv_value,
            gate_pre, value_pre, grad_out,
        )
        return pl.pallas_call(
            deliver,
            in_specs=[vmem] * 3,
            out_specs=[anywhere] * 7,
            out_shape=[
                jax.ShapeDtypeStruct((rows, depth), BF),
                jax.ShapeDtypeStruct((own, columns), F32),
                jax.ShapeDtypeStruct((own, columns), F32),
                jax.ShapeDtypeStruct((columns,), F32),
                jax.ShapeDtypeStruct((columns,), F32),
                jax.ShapeDtypeStruct((3, columns), F32),
                jax.ShapeDtypeStruct((3, columns), F32),
            ],
            scratch_shapes=[
                vm((columns,), F32),
                vm((columns,), F32),
                vm((3, columns), F32),
                vm((3, columns), F32),
                dma((13,)),
            ],
            compiler_params=pltpu.CompilerParams(vmem_limit_bytes=2 * 2**20),
        )(*outs)

    return on_device


def solution(mesh):
    placed = (
        P(("fs", "tp"), None),
        P("fs", "tp"),
        P("fs", "tp"),
        P("tp"),
        P("tp"),
        P(None, "tp"),
        P(None, "tp"),
        P("fs", "tp"),
        P("fs", "tp"),
        P("fs", "tp"),
    )
    body = make(mesh.shape["fs"], mesh.shape["tp"])

    given = (
        P(("fs", "tp"), None),
        P("fs", "tp"),
        P("fs", "tp"),
        P("tp"),
        P("tp"),
        P(None, "tp"),
        P(None, "tp"),
    )

    def spread(one):
        return jax.shard_map(one, mesh=mesh, in_specs=placed, out_specs=given, check_vma=False)

    step = spread(body)
    general = step
    n_fs, n_tp = mesh.shape["fs"], mesh.shape["tp"]
    fast = spread(whole_kernel(n_fs, n_tp))

    def pick(*args):
        columns = args[1].shape[1] // n_tp
        if n_tp == 4 and 2 < n_fs // 2 <= 4 and columns % LANES == 0:
            return fast(*args)
        return general(*args)

    return pick
```

```python
import functools

import jax
import jax.numpy as jnp
from jax import lax
from jax.experimental import pallas as pl
from jax.experimental.pallas import tpu as pltpu
from jax.sharding import PartitionSpec as P


BF = jnp.bfloat16
F32 = jnp.float32


LANES = 128


def elementwise(gs_ref, vs_ref, cg_ref, cv_ref, g_ref, v_ref, up_ref, gc_ref, vc_ref, s_ref):
    tokens = g_ref.shape[0]
    row = lax.broadcasted_iota(jnp.int32, g_ref.shape, 0)

    def down(x, k):
        return jnp.where(row >= k, pltpu.roll(x, k, 0), 0.0)

    def up(x, k):
        return jnp.where(row < tokens - k, pltpu.roll(x, tokens - k, 0), 0.0)

    def shifted(ref):
        x = ref[...].astype(F32)
        return down(x, 2), down(x, 1), x

    def conv(taps, xs):
        return taps[0:1] * xs[0] + taps[1:2] * xs[1] + taps[2:3] * xs[2]

    def back(taps, d):
        return (taps[2:3] * d + taps[1:2] * up(d, 1) + taps[0:1] * up(d, 2)).astype(BF)

    gs, vs = shifted(g_ref), shifted(v_ref)
    g = conv(cg_ref[...] * gs_ref[...], gs)
    v = conv(cv_ref[...] * vs_ref[...], vs)
    sig = 1.0 / (1.0 + jnp.exp(-g))
    base = up_ref[...].astype(F32) * sig
    d_gate = base * v * (1.0 + g * (1.0 - sig))
    d_value = base * g
    for j in range(3):
        s_ref[j : j + 1] = jnp.sum(d_gate * gs[j], axis=0, keepdims=True)
        s_ref[3 + j : 4 + j] = jnp.sum(d_value * vs[j], axis=0, keepdims=True)
    s_ref[6:8] = jnp.zeros((2, g_ref.shape[1]), F32)
    gc_ref[...] = back(cg_ref[...], d_gate)
    vc_ref[...] = back(cv_ref[...], d_value)


def cotangents(gs, vs, cg, cv, g, v, up):
    tokens, columns = g.shape
    big = pl.BlockSpec((tokens, LANES), lambda i: (0, i))

    def small(n):
        return pl.BlockSpec((n, LANES), lambda i: (0, i))

    return pl.pallas_call(
        elementwise,
        grid=(pl.cdiv(columns, LANES),),
        in_specs=[small(1), small(1), small(3), small(3), big, big, big],
        out_specs=[big, big, small(8)],
        out_shape=[jax.ShapeDtypeStruct(g.shape, BF)] * 2
        + [jax.ShapeDtypeStruct((8, columns), F32)],
        compiler_params=pltpu.CompilerParams(vmem_limit_bytes=24 * 2**20),
        cost_estimate=pl.CostEstimate(
            flops=g.size * 400, bytes_accessed=g.size * 10, transcendentals=g.size
        ),
    )(gs[None], vs[None], cg, cv, g, v, up)


def rescale(gs_ref, vs_ref, g_ref, v_ref, out_ref):
    out_ref[0] = (g_ref[...] * gs_ref[...]).astype(BF)
    out_ref[1] = (v_ref[...] * vs_ref[...]).astype(BF)


def scaled_weights(gs, vs, g, v):
    own, columns = g.shape
    parts = 4
    block = pl.BlockSpec((own // parts, columns), lambda i: (i, 0))
    scale = pl.BlockSpec((1, columns), lambda i: (0, 0))
    return pl.pallas_call(
        rescale,
        grid=(parts,),
        in_specs=[scale, scale, block, block],
        out_specs=pl.BlockSpec((2, own // parts, columns), lambda i: (0, i, 0)),
        out_shape=jax.ShapeDtypeStruct((2, own, columns), BF),
        compiler_params=pltpu.CompilerParams(vmem_limit_bytes=24 * 2**20),
        cost_estimate=pl.CostEstimate(
            flops=g.size * 100, bytes_accessed=g.size * 12, transcendentals=0
        ),
    )(gs[None], vs[None], g, v)


def tdot(a, b):
    return lax.dot_general(a, b, (((0,), (0,)), ((), ())), preferred_element_type=F32)


def ndot(a, b):
    return lax.dot_general(a, b, (((1,), (1,)), ((), ())), preferred_element_type=F32)


def make(n_fs, n_tp):
    links = n_fs // 2

    def on_device(
        inputs,
        w_gate,
        w_value,
        gate_scale,
        value_scale,
        conv_gate,
        conv_value,
        gate_pre,
        value_pre,
        grad_out,
    ):
        fs = lax.axis_index("fs")
        tp = lax.axis_index("tp")
        c, y = fs // 2, fs % 2
        rows, depth = inputs.shape
        own = w_gate.shape[0]
        half = depth // 2
        tokens, columns = gate_pre.shape

        def swap(x, axis, bit, n):
            return lax.ppermute(x, axis, [(i, i ^ bit) for i in range(n)])

        def chain(x, right, senders):
            step = 1 if right else -1
            pairs = [(2 * s + j, 2 * (s + step) + j) for s in senders for j in (0, 1)]
            return lax.ppermute(x, "fs", pairs)

        stacked = scaled_weights(gate_scale, value_scale, w_gate, w_value)
        rights, lefts = [], []
        r = l = stacked
        for s in range(links - 1):
            r = chain(r, True, range(s, links - 1))
            l = chain(l, False, range(1, links - s))
            rights.append(r)
            lefts.append(l)

        by_half = inputs.reshape(rows, links, 2, own)
        mine = lax.dynamic_index_in_dim(by_half, y, 2, keepdims=False)
        other = lax.dynamic_index_in_dim(by_half, 1 - y, 2, keepdims=False)
        mine, other = mine.reshape(rows, half), other.reshape(rows, half)
        other = swap(other, "fs", 1, n_fs)
        x = jnp.stack([mine, other])[:, None]
        bit = n_tp // 2
        while bit:
            got = swap(x, "tp", bit, n_tp)
            high = (tp // bit) % 2 == 1
            x = jnp.where(high, jnp.stack([got, x], 2), jnp.stack([x, got], 2))
            x = x.reshape(2, -1, rows, half)
            bit //= 2
        x = x.reshape(2, tokens, half)

        gate_cot, value_cot, sums = cotangents(
            gate_scale, value_scale, conv_gate, conv_value, gate_pre, value_pre, grad_out
        )
        bit = n_fs // 2
        while bit:
            sums = sums + swap(sums, "fs", bit, n_fs)
            bit //= 2

        gate_theirs = swap(gate_cot, "fs", 1, n_fs)
        value_theirs = swap(value_cot, "fs", 1, n_fs)
        pair = [(gate_cot, gate_theirs), (value_cot, value_theirs)]

        def at(blocks, i):
            return lax.dynamic_index_in_dim(
                blocks, jnp.clip(i, 0, links - 1), 0, keepdims=False
            )

        def collect(parts):
            r = l = None
            for t in range(links - 1):
                send_r = at(parts, links - 1 - t + c)
                send_l = at(parts, c - (links - 1 - t) + 0)
                if t:
                    send_r = (send_r.astype(F32) + r.astype(F32)).astype(BF)
                    send_l = (send_l.astype(F32) + l.astype(F32)).astype(BF)
                r = chain(send_r, True, range(0, t + 1))
                l = chain(send_l, False, range(links - 1 - t, links))
            total = at(parts, c).astype(F32)
            if r is not None:
                total = total + r.astype(F32) + l.astype(F32)
            return total

        grads = []
        for (cot, theirs), scale in zip(pair, (gate_scale, value_scale)):
            first = tdot(x[0], cot)
            parts = (first + tdot(x[1], theirs)).astype(BF)
            blocks = parts.reshape(links, own, columns)
            grads.append(collect(blocks) * scale)

        blocks = [stacked]
        for s in range(links - 1):
            blocks.append(jnp.where(c > s, rights[s], lefts[links - 2 - s]))
        columns_of = []
        for block in blocks:
            columns_of.append(
                [
                    (ndot(g, block[0]) + ndot(v, block[1])).astype(BF)
                    for g, v in zip(pair[0], pair[1])
                ]
            )
        part = jnp.stack([jnp.concatenate(t, 1) for t in zip(*columns_of)])
        part = part.reshape(2, n_tp, rows, half)
        bit = 1
        while bit < n_tp:
            split = part.reshape(2, -1, 2, rows, half)
            which = (tp // bit) % 2
            keep = lax.dynamic_index_in_dim(split, which, 2, keepdims=False)
            send = lax.dynamic_index_in_dim(split, 1 - which, 2, keepdims=False)
            got = swap(send, "tp", bit, n_tp)
            part = (keep.astype(F32) + got.astype(F32)).astype(BF)
            bit *= 2
        mine = part.reshape(2, rows, half)[0]
        other = swap(part.reshape(2, rows, half)[1], "fs", 1, n_fs)
        both = jnp.where(
            y == 0, jnp.stack([mine, other], 1), jnp.stack([other, mine], 1)
        ).reshape(rows, 2, links, own)
        order = (c - jnp.arange(links)) % links
        grad_inputs = jnp.take(both, order, axis=2).transpose(0, 2, 1, 3)
        return (
            grad_inputs.reshape(rows, depth),
            grads[0],
            grads[1],
            jnp.sum(conv_gate * sums[0:3], axis=0),
            jnp.sum(conv_value * sums[3:6], axis=0),
            sums[0:3] * gate_scale,
            sums[3:6] * value_scale,
        )

    return on_device


MESH = pl.DeviceIdType.MESH
SKEW = 2


def segments(links, pieces):
    table = []
    for pos in range(links - 1):
        reach = links - 1 - pos
        rows, count, last = [], 0, None
        for tick in range(pieces + SKEW * (reach - 1)):
            live = [k for k in range(reach) if 0 <= tick - SKEW * k < pieces]
            key = (live[0], len(live)) if live else None
            if key and key != last:
                rows.append((count, tick, live[0], len(live)))
            last = key
            count += len(live)
        table.append(rows)
    return table


def fused(dims, *refs):
    n_fs, n_tp = dims
    (
        inp, wg, wv, gs_in, vs_in, cg_in, cv_in, gp, vp, up,
        gi, gw, small,
        wraw, pre, wbuf, cot, part, rs0, rs1, xin, xs, xb, xt,
        acc, dxb, dx1, ds1, dx2, ds2, dx3, gs1, vs1, gs, vs, cg, cv, fin, sown, sfrom, spair, sgot, sput, stot, sall,
        load_sem, hop_sem, z_sem, y_sem, ysend_sem, xsend_sem, xrecv_sem,
        dsend_sem, drecv_sem, ssend_sem, srecv_sem,
    ) = refs
    rs = (rs0, rs1)
    links = n_fs // 2
    pieces = cot.shape[0]
    own = wg.shape[0]
    rows, _ = inp.shape
    tokens = gp.shape[0]
    slots = links * pieces

    fs = lax.axis_index("fs")
    tp = lax.axis_index("tp")
    c, y = lax.div(fs, 2), lax.rem(fs, 2)
    xx, core = lax.div(tp, 2), lax.rem(tp, 2)
    y_dev = (fs + 1 - 2 * y, tp)
    x_dev = (fs, tp + 2 - 4 * xx)
    core_dev = (fs, tp + 1 - 2 * core)
    x_tp = tp + 2 - 4 * xx
    position = (c, links - 1 - c)
    follower = ((fs + 2, tp), (fs - 2, tp))

    def real(way, index):
        return index if way == 0 else links - 1 - index

    def remote(src, dst, send, recv, device):
        return pltpu.make_async_remote_copy(
            src_ref=src, dst_ref=dst, send_sem=send, recv_sem=recv,
            device_id=device, device_id_type=MESH,
        )

    def lanes(j):
        return pl.ds(pl.multiple_of(j * LANES, LANES), LANES)

    def load(src, dst, k):
        copy = pltpu.make_async_copy(src, dst, load_sem.at[k])
        copy.start()
        return copy

    def loaded(ref, k):
        pltpu.make_async_copy(ref, ref, load_sem.at[k]).wait()

    head, rest = pl.ds(0, LANES), pl.ds(LANES, (pieces - 1) * LANES)
    scales = [load(gs_in, gs1, 4), load(vs_in, vs1, 5)]
    for at, k in ((head, 0), (rest, 1)):
        for i, w in enumerate((wg, wv)):
            load(w.at[:, at], wraw.at[i, :, at], k)
    load(inp, xin, 2)
    for i, a in enumerate((gp, vp, up)):
        load(a, pre.at[i], 3)
    taps = [load(cg_in, cg, 6), load(cv_in, cv, 7)]

    barrier = pltpu.get_barrier_semaphore()
    for device in (y_dev, x_dev, core_dev):
        pl.semaphore_signal(barrier, inc=1, device_id=device, device_id_type=MESH)
    for way in (0, 1):
        @pl.when(position[way] < links - 1)
        def _():
            pl.semaphore_signal(barrier, inc=1, device_id=follower[way], device_id_type=MESH)
    inner = jnp.where((c > 0) & (c < links - 1), 5, 4)
    pl.semaphore_wait(barrier, inner)

    def ag_copy(way, o, j):
        return remote(
            wbuf.at[o, j], wbuf.at[o, j], z_sem.at[way], hop_sem.at[way, o, lax.div(j, 2)], follower[way]
        )

    def rs_copy(way, src, t, j):
        return remote(
            src.at[t, j], rs[way].at[t, j], z_sem.at[way], hop_sem.at[way, t, lax.div(j, 2)], follower[way]
        )

    def arrived(way, ref, i, j):
        even = lax.rem(j, 2) == 0

        def take(n):
            both = ref.at[i, pl.ds(j, n)]
            sem = hop_sem.at[way, i, lax.div(j, 2)]
            remote(both, both, z_sem.at[way], sem, follower[way]).wait_recv()

        @pl.when(even & (j + 1 < pieces))
        def _():
            take(2)

        if pieces % 2:
            @pl.when(j == pieces - 1)
            def _():
                take(1)

    def y_copy(j):
        return remote(
            cot.at[j, pl.ds(0, tokens)], cot.at[j, pl.ds(tokens, tokens)],
            ysend_sem.at[0], y_sem.at[j], y_dev,
        )

    for copy in scales:
        copy.wait()
    gs[...] = gs1[...].reshape(gs.shape)
    vs[...] = vs1[...].reshape(vs.shape)
    loaded(wraw.at[:, :, head], 0)

    def weights(j, _):
        at = lanes(j)
        wbuf[c, j, :, 0:LANES] = (wraw[0, :, at] * gs[:, at]).astype(BF)
        wbuf[c, j, :, LANES : 2 * LANES] = (wraw[1, :, at] * vs[:, at]).astype(BF)
        for way in (0, 1):
            @pl.when(position[way] < links - 1)
            def _():
                ag_copy(way, c, j).start()
        return 0

    weights(0, 0)
    loaded(wraw.at[:, :, rest], 1)
    lax.fori_loop(1, pieces, weights, 0)

    loaded(xin, 2)
    for o in range(links):
        for h in (0, 1):
            block = xin[:, (2 * o + h) * own : (2 * o + h + 1) * own]

            @pl.when(y == h)
            def _():
                xb[tp, :, o * own : (o + 1) * own] = block

            @pl.when(y != h)
            def _():
                xs[:, o * own : (o + 1) * own] = block

    xy = remote(xs, xb.at[n_tp + tp], xsend_sem.at[0], xrecv_sem.at[0], y_dev)
    xy.start()
    xx0 = remote(xb.at[tp], xb.at[tp], xsend_sem.at[0], xrecv_sem.at[1], x_dev)
    xx0.start()
    xc0 = remote(xb.at[tp], xb.at[tp], xsend_sem.at[0], xrecv_sem.at[2], core_dev)
    xc0.start()

    loaded(pre, 3)
    for copy in taps:
        copy.wait()

    row = lax.broadcasted_iota(jnp.int32, (tokens, LANES), 0)

    def down(a, k):
        return jnp.where(row >= k, pltpu.roll(a, k, 0), 0.0)

    def upward(a, k):
        return jnp.where(row < tokens - k, pltpu.roll(a, tokens - k, 0), 0.0)

    def elements(j, _):
        at = lanes(j)

        def shifted(i):
            a = pre[i, :, at].astype(F32)
            return down(a, 2), down(a, 1), a

        def conv(taps, a):
            return taps[0:1] * a[0] + taps[1:2] * a[1] + taps[2:3] * a[2]

        def back(taps, d):
            return (taps[2:3] * d + taps[1:2] * upward(d, 1) + taps[0:1] * upward(d, 2)).astype(BF)

        tg, tv = cg[:, at], cv[:, at]
        ga, va = shifted(0), shifted(1)
        g = conv(tg * gs[:, at], ga)
        v = conv(tv * vs[:, at], va)
        sig = 1.0 / (1.0 + jnp.exp(-g))
        base = pre[2, :, at].astype(F32) * sig
        d_gate = base * v * (1.0 + g * (1.0 - sig))
        d_value = base * g
        cot[j, 0:tokens, 0:LANES] = back(tg, d_gate)
        cot[j, 0:tokens, LANES : 2 * LANES] = back(tv, d_value)
        for k in range(3):
            sown[k : k + 1, at] = jnp.sum(d_gate * ga[k], axis=0, keepdims=True)
            sown[3 + k : 4 + k, at] = jnp.sum(d_value * va[k], axis=0, keepdims=True)
        sown[6:8, at] = jnp.zeros((2, LANES), F32)

        @pl.when(j < 2)
        def _():
            y_copy(j).start()

        return 0

    span = (pieces + 1) // 2 * LANES

    def part_of(which):
        return pl.ds(pl.multiple_of(which * (pieces * LANES - span), LANES), span)

    def pair_copy():
        return remote(
            sown.at[:, part_of(1 - y)], sfrom, ssend_sem.at[2], srecv_sem.at[2], y_dev
        )

    def send_y(j, _):
        y_copy(j).start()
        return 0

    lax.fori_loop(0, pieces, elements, 0)
    pair_copy().start()
    lax.fori_loop(2, pieces, send_y, 0)

    xy.wait_recv()
    xx1 = remote(xb.at[n_tp + tp], xb.at[n_tp + tp], xsend_sem.at[0], xrecv_sem.at[3], x_dev)
    xx1.start()
    xc1 = remote(xb.at[n_tp + tp], xb.at[n_tp + tp], xsend_sem.at[0], xrecv_sem.at[2], core_dev)
    xc1.start()
    xx0.wait_recv()
    xc2 = remote(xb.at[x_tp], xb.at[x_tp], xsend_sem.at[0], xrecv_sem.at[2], core_dev)
    xc2.start()
    xx1.wait_recv()
    xc3 = remote(xb.at[n_tp + x_tp], xb.at[n_tp + x_tp], xsend_sem.at[0], xrecv_sem.at[2], core_dev)
    xc3.start()
    four = xb.at[pl.ds(0, 4)]
    remote(four, four, xsend_sem.at[0], xrecv_sem.at[2], core_dev).wait_recv()
    for q in (0, 1):
        for i in range(n_tp):
            for o in range(links):
                at = (q * n_tp + i) * rows
                xt[o, :, at : at + rows] = xb[q * n_tp + i, :, o * own : (o + 1) * own].T

    def wait_y(j):
        y_copy(j).wait_recv()

    def partial(j):
        def one(o, _):
            part[o, j] = jnp.dot(xt[o], cot[j], preferred_element_type=F32).astype(BF)
            return 0

        lax.fori_loop(0, links, one, 0)

    table = segments(links, pieces)

    def decode(p, n):
        m = n - pieces * (p + 1)
        k, j = jnp.int32(0), jnp.int32(0)
        for first, tick, low, count in table[p]:
            q = lax.div(m - first, count)
            kk = low + (m - first) - q * count
            here = m >= first
            k = jnp.where(here, kk, k)
            j = jnp.where(here, tick + q - SKEW * kk, j)
        return k, j

    def relay(way, n):
        pos = position[way]

        @pl.when((pos < links - 1) & (n < pieces * (pos + 1)))
        def _():
            q = lax.div(n, pieces)
            j = n - q * pieces
            o = real(way, pos - q)
            arrived(way, wbuf, o, j)
            ag_copy(way, o, j).start()

        @pl.when((pos < links - 1) & (n >= pieces * (pos + 1)) & (n < slots))
        def _():
            k, j = decode(0, n)
            for p in range(1, links - 1):
                kp, jp = decode(p, n)
                k, j = jnp.where(pos == p, kp, k), jnp.where(pos == p, jp, j)
            t = real(way, links - 1 - k)

            @pl.when(pos == 0)
            def _():
                rs_copy(way, part, t, j).start()

            @pl.when(pos > 0)
            def _():
                arrived(way, rs[way], t, j)
                rs[way][t, j] = (rs[way][t, j].astype(F32) + part[t, j].astype(F32)).astype(BF)
                rs_copy(way, rs[way], t, j).start()

    start = (8 * pieces) // 3

    def sum_copy(way):
        return remote(
            sput.at[way], sgot.at[way], ssend_sem.at[way], srecv_sem.at[way], follower[way]
        )

    total_copy = remote(stot, sall, ssend_sem.at[3], srecv_sem.at[3], y_dev)

    def sums_step(way, n):
        pos = position[way]

        @pl.when(n == pieces + (pieces - 1) * pos)
        def _():
            @pl.when(pos == 0)
            def _():
                sput[way] = spair[...]

            @pl.when(pos > 0)
            def _():
                sum_copy(way).wait_recv()
                sput[way] = spair[...] + sgot[way]

            @pl.when(pos < links - 1)
            def _():
                sum_copy(way).start()

    def sums_total():
        stot[...] = sput[0] + sput[1] - spair[...]
        total_copy.start()

    dx_at = [start + 2 * p for p in range(links - 1)] + [(links - 1) * pieces + 3]
    order = [sorted(range(links), key=lambda o, a=a: (abs(o - a), o)) for a in range(links)]

    def block_at(n, shift):
        p_is = [n == at + shift for at in dx_at]
        o = jnp.int32(0)
        for a in range(links):
            for p in range(links):
                o = jnp.where(p_is[p] & (c == a), order[a][p], o)
        hit = p_is[0]
        for one in p_is[1:]:
            hit = hit | one
        return hit, o

    def core_copy(o):
        return remote(
            dxb.at[o, 1 - core], dx1.at[o], dsend_sem.at[0], drecv_sem.at[0, o], core_dev
        )

    def across_copy(o):
        return remote(
            ds1.at[o, 1 - xx], dx2.at[o], dsend_sem.at[1], drecv_sem.at[1, o], x_dev
        )

    def home_copy(o):
        return remote(
            ds2.at[o, 1], dx3.at[o], dsend_sem.at[2], drecv_sem.at[2, o], y_dev
        )

    first_late = len([n for n in range(slots) if pieces <= n <= start and _is_lead(table, pieces, n)])

    def dx_steps(n):
        hit, o = block_at(n, 0)

        @pl.when(hit)
        def _():
            for way in (0, 1):
                @pl.when((position[way] == links - 1) & (o != c))
                def _():
                    def one(j, _):
                        arrived(way, wbuf, o, j)
                        return 0

                    lax.fori_loop(0, pieces, one, 0)

            group = next(k for k in (5, 4, 3, 2, 1) if (pieces - 1) % k == 0)

            def one(i, _):
                new = acc[...]
                for j in range(group):
                    at = 1 + group * i + j
                    new = new + ndot(cot[at], wbuf[o, at])
                acc[...] = new
                return 0

            acc[...] = ndot(cot[0], wbuf[o, 0])
            lax.fori_loop(0, (pieces - 1) // group, one, 0)
            for q in (0, 1):
                for i in range(n_tp):
                    at = (q * n_tp + i) * rows
                    dxb[o, i % 2, i // 2, q] = acc[at : at + rows].astype(BF)
            core_copy(o).start()

        hit1, o1 = block_at(n, 1)

        @pl.when(hit1)
        def _():
            core_copy(o1).wait_recv()
            ds1[o1] = (dxb[o1, core].astype(F32) + dx1[o1].astype(F32)).astype(BF)
            across_copy(o1).start()

        hit2, o2 = block_at(n, 3)

        @pl.when(hit2)
        def _():
            across_copy(o2).wait_recv()
            ds2[o2] = (ds1[o2, xx].astype(F32) + dx2[o2].astype(F32)).astype(BF)
            home_copy(o2).start()

    def final(j):
        fin[...] = part[c, j].astype(F32)
        for way in (0, 1):
            @pl.when(position[way] > 0)
            def _():
                arrived(way, rs[way], c, j)
                fin[...] += rs[way][c, j].astype(F32)
        at = lanes(j)
        gw[0, :, at] = fin[:, 0:LANES] * gs[:, at]
        gw[1, :, at] = fin[:, LANES : 2 * LANES] * vs[:, at]

    def results():
        for o in range(links):
            home_copy(o).wait_recv()
            for h in (0, 1):
                at = (2 * o + h) * own

                @pl.when(y == h)
                def _():
                    gi[:, at : at + own] = ds2[o, 0]

                @pl.when(y != h)
                def _():
                    gi[:, at : at + own] = dx3[o]

        total_copy.wait_recv()
        pair_copy().wait_send()
        for h in (0, 1):
            sown[:, part_of(h)] = jnp.where(y == h, stot[...], sall[...])
        total = sown[...]
        small[0:3] = total[0:3] * gs[...]
        small[3:6] = total[3:6] * vs[...]
        small[6:7] = jnp.sum(cg[...] * total[0:3], axis=0, keepdims=True)
        small[7:8] = jnp.sum(cv[...] * total[3:6], axis=0, keepdims=True)

    wait_y(0)
    partial(0)
    pair_copy().wait_recv()
    spair[...] = sown[:, part_of(y)] + sfrom[...]
    last = (links - 1) * pieces + 3

    def slot(n, _):
        for way in (0, 1):
            relay(way, n)
            sums_step(way, n)

        @pl.when(n == start)
        def _():
            for late in range(first_late, pieces):
                wait_y(late)

        k, j = decode(0, n + 1)

        @pl.when((k == 0) & (n + 1 < slots))
        def _():
            @pl.when(n < start)
            def _():
                wait_y(j)

            partial(j)

        dx_steps(n)

        @pl.when(n == pieces + (pieces - 1) * (links - 1))
        def _():
            sums_total()

        @pl.when(n >= last)
        def _():
            final(n - last)

        @pl.when(n == last + pieces - 3)
        def _():
            results()

        return 0

    lax.fori_loop(pieces, last + pieces, slot, 0)

    seven = xb.at[pl.ds(0, 7)]
    remote(seven, seven, xsend_sem.at[0], xrecv_sem.at[0], x_dev).wait_send()
    total_copy.wait_send()
    for ref, k in ((dx1, 0), (ds1.at[:, 0], 1), (dx3, 2)):
        remote(ref, ref, dsend_sem.at[k], drecv_sem.at[k, 0], y_dev).wait_send()
    for way in (0, 1):
        @pl.when(position[way] < links - 1)
        def _():
            sum_copy(way).wait_send()
            remote(wbuf, wbuf, z_sem.at[way], hop_sem.at[way, 0, 0], follower[way]).wait_send()
    mine = cot.at[:, pl.ds(0, tokens)]
    remote(mine, mine, ysend_sem.at[0], y_sem.at[0], y_dev).wait_send()


def _is_lead(table, pieces, n):
    m = n - pieces
    k = None
    for first, tick, low, count in table[0]:
        if m >= first:
            k = low + (m - first) % count
    return k == 0


def deliver(gi_in, gw_in, small, *refs):
    gi, gwg, gwv, ggs, gvs, gcg, gcv, sg, sv, tg, tv, sem = refs
    copies = []

    def send(src, dst):
        copies.append(pltpu.make_async_copy(src, dst, sem.at[len(copies)]))
        copies[-1].start()

    send(gw_in.at[0], gwg)
    send(gw_in.at[1], gwv)
    send(gi_in, gi)
    tg[...] = small[0:3]
    tv[...] = small[3:6]
    sg[...] = small[6:7].reshape(sg.shape)
    sv[...] = small[7:8].reshape(sv.shape)
    for src, dst in ((tg, gcg), (tv, gcv), (sg, ggs), (sv, gvs)):
        send(src, dst)
    for copy in copies:
        copy.wait()


def whole_kernel(n_fs, n_tp):
    links = n_fs // 2

    def on_device(inputs, w_gate, w_value, gate_scale, value_scale, conv_gate, conv_value,
                  gate_pre, value_pre, grad_out):
        rows, depth = inputs.shape
        own, columns = w_gate.shape
        tokens = gate_pre.shape[0]
        half = depth // 2
        pieces = columns // LANES
        anywhere = pl.BlockSpec(memory_space=pl.ANY)
        vmem = pl.BlockSpec(memory_space=pltpu.VMEM)
        dma, vm = pltpu.SemaphoreType.DMA, pltpu.VMEM
        wide = 2 * LANES
        span = (pieces + 1) // 2 * LANES
        outs = pl.pallas_call(
            functools.partial(fused, (n_fs, n_tp)),
            in_specs=[anywhere] * 10,
            out_specs=[vmem] * 3,
            out_shape=[
                vm((rows, depth), BF),
                vm((2, own, columns), F32),
                vm((8, columns), F32),
            ],
            scratch_shapes=[
                vm((2, own, columns), F32),
                vm((3, tokens, columns), BF),
                vm((links, pieces, own, wide), BF),
                vm((pieces, 2 * tokens, wide), BF),
                vm((links, pieces, own, wide), BF),
                vm((links, pieces, own, wide), BF),
                vm((links, pieces, own, wide), BF),
                vm((rows, depth), BF),
                vm((rows, half), BF),
                vm((2 * n_tp, rows, half), BF),
                vm((links, own, 2 * tokens), BF),
                vm((2 * tokens, own), F32),
                vm((links, 2, 2, 2, rows, own), BF),
                vm((links, 2, 2, rows, own), BF),
                vm((links, 2, 2, rows, own), BF),
                vm((links, 2, rows, own), BF),
                vm((links, 2, rows, own), BF),
                vm((links, rows, own), BF),
                vm((columns,), F32),
                vm((columns,), F32),
                vm((1, columns), F32),
                vm((1, columns), F32),
                vm((3, columns), F32),
                vm((3, columns), F32),
                vm((own, wide), F32),
                vm((8, columns), F32),
                vm((8, span), F32),
                vm((8, span), F32),
                vm((2, 8, span), F32),
                vm((2, 8, span), F32),
                vm((8, span), F32),
                vm((8, span), F32),
                dma((8,)),
                dma((2, links, (pieces + 1) // 2)),
                dma((2,)),
                dma((pieces,)),
                dma((1,)),
                dma((1,)),
                dma((4,)),
                dma((3,)),
                dma((3, links)),
                dma((4,)),
                dma((4,)),
            ],
            compiler_params=pltpu.CompilerParams(
                collective_id=0, has_side_effects=True, vmem_limit_bytes=52 * 2**20
            ),
        )(
            inputs, w_gate, w_value, gate_scale, value_scale, conv_gate, conv_value,
            gate_pre, value_pre, grad_out,
        )
        return pl.pallas_call(
            deliver,
            in_specs=[vmem] * 3,
            out_specs=[anywhere] * 7,
            out_shape=[
                jax.ShapeDtypeStruct((rows, depth), BF),
                jax.ShapeDtypeStruct((own, columns), F32),
                jax.ShapeDtypeStruct((own, columns), F32),
                jax.ShapeDtypeStruct((columns,), F32),
                jax.ShapeDtypeStruct((columns,), F32),
                jax.ShapeDtypeStruct((3, columns), F32),
                jax.ShapeDtypeStruct((3, columns), F32),
            ],
            scratch_shapes=[
                vm((columns,), F32),
                vm((columns,), F32),
                vm((3, columns), F32),
                vm((3, columns), F32),
                dma((7,)),
            ],
            compiler_params=pltpu.CompilerParams(vmem_limit_bytes=2 * 2**20),
        )(*outs)

    return on_device


def solution(mesh):
    placed = (
        P(("fs", "tp"), None),
        P("fs", "tp"),
        P("fs", "tp"),
        P("tp"),
        P("tp"),
        P(None, "tp"),
        P(None, "tp"),
        P("fs", "tp"),
        P("fs", "tp"),
        P("fs", "tp"),
    )
    body = make(mesh.shape["fs"], mesh.shape["tp"])

    given = (
        P(("fs", "tp"), None),
        P("fs", "tp"),
        P("fs", "tp"),
        P("tp"),
        P("tp"),
        P(None, "tp"),
        P(None, "tp"),
    )

    def spread(one):
        return jax.shard_map(one, mesh=mesh, in_specs=placed, out_specs=given, check_vma=False)

    step = spread(body)
    general = step
    n_fs, n_tp = mesh.shape["fs"], mesh.shape["tp"]
    fast = spread(whole_kernel(n_fs, n_tp))

    def pick(*args):
        columns = args[1].shape[1] // n_tp
        if n_tp == 4 and 2 < n_fs // 2 <= 4 and columns % LANES == 0:
            return fast(*args)
        return general(*args)

    return pick
```

```python
import functools

import jax
import jax.numpy as jnp
from jax import lax
from jax.experimental import pallas as pl
from jax.experimental.pallas import tpu as pltpu
from jax.sharding import PartitionSpec as P


BF = jnp.bfloat16
F32 = jnp.float32


LANES = 128


def elementwise(gs_ref, vs_ref, cg_ref, cv_ref, g_ref, v_ref, up_ref, gc_ref, vc_ref, s_ref):
    tokens = g_ref.shape[0]
    row = lax.broadcasted_iota(jnp.int32, g_ref.shape, 0)

    def down(x, k):
        return jnp.where(row >= k, pltpu.roll(x, k, 0), 0.0)

    def up(x, k):
        return jnp.where(row < tokens - k, pltpu.roll(x, tokens - k, 0), 0.0)

    def shifted(ref):
        x = ref[...].astype(F32)
        return down(x, 2), down(x, 1), x

    def conv(taps, xs):
        return taps[0:1] * xs[0] + taps[1:2] * xs[1] + taps[2:3] * xs[2]

    def back(taps, d):
        return (taps[2:3] * d + taps[1:2] * up(d, 1) + taps[0:1] * up(d, 2)).astype(BF)

    gs, vs = shifted(g_ref), shifted(v_ref)
    g = conv(cg_ref[...] * gs_ref[...], gs)
    v = conv(cv_ref[...] * vs_ref[...], vs)
    sig = 1.0 / (1.0 + jnp.exp(-g))
    base = up_ref[...].astype(F32) * sig
    d_gate = base * v * (1.0 + g * (1.0 - sig))
    d_value = base * g
    for j in range(3):
        s_ref[j : j + 1] = jnp.sum(d_gate * gs[j], axis=0, keepdims=True)
        s_ref[3 + j : 4 + j] = jnp.sum(d_value * vs[j], axis=0, keepdims=True)
    s_ref[6:8] = jnp.zeros((2, g_ref.shape[1]), F32)
    gc_ref[...] = back(cg_ref[...], d_gate)
    vc_ref[...] = back(cv_ref[...], d_value)


def cotangents(gs, vs, cg, cv, g, v, up):
    tokens, columns = g.shape
    big = pl.BlockSpec((tokens, LANES), lambda i: (0, i))

    def small(n):
        return pl.BlockSpec((n, LANES), lambda i: (0, i))

    return pl.pallas_call(
        elementwise,
        grid=(pl.cdiv(columns, LANES),),
        in_specs=[small(1), small(1), small(3), small(3), big, big, big],
        out_specs=[big, big, small(8)],
        out_shape=[jax.ShapeDtypeStruct(g.shape, BF)] * 2
        + [jax.ShapeDtypeStruct((8, columns), F32)],
        compiler_params=pltpu.CompilerParams(vmem_limit_bytes=24 * 2**20),
        cost_estimate=pl.CostEstimate(
            flops=g.size * 400, bytes_accessed=g.size * 10, transcendentals=g.size
        ),
    )(gs[None], vs[None], cg, cv, g, v, up)


def rescale(gs_ref, vs_ref, g_ref, v_ref, out_ref):
    out_ref[0] = (g_ref[...] * gs_ref[...]).astype(BF)
    out_ref[1] = (v_ref[...] * vs_ref[...]).astype(BF)


def scaled_weights(gs, vs, g, v):
    own, columns = g.shape
    parts = 4
    block = pl.BlockSpec((own // parts, columns), lambda i: (i, 0))
    scale = pl.BlockSpec((1, columns), lambda i: (0, 0))
    return pl.pallas_call(
        rescale,
        grid=(parts,),
        in_specs=[scale, scale, block, block],
        out_specs=pl.BlockSpec((2, own // parts, columns), lambda i: (0, i, 0)),
        out_shape=jax.ShapeDtypeStruct((2, own, columns), BF),
        compiler_params=pltpu.CompilerParams(vmem_limit_bytes=24 * 2**20),
        cost_estimate=pl.CostEstimate(
            flops=g.size * 100, bytes_accessed=g.size * 12, transcendentals=0
        ),
    )(gs[None], vs[None], g, v)


def tdot(a, b):
    return lax.dot_general(a, b, (((0,), (0,)), ((), ())), preferred_element_type=F32)


def ndot(a, b):
    return lax.dot_general(a, b, (((1,), (1,)), ((), ())), preferred_element_type=F32)


def make(n_fs, n_tp):
    links = n_fs // 2

    def on_device(
        inputs,
        w_gate,
        w_value,
        gate_scale,
        value_scale,
        conv_gate,
        conv_value,
        gate_pre,
        value_pre,
        grad_out,
    ):
        fs = lax.axis_index("fs")
        tp = lax.axis_index("tp")
        c, y = fs // 2, fs % 2
        rows, depth = inputs.shape
        own = w_gate.shape[0]
        half = depth // 2
        tokens, columns = gate_pre.shape

        def swap(x, axis, bit, n):
            return lax.ppermute(x, axis, [(i, i ^ bit) for i in range(n)])

        def chain(x, right, senders):
            step = 1 if right else -1
            pairs = [(2 * s + j, 2 * (s + step) + j) for s in senders for j in (0, 1)]
            return lax.ppermute(x, "fs", pairs)

        stacked = scaled_weights(gate_scale, value_scale, w_gate, w_value)
        rights, lefts = [], []
        r = l = stacked
        for s in range(links - 1):
            r = chain(r, True, range(s, links - 1))
            l = chain(l, False, range(1, links - s))
            rights.append(r)
            lefts.append(l)

        by_half = inputs.reshape(rows, links, 2, own)
        mine = lax.dynamic_index_in_dim(by_half, y, 2, keepdims=False)
        other = lax.dynamic_index_in_dim(by_half, 1 - y, 2, keepdims=False)
        mine, other = mine.reshape(rows, half), other.reshape(rows, half)
        other = swap(other, "fs", 1, n_fs)
        x = jnp.stack([mine, other])[:, None]
        bit = n_tp // 2
        while bit:
            got = swap(x, "tp", bit, n_tp)
            high = (tp // bit) % 2 == 1
            x = jnp.where(high, jnp.stack([got, x], 2), jnp.stack([x, got], 2))
            x = x.reshape(2, -1, rows, half)
            bit //= 2
        x = x.reshape(2, tokens, half)

        gate_cot, value_cot, sums = cotangents(
            gate_scale, value_scale, conv_gate, conv_value, gate_pre, value_pre, grad_out
        )
        bit = n_fs // 2
        while bit:
            sums = sums + swap(sums, "fs", bit, n_fs)
            bit //= 2

        gate_theirs = swap(gate_cot, "fs", 1, n_fs)
        value_theirs = swap(value_cot, "fs", 1, n_fs)
        pair = [(gate_cot, gate_theirs), (value_cot, value_theirs)]

        def at(blocks, i):
            return lax.dynamic_index_in_dim(
                blocks, jnp.clip(i, 0, links - 1), 0, keepdims=False
            )

        def collect(parts):
            r = l = None
            for t in range(links - 1):
                send_r = at(parts, links - 1 - t + c)
                send_l = at(parts, c - (links - 1 - t) + 0)
                if t:
                    send_r = (send_r.astype(F32) + r.astype(F32)).astype(BF)
                    send_l = (send_l.astype(F32) + l.astype(F32)).astype(BF)
                r = chain(send_r, True, range(0, t + 1))
                l = chain(send_l, False, range(links - 1 - t, links))
            total = at(parts, c).astype(F32)
            if r is not None:
                total = total + r.astype(F32) + l.astype(F32)
            return total

        grads = []
        for (cot, theirs), scale in zip(pair, (gate_scale, value_scale)):
            first = tdot(x[0], cot)
            parts = (first + tdot(x[1], theirs)).astype(BF)
            blocks = parts.reshape(links, own, columns)
            grads.append(collect(blocks) * scale)

        blocks = [stacked]
        for s in range(links - 1):
            blocks.append(jnp.where(c > s, rights[s], lefts[links - 2 - s]))
        columns_of = []
        for block in blocks:
            columns_of.append(
                [
                    (ndot(g, block[0]) + ndot(v, block[1])).astype(BF)
                    for g, v in zip(pair[0], pair[1])
                ]
            )
        part = jnp.stack([jnp.concatenate(t, 1) for t in zip(*columns_of)])
        part = part.reshape(2, n_tp, rows, half)
        bit = 1
        while bit < n_tp:
            split = part.reshape(2, -1, 2, rows, half)
            which = (tp // bit) % 2
            keep = lax.dynamic_index_in_dim(split, which, 2, keepdims=False)
            send = lax.dynamic_index_in_dim(split, 1 - which, 2, keepdims=False)
            got = swap(send, "tp", bit, n_tp)
            part = (keep.astype(F32) + got.astype(F32)).astype(BF)
            bit *= 2
        mine = part.reshape(2, rows, half)[0]
        other = swap(part.reshape(2, rows, half)[1], "fs", 1, n_fs)
        both = jnp.where(
            y == 0, jnp.stack([mine, other], 1), jnp.stack([other, mine], 1)
        ).reshape(rows, 2, links, own)
        order = (c - jnp.arange(links)) % links
        grad_inputs = jnp.take(both, order, axis=2).transpose(0, 2, 1, 3)
        return (
            grad_inputs.reshape(rows, depth),
            grads[0],
            grads[1],
            jnp.sum(conv_gate * sums[0:3], axis=0),
            jnp.sum(conv_value * sums[3:6], axis=0),
            sums[0:3] * gate_scale,
            sums[3:6] * value_scale,
        )

    return on_device


MESH = pl.DeviceIdType.MESH
SKEW = 4


def segments(links, pieces):
    table = []
    for pos in range(links - 1):
        reach = links - 1 - pos
        rows, count, last = [], 0, None
        for tick in range(pieces + SKEW * (reach - 1)):
            live = [k for k in range(reach) if 0 <= tick - SKEW * k < pieces]
            key = (live[0], len(live)) if live else None
            if key and key != last:
                rows.append((count, tick, live[0], len(live)))
            last = key
            count += len(live)
        table.append(rows)
    return table


def shares(pieces):
    body = pieces - 3
    relays = [(i, min(4, body - i)) for i in range(0, body, 4)] + [(body, 2), (pieces - 1, 1)]
    return relays, [(0, pieces - 5), (pieces - 5, 4), (pieces - 1, 1)]


def fused(dims, *refs):
    n_fs, n_tp = dims
    (
        inp, wg, wv, gs_in, vs_in, cg_in, cv_in, gp, vp, up,
        gi, gw, small,
        wraw, pre, wbuf, cot, part, rs0, rs1, xin, xs, xb, xt,
        acc, dxb, dx1, ds1, dx2, ds2, dx3, gs1, vs1, gs, vs, tap, sown, sfrom, spair, sgot, sput, stot, sall,
        load_sem, hop_sem, z_sem, y_sem, ysend_sem, xsend_sem, xrecv_sem,
        dsend_sem, drecv_sem, ssend_sem, srecv_sem,
    ) = refs
    rs = (rs0, rs1)
    links = n_fs // 2
    pieces = cot.shape[0]
    own = wg.shape[0]
    rows, _ = inp.shape
    tokens = gp.shape[0]
    slots = links * pieces

    fs = lax.axis_index("fs")
    tp = lax.axis_index("tp")
    c, y = lax.div(fs, 2), lax.rem(fs, 2)
    xx, core = lax.div(tp, 2), lax.rem(tp, 2)
    y_dev = (fs + 1 - 2 * y, tp)
    x_dev = (fs, tp + 2 - 4 * xx)
    core_dev = (fs, tp + 1 - 2 * core)
    x_tp = tp + 2 - 4 * xx
    position = (c, links - 1 - c)
    follower = ((fs + 2, tp), (fs - 2, tp))

    def real(way, index):
        return index if way == 0 else links - 1 - index

    def remote(src, dst, send, recv, device):
        return pltpu.make_async_remote_copy(
            src_ref=src, dst_ref=dst, send_sem=send, recv_sem=recv,
            device_id=device, device_id_type=MESH,
        )

    def lanes(j):
        return pl.ds(pl.multiple_of(j * LANES, LANES), LANES)

    def load(src, dst, k):
        copy = pltpu.make_async_copy(src, dst, load_sem.at[k])
        copy.start()
        return copy

    def loaded(ref, k):
        pltpu.make_async_copy(ref, ref, load_sem.at[k]).wait()

    head, rest = pl.ds(0, LANES), pl.ds(LANES, (pieces - 1) * LANES)
    scales = [load(gs_in, gs1, 4), load(vs_in, vs1, 5)]
    for at, k in ((head, 0), (rest, 1)):
        for i, w in enumerate((wg, wv)):
            load(w.at[:, at], wraw.at[i, :, at], k)
    load(inp, xin, 2)
    for i, a in enumerate((gp, vp, up)):
        load(a, pre.at[i], 3)
    load(cg_in, tap.at[0], 6)
    load(cv_in, tap.at[1], 6)
    cg, cv = tap.at[0], tap.at[1]

    barrier = pltpu.get_barrier_semaphore()
    for device in (y_dev, x_dev, core_dev):
        pl.semaphore_signal(barrier, inc=1, device_id=device, device_id_type=MESH)
    for way in (0, 1):
        @pl.when(position[way] < links - 1)
        def _():
            pl.semaphore_signal(barrier, inc=1, device_id=follower[way], device_id_type=MESH)
    relays, ends = shares(pieces)

    def index_in(groups, j):
        g = jnp.int32(0)
        for first, _ in groups[1:]:
            g = g + jnp.where(j >= first, 1, 0)
        return g

    def ag_sem(way, o, j):
        row = o if way == 0 else o - 1
        return hop_sem.at[way, row * len(relays) + index_in(relays, j)]

    def rs_sem(way, t, j, there):
        row = t - 1 if way == 0 else t
        relay_at = row * len(relays) + index_in(relays, j)
        end_at = (links - 1) * len(relays) + index_in(ends, j)
        return hop_sem.at[way, jnp.where(t == there, end_at, relay_at)]

    def ag_copy(way, o, j):
        return remote(
            wbuf.at[o, j], wbuf.at[o, j], z_sem.at[way], ag_sem(way, o, j), follower[way]
        )

    def rs_copy(way, src, t, j):
        there = c + 1 - 2 * way
        return remote(
            src.at[t, j], rs[way].at[t, j], z_sem.at[way], rs_sem(way, t, j, there), follower[way]
        )

    def arrived(way, ref, i, j, sem, groups=relays):
        for first, count in groups:
            @pl.when(j == first)
            def _():
                some = ref.at[i, pl.ds(first, count)]
                remote(some, some, z_sem.at[way], sem, follower[way]).wait_recv()

    def y_copy(j):
        return remote(
            cot.at[j, pl.ds(0, tokens)], cot.at[j, pl.ds(tokens, tokens)],
            ysend_sem.at[0], y_sem.at[j], y_dev,
        )

    for copy in scales:
        copy.wait()
    gs[...] = gs1[...].reshape(gs.shape)
    vs[...] = vs1[...].reshape(vs.shape)
    loaded(wraw.at[:, :, head], 0)

    def scaled(j):
        at = lanes(j)
        wbuf[c, j, :, 0:LANES] = (wraw[0, :, at] * gs[:, at]).astype(BF)
        wbuf[c, j, :, LANES : 2 * LANES] = (wraw[1, :, at] * vs[:, at]).astype(BF)

    def send_own(j):
        for way in (0, 1):
            @pl.when(position[way] < links - 1)
            def _():
                ag_copy(way, c, j).start()

    scaled(0)
    inner = jnp.where((c > 0) & (c < links - 1), 5, 4)
    pl.semaphore_wait(barrier, inner)

    def weights(j, _):
        scaled(j)
        send_own(j)
        return 0

    send_own(0)
    loaded(wraw.at[:, :, rest], 1)
    lax.fori_loop(1, pieces, weights, 0)

    loaded(xin, 2)
    for o in range(links):
        for h in (0, 1):
            block = xin[:, (2 * o + h) * own : (2 * o + h + 1) * own]

            @pl.when(y == h)
            def _():
                xb[tp, :, o * own : (o + 1) * own] = block

            @pl.when(y != h)
            def _():
                xs[:, o * own : (o + 1) * own] = block

    xy = remote(xs, xb.at[n_tp + tp], xsend_sem.at[0], xrecv_sem.at[0], y_dev)
    xy.start()
    xx0 = remote(xb.at[tp], xb.at[tp], xsend_sem.at[0], xrecv_sem.at[1], x_dev)
    xx0.start()
    xc0 = remote(xb.at[tp], xb.at[tp], xsend_sem.at[0], xrecv_sem.at[2], core_dev)
    xc0.start()

    loaded(pre, 3)
    loaded(tap, 6)

    row = lax.broadcasted_iota(jnp.int32, (tokens, LANES), 0)

    def down(a, k):
        return jnp.where(row >= k, pltpu.roll(a, k, 0), 0.0)

    def upward(a, k):
        return jnp.where(row < tokens - k, pltpu.roll(a, tokens - k, 0), 0.0)

    def elements(j, _):
        at = lanes(j)

        def shifted(i):
            a = pre[i, :, at].astype(F32)
            return down(a, 2), down(a, 1), a

        def conv(taps, a):
            return taps[0:1] * a[0] + taps[1:2] * a[1] + taps[2:3] * a[2]

        def back(taps, d):
            return (taps[2:3] * d + taps[1:2] * upward(d, 1) + taps[0:1] * upward(d, 2)).astype(BF)

        tg, tv = cg[:, at], cv[:, at]
        ga, va = shifted(0), shifted(1)
        g = conv(tg * gs[:, at], ga)
        v = conv(tv * vs[:, at], va)
        sig = 1.0 / (1.0 + jnp.exp(-g))
        base = pre[2, :, at].astype(F32) * sig
        d_gate = base * v * (1.0 + g * (1.0 - sig))
        d_value = base * g
        cot[j, 0:tokens, 0:LANES] = back(tg, d_gate)
        cot[j, 0:tokens, LANES : 2 * LANES] = back(tv, d_value)
        for k in range(3):
            sown[k : k + 1, at] = jnp.sum(d_gate * ga[k], axis=0, keepdims=True)
            sown[3 + k : 4 + k, at] = jnp.sum(d_value * va[k], axis=0, keepdims=True)
        sown[6:8, at] = jnp.zeros((2, LANES), F32)

        @pl.when(j < 2)
        def _():
            y_copy(j).start()

        return 0

    span = (pieces + 1) // 2 * LANES

    def part_of(which):
        return pl.ds(pl.multiple_of(which * (pieces * LANES - span), LANES), span)

    def pair_copy():
        return remote(
            sown.at[:, part_of(1 - y)], sfrom, ssend_sem.at[2], srecv_sem.at[2], y_dev
        )

    def send_y(j, _):
        y_copy(j).start()
        return 0

    lax.fori_loop(0, pieces, elements, 0)
    pair_copy().start()
    lax.fori_loop(2, pieces, send_y, 0)

    xy.wait_recv()
    xx1 = remote(xb.at[n_tp + tp], xb.at[n_tp + tp], xsend_sem.at[0], xrecv_sem.at[3], x_dev)
    xx1.start()
    xc1 = remote(xb.at[n_tp + tp], xb.at[n_tp + tp], xsend_sem.at[0], xrecv_sem.at[2], core_dev)
    xc1.start()
    xx0.wait_recv()
    xc2 = remote(xb.at[x_tp], xb.at[x_tp], xsend_sem.at[0], xrecv_sem.at[2], core_dev)
    xc2.start()
    xx1.wait_recv()
    xc3 = remote(xb.at[n_tp + x_tp], xb.at[n_tp + x_tp], xsend_sem.at[0], xrecv_sem.at[2], core_dev)
    xc3.start()
    four = xb.at[pl.ds(0, 4)]
    remote(four, four, xsend_sem.at[0], xrecv_sem.at[2], core_dev).wait_recv()
    for q in (0, 1):
        for i in range(n_tp):
            for o in range(links):
                at = (q * n_tp + i) * rows
                xt[o, :, at : at + rows] = xb[q * n_tp + i, :, o * own : (o + 1) * own].T

    def wait_y(j):
        y_copy(j).wait_recv()

    def partial(j):
        def one(o, _):
            part[o, j] = jnp.dot(xt[o], cot[j], preferred_element_type=F32).astype(BF)
            return 0

        lax.fori_loop(0, links, one, 0)

    table = segments(links, pieces)

    def decode(p, n):
        m = n - pieces * (p + 1)
        k, j = jnp.int32(0), jnp.int32(0)
        for first, tick, low, count in table[p]:
            q = lax.div(m - first, count)
            kk = low + (m - first) - q * count
            here = m >= first
            k = jnp.where(here, kk, k)
            j = jnp.where(here, tick + q - SKEW * kk, j)
        return k, j

    def relay(way, n):
        pos = position[way]

        @pl.when((pos < links - 1) & (n < pieces * (pos + 1)))
        def _():
            q = lax.div(n, pieces)
            j = n - q * pieces
            o = real(way, pos - q)
            arrived(way, wbuf, o, j, ag_sem(way, o, j))
            ag_copy(way, o, j).start()

        @pl.when((pos < links - 1) & (n >= pieces * (pos + 1)) & (n < slots))
        def _():
            k, j = decode(0, n)
            for p in range(1, links - 1):
                kp, jp = decode(p, n)
                k, j = jnp.where(pos == p, kp, k), jnp.where(pos == p, jp, j)
            t = real(way, links - 1 - k)

            @pl.when(pos == 0)
            def _():
                rs_copy(way, part, t, j).start()

            @pl.when(pos > 0)
            def _():
                arrived(way, rs[way], t, j, rs_sem(way, t, j, c))
                rs[way][t, j] = (rs[way][t, j].astype(F32) + part[t, j].astype(F32)).astype(BF)
                rs_copy(way, rs[way], t, j).start()

    start = (8 * pieces) // 3

    def sum_copy(way):
        return remote(
            sput.at[way], sgot.at[way], ssend_sem.at[way], srecv_sem.at[way], follower[way]
        )

    total_copy = remote(stot, sall, ssend_sem.at[3], srecv_sem.at[3], y_dev)

    def sums_step(way, n):
        pos = position[way]

        @pl.when(n == pieces + (pieces - 1) * pos)
        def _():
            @pl.when(pos == 0)
            def _():
                sput[way] = spair[...]

            @pl.when(pos > 0)
            def _():
                sum_copy(way).wait_recv()
                sput[way] = spair[...] + sgot[way]

            @pl.when(pos < links - 1)
            def _():
                sum_copy(way).start()

    def sums_total():
        stot[...] = sput[0] + sput[1] - spair[...]
        total_copy.start()

    dx_at = [start + 2 * p for p in range(links - 1)] + [(links - 1) * pieces + 3]
    order = [sorted(range(links), key=lambda o, a=a: (abs(o - a), o)) for a in range(links)]

    def block_at(n, shift):
        p_is = [n == at + shift for at in dx_at]
        o = jnp.int32(0)
        for a in range(links):
            for p in range(links):
                o = jnp.where(p_is[p] & (c == a), order[a][p], o)
        hit = p_is[0]
        for one in p_is[1:]:
            hit = hit | one
        return hit, o

    def core_copy(o):
        return remote(
            dxb.at[o, 1 - core], dx1.at[o], dsend_sem.at[0], drecv_sem.at[0, o], core_dev
        )

    def across_copy(o):
        return remote(
            ds1.at[o, 1 - xx], dx2.at[o], dsend_sem.at[1], drecv_sem.at[1, o], x_dev
        )

    def home_copy(o):
        return remote(
            ds2.at[o, 1], dx3.at[o], dsend_sem.at[2], drecv_sem.at[2, o], y_dev
        )

    first_late = len([n for n in range(slots) if pieces <= n <= start and _is_lead(table, pieces, n)])

    def dx_steps(n):
        hit, o = block_at(n, 0)

        @pl.when(hit)
        def _():
            for way in (0, 1):
                @pl.when((position[way] == links - 1) & (o != c))
                def _():
                    def one(j, _):
                        arrived(way, wbuf, o, j, ag_sem(way, o, j))
                        return 0

                    lax.fori_loop(0, pieces, one, 0)

            group = next(k for k in (5, 4, 3, 2, 1) if (pieces - 1) % k == 0)

            def one(i, _):
                new = acc[...]
                for j in range(group):
                    at = 1 + group * i + j
                    new = new + ndot(cot[at], wbuf[o, at])
                acc[...] = new
                return 0

            acc[...] = ndot(cot[0], wbuf[o, 0])
            lax.fori_loop(0, (pieces - 1) // group, one, 0)
            for q in (0, 1):
                for i in range(n_tp):
                    at = (q * n_tp + i) * rows
                    dxb[o, i % 2, i // 2, q] = acc[at : at + rows].astype(BF)
            core_copy(o).start()

        hit1, o1 = block_at(n, 1)

        @pl.when(hit1)
        def _():
            core_copy(o1).wait_recv()
            ds1[o1] = (dxb[o1, core].astype(F32) + dx1[o1].astype(F32)).astype(BF)
            across_copy(o1).start()

        hit2, o2 = block_at(n, 3)

        @pl.when(hit2)
        def _():
            across_copy(o2).wait_recv()
            ds2[o2] = (ds1[o2, xx].astype(F32) + dx2[o2].astype(F32)).astype(BF)
            home_copy(o2).start()

    def final(j):
        for way in (0, 1):
            @pl.when(position[way] > 0)
            def _():
                arrived(way, rs[way], c, j, rs_sem(way, c, j, c), ends)
        at = lanes(j)

        def close(ways):
            total = part[c, j].astype(F32)
            for way in ways:
                total = total + rs[way][c, j].astype(F32)
            gw[0, :, at] = total[:, 0:LANES] * gs[:, at]
            gw[1, :, at] = total[:, LANES : 2 * LANES] * vs[:, at]

        pl.when((c > 0) & (c < links - 1))(lambda: close((0, 1)))
        pl.when(c == links - 1)(lambda: close((0,)))
        pl.when(c == 0)(lambda: close((1,)))

    def results():
        for o in range(links):
            home_copy(o).wait_recv()
            for h in (0, 1):
                at = (2 * o + h) * own

                @pl.when(y == h)
                def _():
                    gi[:, at : at + own] = ds2[o, 0]

                @pl.when(y != h)
                def _():
                    gi[:, at : at + own] = dx3[o]

        total_copy.wait_recv()
        pair_copy().wait_send()
        for h in (0, 1):
            sown[:, part_of(h)] = jnp.where(y == h, stot[...], sall[...])
        total = sown[...]
        small[0:3] = total[0:3] * gs[...]
        small[3:6] = total[3:6] * vs[...]
        small[6:7] = jnp.sum(cg[...] * total[0:3], axis=0, keepdims=True)
        small[7:8] = jnp.sum(cv[...] * total[3:6], axis=0, keepdims=True)

    wait_y(0)
    partial(0)
    pair_copy().wait_recv()
    spair[...] = sown[:, part_of(y)] + sfrom[...]
    last = slots - 3

    def slot(n, _):
        for way in (0, 1):
            relay(way, n)
            sums_step(way, n)

        @pl.when(n == start)
        def _():
            for late in range(first_late, pieces):
                wait_y(late)

        k, j = decode(0, n + 1)

        @pl.when((k == 0) & (n + 1 < slots))
        def _():
            @pl.when(n < start)
            def _():
                wait_y(j)

            partial(j)

        dx_steps(n)

        @pl.when(n == pieces + (pieces - 1) * (links - 1))
        def _():
            sums_total()

        @pl.when(n == last + pieces - 5)
        def _():
            results()

        @pl.when(n >= last)
        def _():
            final(n - last)

        return 0

    lax.fori_loop(pieces, last + pieces, slot, 0)

    seven = xb.at[pl.ds(0, 7)]
    remote(seven, seven, xsend_sem.at[0], xrecv_sem.at[0], x_dev).wait_send()
    total_copy.wait_send()
    for ref, k in ((dx1, 0), (ds1.at[:, 0], 1), (dx3, 2)):
        remote(ref, ref, dsend_sem.at[k], drecv_sem.at[k, 0], y_dev).wait_send()
    for way in (0, 1):
        @pl.when(position[way] < links - 1)
        def _():
            sum_copy(way).wait_send()
            remote(wbuf, wbuf, z_sem.at[way], hop_sem.at[way, 0], follower[way]).wait_send()
    mine = cot.at[:, pl.ds(0, tokens)]
    remote(mine, mine, ysend_sem.at[0], y_sem.at[0], y_dev).wait_send()


def _is_lead(table, pieces, n):
    m = n - pieces
    k = None
    for first, tick, low, count in table[0]:
        if m >= first:
            k = low + (m - first) % count
    return k == 0


def deliver(gi_in, gw_in, small, *refs):
    gi, gwg, gwv, ggs, gvs, gcg, gcv, sg, sv, tg, tv, sem = refs
    copies = []

    def send(src, dst):
        copies.append(pltpu.make_async_copy(src, dst, sem.at[len(copies)]))
        copies[-1].start()

    send(gw_in.at[0], gwg)
    send(gw_in.at[1], gwv)
    send(gi_in, gi)
    tg[...] = small[0:3]
    tv[...] = small[3:6]
    sg[...] = small[6:7].reshape(sg.shape)
    sv[...] = small[7:8].reshape(sv.shape)
    for src, dst in ((tg, gcg), (tv, gcv), (sg, ggs), (sv, gvs)):
        send(src, dst)
    for copy in copies:
        copy.wait()


def whole_kernel(n_fs, n_tp):
    links = n_fs // 2

    def on_device(inputs, w_gate, w_value, gate_scale, value_scale, conv_gate, conv_value,
                  gate_pre, value_pre, grad_out):
        rows, depth = inputs.shape
        own, columns = w_gate.shape
        tokens = gate_pre.shape[0]
        half = depth // 2
        pieces = columns // LANES
        anywhere = pl.BlockSpec(memory_space=pl.ANY)
        vmem = pl.BlockSpec(memory_space=pltpu.VMEM)
        dma, vm = pltpu.SemaphoreType.DMA, pltpu.VMEM
        wide = 2 * LANES
        span = (pieces + 1) // 2 * LANES
        outs = pl.pallas_call(
            functools.partial(fused, (n_fs, n_tp)),
            in_specs=[anywhere] * 10,
            out_specs=[vmem] * 3,
            out_shape=[
                vm((rows, depth), BF),
                vm((2, own, columns), F32),
                vm((8, columns), F32),
            ],
            scratch_shapes=[
                vm((2, own, columns), F32),
                vm((3, tokens, columns), BF),
                vm((links, pieces, own, wide), BF),
                vm((pieces, 2 * tokens, wide), BF),
                vm((links, pieces, own, wide), BF),
                vm((links, pieces, own, wide), BF),
                vm((links, pieces, own, wide), BF),
                vm((rows, depth), BF),
                vm((rows, half), BF),
                vm((2 * n_tp, rows, half), BF),
                vm((links, own, 2 * tokens), BF),
                vm((2 * tokens, own), F32),
                vm((links, 2, 2, 2, rows, own), BF),
                vm((links, 2, 2, rows, own), BF),
                vm((links, 2, 2, rows, own), BF),
                vm((links, 2, rows, own), BF),
                vm((links, 2, rows, own), BF),
                vm((links, rows, own), BF),
                vm((columns,), F32),
                vm((columns,), F32),
                vm((1, columns), F32),
                vm((1, columns), F32),
                vm((2, 3, columns), F32),
                vm((8, columns), F32),
                vm((8, span), F32),
                vm((8, span), F32),
                vm((2, 8, span), F32),
                vm((2, 8, span), F32),
                vm((8, span), F32),
                vm((8, span), F32),
                dma((7,)),
                dma((2, (links - 1) * len(shares(pieces)[0]) + len(shares(pieces)[1]))),
                dma((2,)),
                dma((pieces,)),
                dma((1,)),
                dma((1,)),
                dma((4,)),
                dma((3,)),
                dma((3, links)),
                dma((4,)),
                dma((4,)),
            ],
            compiler_params=pltpu.CompilerParams(
                collective_id=0, has_side_effects=True, vmem_limit_bytes=52 * 2**20
            ),
        )(
            inputs, w_gate, w_value, gate_scale, value_scale, conv_gate, conv_value,
            gate_pre, value_pre, grad_out,
        )
        return pl.pallas_call(
            deliver,
            in_specs=[vmem] * 3,
            out_specs=[anywhere] * 7,
            out_shape=[
                jax.ShapeDtypeStruct((rows, depth), BF),
                jax.ShapeDtypeStruct((own, columns), F32),
                jax.ShapeDtypeStruct((own, columns), F32),
                jax.ShapeDtypeStruct((columns,), F32),
                jax.ShapeDtypeStruct((columns,), F32),
                jax.ShapeDtypeStruct((3, columns), F32),
                jax.ShapeDtypeStruct((3, columns), F32),
            ],
            scratch_shapes=[
                vm((columns,), F32),
                vm((columns,), F32),
                vm((3, columns), F32),
                vm((3, columns), F32),
                dma((7,)),
            ],
            compiler_params=pltpu.CompilerParams(vmem_limit_bytes=2 * 2**20),
        )(*outs)

    return on_device


def solution(mesh):
    placed = (
        P(("fs", "tp"), None),
        P("fs", "tp"),
        P("fs", "tp"),
        P("tp"),
        P("tp"),
        P(None, "tp"),
        P(None, "tp"),
        P("fs", "tp"),
        P("fs", "tp"),
        P("fs", "tp"),
    )
    body = make(mesh.shape["fs"], mesh.shape["tp"])

    given = (
        P(("fs", "tp"), None),
        P("fs", "tp"),
        P("fs", "tp"),
        P("tp"),
        P("tp"),
        P(None, "tp"),
        P(None, "tp"),
    )

    def spread(one):
        return jax.shard_map(one, mesh=mesh, in_specs=placed, out_specs=given, check_vma=False)

    step = spread(body)
    general = step
    n_fs, n_tp = mesh.shape["fs"], mesh.shape["tp"]
    fast = spread(whole_kernel(n_fs, n_tp))

    def pick(*args):
        columns = args[1].shape[1] // n_tp
        if n_tp == 4 and 2 < n_fs // 2 <= 4 and columns % LANES == 0 and columns >= 8 * LANES:
            return fast(*args)
        return general(*args)

    return pick
```

```python
import functools

import jax
import jax.numpy as jnp
from jax import lax
from jax.experimental import pallas as pl
from jax.experimental.pallas import tpu as pltpu
from jax.sharding import PartitionSpec as P


BF = jnp.bfloat16
F32 = jnp.float32


LANES = 128


def elementwise(gs_ref, vs_ref, cg_ref, cv_ref, g_ref, v_ref, up_ref, gc_ref, vc_ref, s_ref):
    tokens = g_ref.shape[0]
    row = lax.broadcasted_iota(jnp.int32, g_ref.shape, 0)

    def down(x, k):
        return jnp.where(row >= k, pltpu.roll(x, k, 0), 0.0)

    def up(x, k):
        return jnp.where(row < tokens - k, pltpu.roll(x, tokens - k, 0), 0.0)

    def shifted(ref):
        x = ref[...].astype(F32)
        return down(x, 2), down(x, 1), x

    def conv(taps, xs):
        return taps[0:1] * xs[0] + taps[1:2] * xs[1] + taps[2:3] * xs[2]

    def back(taps, d):
        return (taps[2:3] * d + taps[1:2] * up(d, 1) + taps[0:1] * up(d, 2)).astype(BF)

    gs, vs = shifted(g_ref), shifted(v_ref)
    g = conv(cg_ref[...] * gs_ref[...], gs)
    v = conv(cv_ref[...] * vs_ref[...], vs)
    sig = 1.0 / (1.0 + jnp.exp(-g))
    base = up_ref[...].astype(F32) * sig
    d_gate = base * v * (1.0 + g * (1.0 - sig))
    d_value = base * g
    for j in range(3):
        s_ref[j : j + 1] = jnp.sum(d_gate * gs[j], axis=0, keepdims=True)
        s_ref[3 + j : 4 + j] = jnp.sum(d_value * vs[j], axis=0, keepdims=True)
    s_ref[6:8] = jnp.zeros((2, g_ref.shape[1]), F32)
    gc_ref[...] = back(cg_ref[...], d_gate)
    vc_ref[...] = back(cv_ref[...], d_value)


def cotangents(gs, vs, cg, cv, g, v, up):
    tokens, columns = g.shape
    big = pl.BlockSpec((tokens, LANES), lambda i: (0, i))

    def small(n):
        return pl.BlockSpec((n, LANES), lambda i: (0, i))

    return pl.pallas_call(
        elementwise,
        grid=(pl.cdiv(columns, LANES),),
        in_specs=[small(1), small(1), small(3), small(3), big, big, big],
        out_specs=[big, big, small(8)],
        out_shape=[jax.ShapeDtypeStruct(g.shape, BF)] * 2
        + [jax.ShapeDtypeStruct((8, columns), F32)],
        compiler_params=pltpu.CompilerParams(vmem_limit_bytes=24 * 2**20),
        cost_estimate=pl.CostEstimate(
            flops=g.size * 400, bytes_accessed=g.size * 10, transcendentals=g.size
        ),
    )(gs[None], vs[None], cg, cv, g, v, up)


def rescale(gs_ref, vs_ref, g_ref, v_ref, out_ref):
    out_ref[0] = (g_ref[...] * gs_ref[...]).astype(BF)
    out_ref[1] = (v_ref[...] * vs_ref[...]).astype(BF)


def scaled_weights(gs, vs, g, v):
    own, columns = g.shape
    parts = 4
    block = pl.BlockSpec((own // parts, columns), lambda i: (i, 0))
    scale = pl.BlockSpec((1, columns), lambda i: (0, 0))
    return pl.pallas_call(
        rescale,
        grid=(parts,),
        in_specs=[scale, scale, block, block],
        out_specs=pl.BlockSpec((2, own // parts, columns), lambda i: (0, i, 0)),
        out_shape=jax.ShapeDtypeStruct((2, own, columns), BF),
        compiler_params=pltpu.CompilerParams(vmem_limit_bytes=24 * 2**20),
        cost_estimate=pl.CostEstimate(
            flops=g.size * 100, bytes_accessed=g.size * 12, transcendentals=0
        ),
    )(gs[None], vs[None], g, v)


def tdot(a, b):
    return lax.dot_general(a, b, (((0,), (0,)), ((), ())), preferred_element_type=F32)


def ndot(a, b):
    return lax.dot_general(a, b, (((1,), (1,)), ((), ())), preferred_element_type=F32)


def make(n_fs, n_tp):
    links = n_fs // 2

    def on_device(
        inputs,
        w_gate,
        w_value,
        gate_scale,
        value_scale,
        conv_gate,
        conv_value,
        gate_pre,
        value_pre,
        grad_out,
    ):
        fs = lax.axis_index("fs")
        tp = lax.axis_index("tp")
        c, y = fs // 2, fs % 2
        rows, depth = inputs.shape
        own = w_gate.shape[0]
        half = depth // 2
        tokens, columns = gate_pre.shape

        def swap(x, axis, bit, n):
            return lax.ppermute(x, axis, [(i, i ^ bit) for i in range(n)])

        def chain(x, right, senders):
            step = 1 if right else -1
            pairs = [(2 * s + j, 2 * (s + step) + j) for s in senders for j in (0, 1)]
            return lax.ppermute(x, "fs", pairs)

        stacked = scaled_weights(gate_scale, value_scale, w_gate, w_value)
        rights, lefts = [], []
        r = l = stacked
        for s in range(links - 1):
            r = chain(r, True, range(s, links - 1))
            l = chain(l, False, range(1, links - s))
            rights.append(r)
            lefts.append(l)

        by_half = inputs.reshape(rows, links, 2, own)
        mine = lax.dynamic_index_in_dim(by_half, y, 2, keepdims=False)
        other = lax.dynamic_index_in_dim(by_half, 1 - y, 2, keepdims=False)
        mine, other = mine.reshape(rows, half), other.reshape(rows, half)
        other = swap(other, "fs", 1, n_fs)
        x = jnp.stack([mine, other])[:, None]
        bit = n_tp // 2
        while bit:
            got = swap(x, "tp", bit, n_tp)
            high = (tp // bit) % 2 == 1
            x = jnp.where(high, jnp.stack([got, x], 2), jnp.stack([x, got], 2))
            x = x.reshape(2, -1, rows, half)
            bit //= 2
        x = x.reshape(2, tokens, half)

        gate_cot, value_cot, sums = cotangents(
            gate_scale, value_scale, conv_gate, conv_value, gate_pre, value_pre, grad_out
        )
        bit = n_fs // 2
        while bit:
            sums = sums + swap(sums, "fs", bit, n_fs)
            bit //= 2

        gate_theirs = swap(gate_cot, "fs", 1, n_fs)
        value_theirs = swap(value_cot, "fs", 1, n_fs)
        pair = [(gate_cot, gate_theirs), (value_cot, value_theirs)]

        def at(blocks, i):
            return lax.dynamic_index_in_dim(
                blocks, jnp.clip(i, 0, links - 1), 0, keepdims=False
            )

        def collect(parts):
            r = l = None
            for t in range(links - 1):
                send_r = at(parts, links - 1 - t + c)
                send_l = at(parts, c - (links - 1 - t) + 0)
                if t:
                    send_r = (send_r.astype(F32) + r.astype(F32)).astype(BF)
                    send_l = (send_l.astype(F32) + l.astype(F32)).astype(BF)
                r = chain(send_r, True, range(0, t + 1))
                l = chain(send_l, False, range(links - 1 - t, links))
            total = at(parts, c).astype(F32)
            if r is not None:
                total = total + r.astype(F32) + l.astype(F32)
            return total

        grads = []
        for (cot, theirs), scale in zip(pair, (gate_scale, value_scale)):
            first = tdot(x[0], cot)
            parts = (first + tdot(x[1], theirs)).astype(BF)
            blocks = parts.reshape(links, own, columns)
            grads.append(collect(blocks) * scale)

        blocks = [stacked]
        for s in range(links - 1):
            blocks.append(jnp.where(c > s, rights[s], lefts[links - 2 - s]))
        columns_of = []
        for block in blocks:
            columns_of.append(
                [
                    (ndot(g, block[0]) + ndot(v, block[1])).astype(BF)
                    for g, v in zip(pair[0], pair[1])
                ]
            )
        part = jnp.stack([jnp.concatenate(t, 1) for t in zip(*columns_of)])
        part = part.reshape(2, n_tp, rows, half)
        bit = 1
        while bit < n_tp:
            split = part.reshape(2, -1, 2, rows, half)
            which = (tp // bit) % 2
            keep = lax.dynamic_index_in_dim(split, which, 2, keepdims=False)
            send = lax.dynamic_index_in_dim(split, 1 - which, 2, keepdims=False)
            got = swap(send, "tp", bit, n_tp)
            part = (keep.astype(F32) + got.astype(F32)).astype(BF)
            bit *= 2
        mine = part.reshape(2, rows, half)[0]
        other = swap(part.reshape(2, rows, half)[1], "fs", 1, n_fs)
        both = jnp.where(
            y == 0, jnp.stack([mine, other], 1), jnp.stack([other, mine], 1)
        ).reshape(rows, 2, links, own)
        order = (c - jnp.arange(links)) % links
        grad_inputs = jnp.take(both, order, axis=2).transpose(0, 2, 1, 3)
        return (
            grad_inputs.reshape(rows, depth),
            grads[0],
            grads[1],
            jnp.sum(conv_gate * sums[0:3], axis=0),
            jnp.sum(conv_value * sums[3:6], axis=0),
            sums[0:3] * gate_scale,
            sums[3:6] * value_scale,
        )

    return on_device


MESH = pl.DeviceIdType.MESH
SKEW = 4


def segments(links, pieces):
    table = []
    for pos in range(links - 1):
        reach = links - 1 - pos
        rows, count, last = [], 0, None
        for tick in range(pieces + SKEW * (reach - 1)):
            live = [k for k in range(reach) if 0 <= tick - SKEW * k < pieces]
            key = (live[0], len(live)) if live else None
            if key and key != last:
                rows.append((count, tick, live[0], len(live)))
            last = key
            count += len(live)
        table.append(rows)
    return table


def shares(pieces):
    body = pieces - 3
    relays = [(i, min(4, body - i)) for i in range(0, body, 4)] + [(body, 2), (pieces - 1, 1)]
    return relays, [(0, pieces - 5), (pieces - 5, 4), (pieces - 1, 1)]


def fused(dims, *refs):
    n_fs, n_tp = dims
    (
        inp, wg, wv, gs_in, vs_in, cg_in, cv_in, gp, vp, up,
        gi, gw, small,
        wraw, pre, wbuf, cot, part, rs0, rs1, xin, xs, xb, xt,
        acc, dxb, dx1, ds1, dx2, ds2, dx3, gs1, vs1, gs, vs, tap, sown, sfrom, spair, sgot, sput, stot, sall,
        load_sem, hop_sem, z_sem, y_sem, ysend_sem, xsend_sem, xrecv_sem,
        dsend_sem, drecv_sem, ssend_sem, srecv_sem,
    ) = refs
    rs = (rs0, rs1)
    links = n_fs // 2
    pieces = cot.shape[0]
    own = wg.shape[0]
    rows, _ = inp.shape
    tokens = gp.shape[0]
    slots = links * pieces

    fs = lax.axis_index("fs")
    tp = lax.axis_index("tp")
    c, y = lax.div(fs, 2), lax.rem(fs, 2)
    xx, core = lax.div(tp, 2), lax.rem(tp, 2)
    y_dev = (fs + 1 - 2 * y, tp)
    x_dev = (fs, tp + 2 - 4 * xx)
    core_dev = (fs, tp + 1 - 2 * core)
    x_tp = tp + 2 - 4 * xx
    position = (c, links - 1 - c)
    follower = ((fs + 2, tp), (fs - 2, tp))

    def real(way, index):
        return index if way == 0 else links - 1 - index

    def remote(src, dst, send, recv, device):
        return pltpu.make_async_remote_copy(
            src_ref=src, dst_ref=dst, send_sem=send, recv_sem=recv,
            device_id=device, device_id_type=MESH,
        )

    def lanes(j):
        return pl.ds(pl.multiple_of(j * LANES, LANES), LANES)

    def load(src, dst, k):
        copy = pltpu.make_async_copy(src, dst, load_sem.at[k])
        copy.start()
        return copy

    def loaded(ref, k):
        pltpu.make_async_copy(ref, ref, load_sem.at[k]).wait()

    head, rest = pl.ds(0, LANES), pl.ds(LANES, (pieces - 1) * LANES)
    scales = [load(gs_in, gs1, 4), load(vs_in, vs1, 5)]
    for at, k in ((head, 0), (rest, 1)):
        for i, w in enumerate((wg, wv)):
            load(w.at[:, at], wraw.at[i, :, at], k)
    load(inp, xin, 2)
    for i, a in enumerate((gp, vp, up)):
        load(a, pre.at[i], 3)
    load(cg_in, tap.at[0], 6)
    load(cv_in, tap.at[1], 6)
    cg, cv = tap.at[0], tap.at[1]

    barrier = pltpu.get_barrier_semaphore()
    for device in (y_dev, x_dev, core_dev):
        pl.semaphore_signal(barrier, inc=1, device_id=device, device_id_type=MESH)
    for way in (0, 1):
        @pl.when(position[way] < links - 1)
        def _():
            pl.semaphore_signal(barrier, inc=1, device_id=follower[way], device_id_type=MESH)
    relays, ends = shares(pieces)

    def index_in(groups, j):
        g = jnp.int32(0)
        for first, _ in groups[1:]:
            g = g + jnp.where(j >= first, 1, 0)
        return g

    def ag_sem(way, o, j):
        row = o if way == 0 else o - 1
        return hop_sem.at[way, row * len(relays) + index_in(relays, j)]

    def rs_sem(way, t, j, there):
        row = t - 1 if way == 0 else t
        relay_at = row * len(relays) + index_in(relays, j)
        end_at = (links - 1) * len(relays) + index_in(ends, j)
        return hop_sem.at[way, jnp.where(t == there, end_at, relay_at)]

    def ag_copy(way, o, j):
        return remote(
            wbuf.at[o, j], wbuf.at[o, j], z_sem.at[way], ag_sem(way, o, j), follower[way]
        )

    def rs_copy(way, src, t, j):
        there = c + 1 - 2 * way
        return remote(
            src.at[t, j], rs[way].at[t, j], z_sem.at[way], rs_sem(way, t, j, there), follower[way]
        )

    def arrived(way, ref, i, j, sem, groups=relays):
        for first, count in groups:
            @pl.when(j == first)
            def _():
                some = ref.at[i, pl.ds(first, count)]
                remote(some, some, z_sem.at[way], sem, follower[way]).wait_recv()

    def y_copy(j):
        return remote(
            cot.at[j, pl.ds(0, tokens)], cot.at[j, pl.ds(tokens, tokens)],
            ysend_sem.at[0], y_sem.at[j], y_dev,
        )

    for copy in scales:
        copy.wait()
    gs[...] = gs1[...].reshape(gs.shape)
    vs[...] = vs1[...].reshape(vs.shape)
    loaded(wraw.at[:, :, head], 0)

    def scaled(j):
        at = lanes(j)
        wbuf[c, j, :, 0:LANES] = (wraw[0, :, at] * gs[:, at]).astype(BF)
        wbuf[c, j, :, LANES : 2 * LANES] = (wraw[1, :, at] * vs[:, at]).astype(BF)

    def send_own(j):
        for way in (0, 1):
            @pl.when(position[way] < links - 1)
            def _():
                ag_copy(way, c, j).start()

    scaled(0)
    inner = jnp.where((c > 0) & (c < links - 1), 5, 4)
    pl.semaphore_wait(barrier, inner)

    def weights(j, _):
        scaled(j)
        send_own(j)
        return 0

    send_own(0)
    loaded(wraw.at[:, :, rest], 1)
    lax.fori_loop(1, pieces, weights, 0)

    loaded(xin, 2)
    for o in range(links):
        for h in (0, 1):
            block = xin[:, (2 * o + h) * own : (2 * o + h + 1) * own]

            @pl.when(y == h)
            def _():
                xb[tp, :, o * own : (o + 1) * own] = block

            @pl.when(y != h)
            def _():
                xs[:, o * own : (o + 1) * own] = block

    xy = remote(xs, xb.at[n_tp + tp], xsend_sem.at[0], xrecv_sem.at[0], y_dev)
    xy.start()
    xx0 = remote(xb.at[tp], xb.at[tp], xsend_sem.at[0], xrecv_sem.at[1], x_dev)
    xx0.start()
    xc0 = remote(xb.at[tp], xb.at[tp], xsend_sem.at[0], xrecv_sem.at[2], core_dev)
    xc0.start()

    loaded(pre, 3)
    loaded(tap, 6)

    row = lax.broadcasted_iota(jnp.int32, (tokens, LANES), 0)

    def down(a, k):
        return jnp.where(row >= k, pltpu.roll(a, k, 0), 0.0)

    def upward(a, k):
        return jnp.where(row < tokens - k, pltpu.roll(a, tokens - k, 0), 0.0)

    def elements(j, _):
        at = lanes(j)

        def shifted(i):
            a = pre[i, :, at].astype(F32)
            return down(a, 2), down(a, 1), a

        def conv(taps, a):
            return taps[0:1] * a[0] + taps[1:2] * a[1] + taps[2:3] * a[2]

        def back(taps, d):
            return (taps[2:3] * d + taps[1:2] * upward(d, 1) + taps[0:1] * upward(d, 2)).astype(BF)

        tg, tv = cg[:, at], cv[:, at]
        ga, va = shifted(0), shifted(1)
        g = conv(tg * gs[:, at], ga)
        v = conv(tv * vs[:, at], va)
        sig = 1.0 / (1.0 + jnp.exp(-g))
        base = pre[2, :, at].astype(F32) * sig
        d_gate = base * v * (1.0 + g * (1.0 - sig))
        d_value = base * g
        cot[j, 0:tokens, 0:LANES] = back(tg, d_gate)
        cot[j, 0:tokens, LANES : 2 * LANES] = back(tv, d_value)
        for k in range(3):
            sown[k : k + 1, at] = jnp.sum(d_gate * ga[k], axis=0, keepdims=True)
            sown[3 + k : 4 + k, at] = jnp.sum(d_value * va[k], axis=0, keepdims=True)

        @pl.when(j < 2)
        def _():
            y_copy(j).start()

        return 0

    span = (pieces + 1) // 2 * LANES

    def part_of(which):
        return pl.ds(pl.multiple_of(which * (pieces * LANES - span), LANES), span)

    def pair_copy():
        return remote(
            sown.at[:, part_of(1 - y)], sfrom, ssend_sem.at[2], srecv_sem.at[2], y_dev
        )

    def send_y(j, _):
        y_copy(j).start()
        return 0

    lax.fori_loop(0, pieces, elements, 0)
    pair_copy().start()
    lax.fori_loop(2, pieces, send_y, 0)

    xy.wait_recv()
    xx1 = remote(xb.at[n_tp + tp], xb.at[n_tp + tp], xsend_sem.at[0], xrecv_sem.at[3], x_dev)
    xx1.start()
    xc1 = remote(xb.at[n_tp + tp], xb.at[n_tp + tp], xsend_sem.at[0], xrecv_sem.at[2], core_dev)
    xc1.start()
    xx0.wait_recv()
    xc2 = remote(xb.at[x_tp], xb.at[x_tp], xsend_sem.at[0], xrecv_sem.at[2], core_dev)
    xc2.start()
    xx1.wait_recv()
    xc3 = remote(xb.at[n_tp + x_tp], xb.at[n_tp + x_tp], xsend_sem.at[0], xrecv_sem.at[2], core_dev)
    xc3.start()
    four = xb.at[pl.ds(0, 4)]
    remote(four, four, xsend_sem.at[0], xrecv_sem.at[2], core_dev).wait_recv()
    for q in (0, 1):
        for i in range(n_tp):
            for o in range(links):
                at = (q * n_tp + i) * rows
                xt[o, :, at : at + rows] = xb[q * n_tp + i, :, o * own : (o + 1) * own].T

    def wait_y(j):
        y_copy(j).wait_recv()

    def partial(j):
        def one(o, _):
            part[o, j] = jnp.dot(xt[o], cot[j], preferred_element_type=F32).astype(BF)
            return 0

        lax.fori_loop(0, links, one, 0)

    table = segments(links, pieces)

    def decode(p, n):
        m = n - pieces * (p + 1)
        k, j = jnp.int32(0), jnp.int32(0)
        for first, tick, low, count in table[p]:
            q = lax.div(m - first, count)
            kk = low + (m - first) - q * count
            here = m >= first
            k = jnp.where(here, kk, k)
            j = jnp.where(here, tick + q - SKEW * kk, j)
        return k, j

    def relay(way, n):
        pos = position[way]

        @pl.when((pos < links - 1) & (n < pieces * (pos + 1)))
        def _():
            q = lax.div(n, pieces)
            j = n - q * pieces
            o = real(way, pos - q)
            arrived(way, wbuf, o, j, ag_sem(way, o, j))
            ag_copy(way, o, j).start()

        @pl.when((pos < links - 1) & (n >= pieces * (pos + 1)) & (n < slots))
        def _():
            k, j = decode(0, n)
            for p in range(1, links - 1):
                kp, jp = decode(p, n)
                k, j = jnp.where(pos == p, kp, k), jnp.where(pos == p, jp, j)
            t = real(way, links - 1 - k)

            @pl.when(pos == 0)
            def _():
                rs_copy(way, part, t, j).start()

            @pl.when(pos > 0)
            def _():
                arrived(way, rs[way], t, j, rs_sem(way, t, j, c))
                rs[way][t, j] = (rs[way][t, j].astype(F32) + part[t, j].astype(F32)).astype(BF)
                rs_copy(way, rs[way], t, j).start()

    start = (8 * pieces) // 3

    def sum_copy(way):
        return remote(
            sput.at[way], sgot.at[way], ssend_sem.at[way], srecv_sem.at[way], follower[way]
        )

    total_copy = remote(stot, sall, ssend_sem.at[3], srecv_sem.at[3], y_dev)

    def sums_step(way, n):
        pos = position[way]

        @pl.when(n == pieces + (pieces - 1) * pos)
        def _():
            @pl.when(pos == 0)
            def _():
                sput[way] = spair[...]

            @pl.when(pos > 0)
            def _():
                sum_copy(way).wait_recv()
                sput[way] = spair[...] + sgot[way]

            @pl.when(pos < links - 1)
            def _():
                sum_copy(way).start()

    def sums_total():
        stot[...] = sput[0] + sput[1] - spair[...]
        total_copy.start()

    dx_at = [start + 2 * p for p in range(links - 1)] + [(links - 1) * pieces + 3]
    order = [sorted(range(links), key=lambda o, a=a: (abs(o - a), o)) for a in range(links)]

    def block_at(n, shift):
        p_is = [n == at + shift for at in dx_at]
        o = jnp.int32(0)
        for a in range(links):
            for p in range(links):
                o = jnp.where(p_is[p] & (c == a), order[a][p], o)
        hit = p_is[0]
        for one in p_is[1:]:
            hit = hit | one
        return hit, o

    def core_copy(o):
        return remote(
            dxb.at[o, 1 - core], dx1.at[o], dsend_sem.at[0], drecv_sem.at[0, o], core_dev
        )

    def across_copy(o):
        return remote(
            ds1.at[o, 1 - xx], dx2.at[o], dsend_sem.at[1], drecv_sem.at[1, o], x_dev
        )

    def home_copy(o):
        return remote(
            ds2.at[o, 1], dx3.at[o], dsend_sem.at[2], drecv_sem.at[2, o], y_dev
        )

    first_late = len([n for n in range(slots) if pieces <= n <= start and _is_lead(table, pieces, n)])

    def dx_steps(n):
        hit, o = block_at(n, 0)

        @pl.when(hit)
        def _():
            for way in (0, 1):
                @pl.when((position[way] == links - 1) & (o != c))
                def _():
                    def one(j, _):
                        arrived(way, wbuf, o, j, ag_sem(way, o, j))
                        return 0

                    lax.fori_loop(0, pieces, one, 0)

            group = next(k for k in (5, 4, 3, 2, 1) if (pieces - 1) % k == 0)

            def one(i, _):
                new = acc[...]
                for j in range(group):
                    at = 1 + group * i + j
                    new = new + ndot(cot[at], wbuf[o, at])
                acc[...] = new
                return 0

            acc[...] = ndot(cot[0], wbuf[o, 0])
            lax.fori_loop(0, (pieces - 1) // group, one, 0)
            for q in (0, 1):
                for i in range(n_tp):
                    at = (q * n_tp + i) * rows
                    dxb[o, i % 2, i // 2, q] = acc[at : at + rows].astype(BF)
            core_copy(o).start()

        hit1, o1 = block_at(n, 1)

        @pl.when(hit1)
        def _():
            core_copy(o1).wait_recv()
            ds1[o1] = (dxb[o1, core].astype(F32) + dx1[o1].astype(F32)).astype(BF)
            across_copy(o1).start()

        hit2, o2 = block_at(n, 3)

        @pl.when(hit2)
        def _():
            across_copy(o2).wait_recv()
            ds2[o2] = (ds1[o2, xx].astype(F32) + dx2[o2].astype(F32)).astype(BF)
            home_copy(o2).start()

    def final(j):
        for way in (0, 1):
            @pl.when(position[way] > 0)
            def _():
                arrived(way, rs[way], c, j, rs_sem(way, c, j, c), ends)
        at = lanes(j)

        def close(ways):
            total = part[c, j].astype(F32)
            for way in ways:
                total = total + rs[way][c, j].astype(F32)
            gw[0, :, at] = total[:, 0:LANES] * gs[:, at]
            gw[1, :, at] = total[:, LANES : 2 * LANES] * vs[:, at]

        pl.when((c > 0) & (c < links - 1))(lambda: close((0, 1)))
        pl.when(c == links - 1)(lambda: close((0,)))
        pl.when(c == 0)(lambda: close((1,)))

    def results():
        for o in range(links):
            home_copy(o).wait_recv()
            for h in (0, 1):
                at = (2 * o + h) * own

                @pl.when(y == h)
                def _():
                    gi[:, at : at + own] = ds2[o, 0]

                @pl.when(y != h)
                def _():
                    gi[:, at : at + own] = dx3[o]

        total_copy.wait_recv()
        pair_copy().wait_send()
        for h in (0, 1):
            sown[:, part_of(h)] = jnp.where(y == h, stot[...], sall[...])
        total = sown[...]
        small[0:3] = total[0:3] * gs[...]
        small[3:6] = total[3:6] * vs[...]
        small[6:7] = jnp.sum(cg[...] * total[0:3], axis=0, keepdims=True)
        small[7:8] = jnp.sum(cv[...] * total[3:6], axis=0, keepdims=True)

    wait_y(0)
    partial(0)
    pair_copy().wait_recv()
    spair[...] = sown[:, part_of(y)] + sfrom[...]
    last = slots - 3

    def slot(n, _):
        for way in (0, 1):
            relay(way, n)
            sums_step(way, n)

        @pl.when(n == start)
        def _():
            for late in range(first_late, pieces):
                wait_y(late)

        k, j = decode(0, n + 1)

        @pl.when((k == 0) & (n + 1 < slots))
        def _():
            @pl.when(n < start)
            def _():
                wait_y(j)

            partial(j)

        dx_steps(n)

        @pl.when(n == pieces + (pieces - 1) * (links - 1))
        def _():
            sums_total()

        @pl.when(n == last + pieces - 5)
        def _():
            results()

        @pl.when(n >= last)
        def _():
            final(n - last)

        return 0

    lax.fori_loop(pieces, last + pieces, slot, 0)

    seven = xb.at[pl.ds(0, 7)]
    remote(seven, seven, xsend_sem.at[0], xrecv_sem.at[0], x_dev).wait_send()
    total_copy.wait_send()
    for ref, k in ((dx1, 0), (ds1.at[:, 0], 1), (dx3, 2)):
        remote(ref, ref, dsend_sem.at[k], drecv_sem.at[k, 0], y_dev).wait_send()
    for way in (0, 1):
        @pl.when(position[way] < links - 1)
        def _():
            sum_copy(way).wait_send()
            remote(wbuf, wbuf, z_sem.at[way], hop_sem.at[way, 0], follower[way]).wait_send()
    mine = cot.at[:, pl.ds(0, tokens)]
    remote(mine, mine, ysend_sem.at[0], y_sem.at[0], y_dev).wait_send()


def _is_lead(table, pieces, n):
    m = n - pieces
    k = None
    for first, tick, low, count in table[0]:
        if m >= first:
            k = low + (m - first) % count
    return k == 0


def deliver(gi_in, gw_in, small, *refs):
    gi, gwg, gwv, ggs, gvs, gcg, gcv, sg, sv, tg, tv, sem = refs
    copies = []

    def send(src, dst):
        copies.append(pltpu.make_async_copy(src, dst, sem.at[len(copies)]))
        copies[-1].start()

    send(gw_in.at[0], gwg)
    send(gw_in.at[1], gwv)
    send(gi_in, gi)
    tg[...] = small[0:3]
    tv[...] = small[3:6]
    sg[...] = small[6:7].reshape(sg.shape)
    sv[...] = small[7:8].reshape(sv.shape)
    for src, dst in ((tg, gcg), (tv, gcv), (sg, ggs), (sv, gvs)):
        send(src, dst)
    for copy in copies:
        copy.wait()


def whole_kernel(n_fs, n_tp):
    links = n_fs // 2

    def on_device(inputs, w_gate, w_value, gate_scale, value_scale, conv_gate, conv_value,
                  gate_pre, value_pre, grad_out):
        rows, depth = inputs.shape
        own, columns = w_gate.shape
        tokens = gate_pre.shape[0]
        half = depth // 2
        pieces = columns // LANES
        anywhere = pl.BlockSpec(memory_space=pl.ANY)
        vmem = pl.BlockSpec(memory_space=pltpu.VMEM)
        dma, vm = pltpu.SemaphoreType.DMA, pltpu.VMEM
        wide = 2 * LANES
        span = (pieces + 1) // 2 * LANES
        outs = pl.pallas_call(
            functools.partial(fused, (n_fs, n_tp)),
            in_specs=[anywhere] * 10,
            out_specs=[vmem] * 3,
            out_shape=[
                vm((rows, depth), BF),
                vm((2, own, columns), F32),
                vm((8, columns), F32),
            ],
            scratch_shapes=[
                vm((2, own, columns), F32),
                vm((3, tokens, columns), BF),
                vm((links, pieces, own, wide), BF),
                vm((pieces, 2 * tokens, wide), BF),
                vm((links, pieces, own, wide), BF),
                vm((links, pieces, own, wide), BF),
                vm((links, pieces, own, wide), BF),
                vm((rows, depth), BF),
                vm((rows, half), BF),
                vm((2 * n_tp, rows, half), BF),
                vm((links, own, 2 * tokens), BF),
                vm((2 * tokens, own), F32),
                vm((links, 2, 2, 2, rows, own), BF),
                vm((links, 2, 2, rows, own), BF),
                vm((links, 2, 2, rows, own), BF),
                vm((links, 2, rows, own), BF),
                vm((links, 2, rows, own), BF),
                vm((links, rows, own), BF),
                vm((columns,), F32),
                vm((columns,), F32),
                vm((1, columns), F32),
                vm((1, columns), F32),
                vm((2, 3, columns), F32),
                vm((6, columns), F32),
                vm((6, span), F32),
                vm((6, span), F32),
                vm((2, 6, span), F32),
                vm((2, 6, span), F32),
                vm((6, span), F32),
                vm((6, span), F32),
                dma((7,)),
                dma((2, (links - 1) * len(shares(pieces)[0]) + len(shares(pieces)[1]))),
                dma((2,)),
                dma((pieces,)),
                dma((1,)),
                dma((1,)),
                dma((4,)),
                dma((3,)),
                dma((3, links)),
                dma((4,)),
                dma((4,)),
            ],
            compiler_params=pltpu.CompilerParams(
                collective_id=0, has_side_effects=True, vmem_limit_bytes=52 * 2**20
            ),
        )(
            inputs, w_gate, w_value, gate_scale, value_scale, conv_gate, conv_value,
            gate_pre, value_pre, grad_out,
        )
        return pl.pallas_call(
            deliver,
            in_specs=[vmem] * 3,
            out_specs=[anywhere] * 7,
            out_shape=[
                jax.ShapeDtypeStruct((rows, depth), BF),
                jax.ShapeDtypeStruct((own, columns), F32),
                jax.ShapeDtypeStruct((own, columns), F32),
                jax.ShapeDtypeStruct((columns,), F32),
                jax.ShapeDtypeStruct((columns,), F32),
                jax.ShapeDtypeStruct((3, columns), F32),
                jax.ShapeDtypeStruct((3, columns), F32),
            ],
            scratch_shapes=[
                vm((columns,), F32),
                vm((columns,), F32),
                vm((3, columns), F32),
                vm((3, columns), F32),
                dma((7,)),
            ],
            compiler_params=pltpu.CompilerParams(vmem_limit_bytes=2 * 2**20),
        )(*outs)

    return on_device


def solution(mesh):
    placed = (
        P(("fs", "tp"), None),
        P("fs", "tp"),
        P("fs", "tp"),
        P("tp"),
        P("tp"),
        P(None, "tp"),
        P(None, "tp"),
        P("fs", "tp"),
        P("fs", "tp"),
        P("fs", "tp"),
    )
    body = make(mesh.shape["fs"], mesh.shape["tp"])

    given = (
        P(("fs", "tp"), None),
        P("fs", "tp"),
        P("fs", "tp"),
        P("tp"),
        P("tp"),
        P(None, "tp"),
        P(None, "tp"),
    )

    def spread(one):
        return jax.shard_map(one, mesh=mesh, in_specs=placed, out_specs=given, check_vma=False)

    step = spread(body)
    general = step
    n_fs, n_tp = mesh.shape["fs"], mesh.shape["tp"]
    fast = spread(whole_kernel(n_fs, n_tp))

    def pick(*args):
        columns = args[1].shape[1] // n_tp
        if n_tp == 4 and 2 < n_fs // 2 <= 4 and columns % LANES == 0 and columns >= 8 * LANES:
            return fast(*args)
        return general(*args)

    return pick
```
